32 devices in a mesh: sp: 8 (over z, x), tp: 4 (over y, core).
Axes of the slice: x: 2, y: 2, z: 4, core: 2. Of those that a mesh axis runs over, the one named last changes fastest.
Arguments:
- residual_in: bfloat16 [1024, 2048], P('sp', 'tp'), may hold values from -8 to 8
- query_alpha: bfloat16 [1024, 2048], P('sp', 'tp'), may hold values from -8 to 8
- pairs_alpha: bfloat16 [1024, 16, 128], P('sp', 'tp'), may hold values from -8 to 8
- offset_alpha: float32 [1024, 32], P('sp', 'tp'), may hold values from -18 to -1
- gain_alpha: float32 [2048], P('tp'), may hold values from 0.1 to 1.9
- query_beta: bfloat16 [1024, 2048], P('sp', 'tp'), may hold values from -8 to 8
- pairs_beta: bfloat16 [1024, 16, 256], P('sp', 'tp'), may hold values from -8 to 8
- offset_beta: float32 [1024, 16], P('sp', 'tp'), may hold values from -18 to -1
- gain_beta: float32 [2048], P('tp'), may hold values from 0.1 to 1.9
- project_alpha: bfloat16 [2048, 2048], P('tp'), may hold values from -0.09375 to 0.09375
- project_beta: bfloat16 [2048, 2048], P('tp'), may hold values from -0.09375 to 0.09375
- gain_settle: float32 [2048], P('tp'), may hold values from 0 to 4
- bias_settle: float32 [2048], P('tp'), may hold values from -2.5 to 2.5
- expert_ids: int32 [1024, 2], P('sp'), may hold values from 0 to 7, as said below
- route_weight: float32 [1024, 2], P('sp'), may hold values from 0.1 to 0.9
- expert_gate: bfloat16 [8, 2048, 4096], P('sp', None, 'tp'), may hold values from -0.125 to 0.125
- expert_up: bfloat16 [8, 2048, 4096], P('sp', None, 'tp'), may hold values from -0.125 to 0.125
- expert_down: bfloat16 [8, 4096, 2048], P('sp', 'tp'), may hold values from -0.1875 to 0.1875
- gain_final: float32 [2048], P('tp'), may hold values from 0.1 to 1.9
- bias_final: float32 [2048], P('tp'), may hold values from -2.5 to 2.5
Outputs:
- layer_out: bfloat16 [1024, 2048], P('sp', 'tp')
The draws below stay inside these ranges and needn't reach their ends.
Inputs may be any that keep to these rules, and one draw needn't show every extreme that they name: `expert_ids`: the two numbers of a row differ and lie in one group of 2 consecutive experts. Among the rows of one device, no expert is named more than 48 times, and every expert of one group, the same group for all devices, is named exactly 48 times.
All inputs are finite; a program needn't handle non-finite values.
Results may differ from the reference program's by a relative error of at most 0.018.
Values may be sent and summed in bfloat16 or wider, within the bound.
A program may use at most 64 MiB of HBM per device.

```python
import math
import jax
import jax.numpy as jnp
from jax import lax

D = 2048
HA = 32
DA = 64
HKA = 16
HB = 16
DB = 128
FFE = 4096
GROUPS = 4
TOK_DEV = 128
TOKEN_COUNT = 1024
EXPERTS = 8
EPG = 2
CAP = 48
HEAVY = 48
N_SP = 8
N_TP = 4


def rising(count, top):
    return top ** (jnp.arange(count, dtype=jnp.float32) / (count - 1))


def draw_residual_in(key, part):
    stream = jax.random.fold_in(key, 11)
    anchor_figure = jnp.clip(jax.random.normal(stream, (TOKEN_COUNT, D), jnp.float32), -4.0, 4.0)
    scale = rising(D, 3.0) / 1.7
    return (anchor_figure * scale[None, :]).astype(jnp.bfloat16)


def pair_draw(key, heads, width):
    first, second = jax.random.split(key)
    keys = 1.6 * jnp.clip(jax.random.normal(first, (TOKEN_COUNT, heads, width), jnp.float32), -4.0, 4.0)
    values = jnp.clip(jax.random.normal(second, (TOKEN_COUNT, heads, width), jnp.float32), -4.0, 4.0)
    values = values * (rising(heads, 3.0) / 1.7)[None, :, None]
    return jnp.concatenate([keys, values], axis=2).astype(jnp.bfloat16)


def draw_pairs_alpha(key, part):
    return pair_draw(jax.random.fold_in(key, 21), HKA, DA)


def draw_pairs_beta(key, part):
    return pair_draw(jax.random.fold_in(key, 22), HB, DB)


def offset_draw(key, heads):
    streams = jax.random.split(key, 7)
    blocks = TOKEN_COUNT // TOK_DEV
    share = 0.5
    fast = jax.random.uniform(streams[0], (heads,), jnp.float32) < share
    slow_base = -math.log(TOKEN_COUNT) - 3.3 - jax.random.uniform(streams[1], (heads,), jnp.float32, 0.5, 2.5)
    fast_base = -math.log(40.0) - 3.3 + jax.random.uniform(streams[2], (heads,), jnp.float32, -0.5, 0.5)
    anchor_figure = jnp.where(fast, fast_base, slow_base)
    slope_figure = jnp.repeat(jax.random.uniform(streams[3], (blocks, heads), jnp.float32, -0.7, 0.7), TOK_DEV, axis=0)
    coarse_estimate = jax.random.uniform(streams[4], (TOKEN_COUNT, heads), jnp.float32, -0.4, 0.4)
    marked_places = jax.random.randint(streams[5], (3, heads), 1, TOKEN_COUNT)
    sudden_jump_figure = jnp.any(jnp.arange(TOKEN_COUNT)[:, None, None] == marked_places[None, :, :], axis=1)
    dominant_figure = jax.random.uniform(streams[6], (TOKEN_COUNT, heads), jnp.float32, -2.5, -1.0)
    return jnp.where(sudden_jump_figure, dominant_figure, anchor_figure[None, :] + slope_figure + coarse_estimate).astype(jnp.float32)


def draw_offset_alpha(key, part):
    return offset_draw(jax.random.fold_in(key, 31), HA)


def draw_offset_beta(key, part):
    return offset_draw(jax.random.fold_in(key, 32), HB)


def draw_gain_settle(key, part):
    stream = jax.random.fold_in(key, 41)
    anchor_figure = 1.0 + 0.18 * jax.random.uniform(stream, (D,), jnp.float32, -1.0, 1.0)
    scale = rising(D, 3.0) / 1.7
    return (anchor_figure * scale).astype(jnp.float32)


def draw_expert_ids(key, part):
    blocks = TOKEN_COUNT // TOK_DEV
    heavy_group = jax.random.randint(jax.random.fold_in(key, 51), (), 0, GROUPS)

    def one_block(block_key):
        streams = jax.random.split(block_key, 5)
        rank = jax.random.permutation(streams[0], TOK_DEV)
        offset = jax.random.randint(streams[1], (GROUPS,), 0, EPG)
        stride = jax.random.randint(streams[2], (GROUPS,), 1, EPG)
        rotate = jax.random.randint(streams[3], (), 0, GROUPS - 1)
        flip = jax.random.randint(streams[4], (TOK_DEV,), 0, 2)
        in_heavy = rank < HEAVY
        rest = rank - HEAVY
        other = (heavy_group + 1 + (rest % (GROUPS - 1) + rotate) % (GROUPS - 1)) % GROUPS
        group = jnp.where(in_heavy, heavy_group, other)
        index = jnp.where(in_heavy, rank, rest // (GROUPS - 1))
        lead = group * EPG + (offset[group] + index) % EPG
        trail = group * EPG + (offset[group] + index + stride[group]) % EPG
        left = jnp.where(flip == 1, trail, lead)
        right = jnp.where(flip == 1, lead, trail)
        return jnp.stack([left, right], axis=1)
    ids = jax.vmap(one_block)(jax.random.split(jax.random.fold_in(key, 52), blocks))
    return ids.reshape(TOKEN_COUNT, 2).astype(jnp.int32)


def shard_levels(own_key, shape, shards, low, largest):
    def one(position, blocks):
        heights = jax.random.uniform(jax.random.fold_in(jax.random.fold_in(own_key, 6), position), (blocks,), jnp.float32, low / len(shards), largest / len(shards))
        return jnp.repeat(jnp.exp(heights), shape[position] // blocks).reshape((-1,) + (1,) * (len(shape) - position - 1))

    level = one(*shards[0])
    for cut in shards[1:]:
        level = level * one(*cut)
    return level


def noise(own_key, extent, deviation, most, cuts=(), kind=jnp.bfloat16):
    drawn = deviation * jax.random.normal(own_key, extent, jnp.float32)
    if cuts:
        drawn = drawn * shard_levels(own_key, extent, cuts, -0.22, 0.18)
    return jnp.clip(drawn, -most, most).astype(kind)


def setup_inputs(seed: int = 0) -> dict:
    arg_keys = jax.random.split(jax.random.key(seed), 21)
    residual_in = draw_residual_in(jax.random.fold_in(arg_keys[20], 71), 0)
    query_alpha = noise(arg_keys[1], (TOKEN_COUNT, HA * DA), 1.6, 8.0, ((0, 8), (1, 4)))
    pairs_alpha = draw_pairs_alpha(jax.random.fold_in(arg_keys[20], 71), 0)
    offset_alpha = draw_offset_alpha(jax.random.fold_in(arg_keys[20], 71), 0)
    gain_alpha = jnp.clip(1.0 + 0.18 * jax.random.normal(arg_keys[4], (HA * DA,), jnp.float32), 0.1, 1.9)
    query_beta = noise(arg_keys[5], (TOKEN_COUNT, HB * DB), 1.6, 8.0, ((0, 8), (1, 4)))
    pairs_beta = draw_pairs_beta(jax.random.fold_in(arg_keys[20], 71), 0)
    offset_beta = draw_offset_beta(jax.random.fold_in(arg_keys[20], 71), 0)
    gain_beta = jnp.clip(1.0 + 0.18 * jax.random.normal(arg_keys[8], (HB * DB,), jnp.float32), 0.1, 1.9)
    project_alpha = noise(arg_keys[9], (HA * DA, D), (HA * DA + HB * DB) ** -0.5, 0.09375, ((0, 4),))
    project_beta = noise(arg_keys[10], (HB * DB, D), (HA * DA + HB * DB) ** -0.5, 0.09375, ((0, 4),))
    gain_settle = draw_gain_settle(jax.random.fold_in(arg_keys[20], 71), 0)
    bias_settle = noise(arg_keys[12], (D,), 0.5, 2.5, ((0, 4),), jnp.float32)
    expert_ids = draw_expert_ids(jax.random.fold_in(arg_keys[20], 71), 0)
    route_weight = jnp.clip(0.1 + 0.79999997 * jax.random.uniform(arg_keys[14], (TOKEN_COUNT, 2), jnp.float32) ** shard_levels(arg_keys[14], (TOKEN_COUNT, 2), ((0, 8),), -0.2, 0.2), 0.1, 0.9)
    expert_gate = noise(arg_keys[15], (EXPERTS, D, FFE), D ** -0.5, 0.125, ((0, 8), (2, 4)))
    expert_up = noise(arg_keys[16], (EXPERTS, D, FFE), D ** -0.5, 0.125, ((0, 8), (2, 4)))
    expert_down = noise(arg_keys[17], (EXPERTS, FFE, D), (FFE // 4) ** -0.5, 0.1875, ((0, 8), (1, 4)))
    gain_final = jnp.clip(1.0 + 0.18 * jax.random.normal(arg_keys[18], (D,), jnp.float32), 0.1, 1.9)
    bias_final = noise(arg_keys[19], (D,), 0.5, 2.5, ((0, 4),), jnp.float32)
    return dict(residual_in=residual_in, query_alpha=query_alpha, pairs_alpha=pairs_alpha, offset_alpha=offset_alpha, gain_alpha=gain_alpha, query_beta=query_beta, pairs_beta=pairs_beta, offset_beta=offset_beta, gain_beta=gain_beta, project_alpha=project_alpha, project_beta=project_beta, gain_settle=gain_settle, bias_settle=bias_settle, expert_ids=expert_ids, route_weight=route_weight, expert_gate=expert_gate, expert_up=expert_up, expert_down=expert_down, gain_final=gain_final, bias_final=bias_final)


depth_scale = 2.0 ** 0.5
norm_eps = 1e-05

def stick_heads(queries, pairs, offsets, heads, kv_heads, width):
    share = heads // kv_heads
    q_heads = jnp.transpose(queries.reshape(TOKEN_COUNT, heads, width), (1, 0, 2))
    k_heads = jnp.transpose(pairs[:, :, :width], (1, 0, 2))
    v_heads = jnp.transpose(pairs[:, :, width:], (1, 0, 2))
    scale = width ** (-0.5)
    key_pos = jnp.arange(TOKEN_COUNT, dtype=jnp.int32)
    firsts = jnp.arange(TOKEN_COUNT // TOK_DEV, dtype=jnp.int32) * TOK_DEV

    def one_head(args):
        q_all, bias, index = args
        keys = k_heads[index // share]
        values = v_heads[index // share]
        blocks = q_all.reshape(TOKEN_COUNT // TOK_DEV, TOK_DEV, width)

        def one_block(inner):
            q_rows, first = inner
            scores = jnp.dot(q_rows, keys.T, preferred_element_type=jnp.float32) * scale + bias[None, :]
            query_pos = first + jnp.arange(TOK_DEV, dtype=jnp.int32)
            valid = key_pos[None, :] < query_pos[:, None]
            soft = jnp.where(valid, jax.nn.softplus(scores), 0.0)
            later = lax.cumsum(soft, axis=1, reverse=True) - soft
            weights = jnp.where(valid, jnp.exp(jax.nn.log_sigmoid(scores) - later), 0.0).astype(jnp.bfloat16)
            return jnp.dot(weights, values, preferred_element_type=jnp.float32)
        return lax.map(one_block, (blocks, firsts)).reshape(TOKEN_COUNT, width)
    out = lax.map(one_head, (q_heads, jnp.transpose(offsets), jnp.arange(heads, dtype=jnp.int32)))
    return jnp.transpose(out, (1, 0, 2)).reshape(TOKEN_COUNT, heads * width)

def group_norm(attend, gain):
    mean_sq = lax.optimization_barrier(jnp.mean(attend * attend, axis=1, keepdims=True))
    return (attend * lax.rsqrt(mean_sq + norm_eps) * gain).astype(jnp.bfloat16)

def shard_sum(products, count):

    def add_piece(total, index):
        term = jnp.zeros((count, D), jnp.float32)
        for left, right in products:
            width = left.shape[1] // N_TP
            piece = lax.dynamic_slice_in_dim(left, index * width, width, 1)
            block = lax.dynamic_slice_in_dim(right, index * width, width, 0)
            term = term + jnp.dot(piece, block, preferred_element_type=jnp.float32)
        rounded = lax.optimization_barrier(term.astype(jnp.bfloat16))
        return (total + rounded.astype(jnp.float32), None)
    total, _ = lax.scan(add_piece, jnp.zeros((count, D), jnp.float32), jnp.arange(N_TP, dtype=jnp.int32))
    return total

def layer_norm(total, gain, bias):
    mean = lax.optimization_barrier(jnp.sum(total, axis=1, keepdims=True)) / D
    var = lax.optimization_barrier(jnp.sum(total * total, axis=1, keepdims=True)) / D - mean * mean
    return ((total - mean) * lax.rsqrt(var + norm_eps) * gain + bias).astype(jnp.bfloat16)

def reference(residual_in, query_alpha, pairs_alpha, offset_alpha, gain_alpha, query_beta, pairs_beta, offset_beta, gain_beta, project_alpha, project_beta, gain_settle, bias_settle, expert_ids, route_weight, expert_gate, expert_up, expert_down, gain_final, bias_final):
    attend_alpha = stick_heads(query_alpha, pairs_alpha, offset_alpha, HA, HKA, DA)
    attend_beta = stick_heads(query_beta, pairs_beta, offset_beta, HB, HB, DB)
    normed_alpha = group_norm(attend_alpha, gain_alpha)
    normed_beta = group_norm(attend_beta, gain_beta)
    mixed = shard_sum(((normed_alpha, project_alpha), (normed_beta, project_beta)), TOKEN_COUNT).astype(jnp.bfloat16)
    first = depth_scale * residual_in.astype(jnp.float32) + mixed.astype(jnp.float32)
    settled = layer_norm(first, gain_settle, bias_settle)
    ids = expert_ids.reshape(N_SP, 2 * TOK_DEV)
    onehot = (ids[:, :, None] == jnp.arange(EXPERTS, dtype=jnp.int32)[None, None, :]).astype(jnp.int32)
    before = jnp.cumsum(onehot, axis=1, dtype=jnp.int32) - onehot
    slot = lax.optimization_barrier(jnp.sum(before * onehot, axis=2, dtype=jnp.int32))
    place = (jnp.arange(N_SP, dtype=jnp.int32)[:, None] * CAP + slot).reshape(TOKEN_COUNT * 2)
    owner = jnp.arange(TOKEN_COUNT * 2, dtype=jnp.int32) // 2
    table = jnp.full((EXPERTS, N_SP * CAP), TOKEN_COUNT, jnp.int32).at[expert_ids.reshape(TOKEN_COUNT * 2), place].set(owner)
    padded = jnp.concatenate([settled, jnp.zeros((1, D), jnp.bfloat16)], axis=0)

    def one_expert(args):
        rows, gate_w, up_w, down_w = args
        inputs = padded[rows]
        gate = jnp.dot(inputs, gate_w, preferred_element_type=jnp.float32)
        up = jnp.dot(inputs, up_w, preferred_element_type=jnp.float32)
        hidden = (jax.nn.silu(gate) * up).astype(jnp.bfloat16)
        return shard_sum(((hidden, down_w),), N_SP * CAP).astype(jnp.bfloat16)
    outputs = lax.map(one_expert, (table, expert_gate, expert_up, expert_down))
    picked = outputs[expert_ids, place.reshape(TOKEN_COUNT, 2)].astype(jnp.float32)
    routed = route_weight[:, 0:1] * picked[:, 0] + route_weight[:, 1:2] * picked[:, 1]
    second = depth_scale * settled.astype(jnp.float32) + routed
    return layer_norm(second, gain_final, bias_final)
```

```python
import functools
import jax
import jax.numpy as jnp
from jax import lax
from jax.experimental import pallas as pl
from jax.experimental.pallas import tpu as pltpu
from jax.sharding import PartitionSpec as P

depth_scale = 2.0**0.5
norm_eps = 1e-05
F32 = jnp.float32
BF16 = jnp.bfloat16
VMEM = pltpu.VMEM
DMA = pltpu.SemaphoreType.DMA


def remote(src, dst, send, recv, where):
    return pltpu.make_async_remote_copy(
        src_ref=src,
        dst_ref=dst,
        send_sem=send,
        recv_sem=recv,
        device_id=where,
        device_id_type=pl.DeviceIdType.MESH,
    )


def greet(n_sp, n_tp, sp, tp):
    barrier = pltpu.get_barrier_semaphore()
    for o in range(1, n_sp):
        pl.semaphore_signal(
            barrier,
            inc=1,
            device_id={"sp": lax.rem(sp + o, n_sp), "tp": tp},
            device_id_type=pl.DeviceIdType.MESH,
        )
    for o in range(1, n_tp):
        pl.semaphore_signal(
            barrier,
            inc=1,
            device_id={"sp": sp, "tp": lax.rem(tp + o, n_tp)},
            device_id_type=pl.DeviceIdType.MESH,
        )
    pl.semaphore_wait(barrier, n_sp + n_tp - 2)


def split(x):
    high = x.astype(BF16)
    return high, (x - high.astype(F32)).astype(BF16)


def lane_sums(x):
    ones = jnp.ones((8, x.shape[1]), BF16)
    dims = (((1,), (1,)), ((), ()))
    high, low = split(x)
    return lax.dot_general(ones, high, dims, preferred_element_type=F32) + lax.dot_general(
        ones, low, dims, preferred_element_type=F32
    )


def column(row, rows):
    return jnp.transpose(jnp.broadcast_to(row[0:1, :], (rows, rows)))[:, 0:1]


def stats_start(n_tp, sp, tp, one, two, stat, send, recv):
    stat[tp, 0] = one
    stat[tp, 1] = two
    for o in range(1, n_tp):
        remote(
            stat.at[tp], stat.at[tp], send.at[o], recv.at[tp], {"sp": sp, "tp": lax.rem(tp + o, n_tp)}
        ).start()


def stats_finish(n_tp, sp, tp, stat, send, recv, rows):
    for o in range(1, n_tp):
        peer = lax.rem(tp + o, n_tp)
        remote(stat.at[peer], stat.at[peer], send.at[o], recv.at[peer], {"sp": sp, "tp": peer}).wait_recv()
    for o in range(1, n_tp):
        peer = lax.rem(tp + o, n_tp)
        remote(stat.at[tp], stat.at[tp], send.at[o], recv.at[tp], {"sp": sp, "tp": peer}).wait_send()
    total = stat[0]
    for t in range(1, n_tp):
        total = total + stat[t]
    return column(total[0], rows), column(total[1], rows)


def norm(total, one, two, gain, bias, columns):
    mean = one / columns
    var = two / columns - mean * mean
    return ((total - mean) * lax.rsqrt(var + norm_eps) * gain + bias).astype(BF16)


def attend_kernel(
    early,
    n_sp,
    n_tp,
    nx,
    kva,
    kvb,
    qa_ref,
    qb_ref,
    kva_hbm,
    kvb_hbm,
    off_hbm,
    res_ref,
    ga_ref,
    gb_ref,
    pa_hbm,
    pb_hbm,
    gs_ref,
    bs_ref,
    out_ref,
    kvbuf,
    offbuf,
    qs,
    acc,
    rem,
    pa,
    pb,
    ya,
    yb,
    part,
    got,
    stat1,
    stat2,
    load_sem,
    kv_send,
    kv_recv,
    off_send,
    off_recv,
    part_send,
    part_recv,
    s1_send,
    s1_recv,
    s2_send,
    s2_recv,
):
    sp = lax.axis_index("sp")
    tp = lax.axis_index("tp")
    nz = n_sp // nx
    z = sp // nx
    x = lax.rem(sp, nx)
    rows = qa_ref.shape[0]
    cols = out_ref.shape[1]
    loads = (
        pltpu.make_async_copy(kva_hbm, kvbuf.at[sp, :, 0 : kva * 128], load_sem.at[0]),
        pltpu.make_async_copy(off_hbm, offbuf.at[sp], load_sem.at[1]),
        pltpu.make_async_copy(pa_hbm, pa, load_sem.at[2]),
        pltpu.make_async_copy(pb_hbm, pb, load_sem.at[3]),
        pltpu.make_async_copy(kvb_hbm, kvbuf.at[sp, :, kva * 128 :], load_sem.at[4]),
    )
    for load in loads:
        load.start()
    greet(n_sp, n_tp, sp, tp)
    lane = lax.broadcasted_iota(jnp.int32, (rows, 128), 1)
    row_i = lax.broadcasted_iota(jnp.int32, (rows, 128), 0)
    first_half = lane < 64
    for u in range(kva):
        q32 = qa_ref[:, u * 128 : (u + 1) * 128].astype(F32) * (64**-0.5)
        qs[u, 0:rows] = jnp.where(first_half, q32, 0.0).astype(BF16)
        qs[u, rows : 2 * rows] = jnp.where(first_half, pltpu.roll(q32, 64, 1), 0.0).astype(BF16)
    acc[...] = jnp.zeros_like(acc)
    rem[...] = jnp.zeros_like(rem)
    tri_r = lax.broadcasted_iota(jnp.int32, (256, 256), 0) % 128
    tri_c = lax.broadcasted_iota(jnp.int32, (256, 256), 1)
    tri = jnp.where((tri_r > tri_c) | (tri_c >= 128), 1.0, 0.0).astype(BF16)

    def block(j):
        gap = (sp - j) * rows
        valid1 = lane < row_i + gap
        valid2 = jnp.concatenate([valid1.astype(F32)] * 2, axis=0) > 0.5

        def unit(query, key, value, offset, scale, valid, left):
            s = lax.dot_general(query, key, (((1,), (1,)), ((), ())), preferred_element_type=F32)
            s = (s if scale is None else s * scale) + offset
            soft = jnp.maximum(s, 0.0) + jnp.log(1.0 + jnp.exp(-jnp.abs(s)))
            used = jnp.where(valid, soft, 0.0)
            high, low = split(used)
            sums = jnp.dot(jnp.concatenate([high, low], axis=1), tri, preferred_element_type=F32)
            w = jnp.where(valid, jnp.exp(s - soft - sums[:, :128] + left), 0.0).astype(BF16)
            return jnp.dot(w, value, preferred_element_type=F32), sums[:, 128:]

        for u in range(kva):
            pair = kvbuf[j, :, u * 128 : (u + 1) * 128]
            offset = jnp.concatenate(
                [
                    jnp.broadcast_to(offbuf[j, 2 * u : 2 * u + 1, :], (rows, 128)),
                    jnp.broadcast_to(offbuf[j, 2 * u + 1 : 2 * u + 2, :], (rows, 128)),
                ],
                axis=0,
            )
            left = rem[2 * u * rows : (2 * u + 2) * rows]
            o, total = unit(qs[u], pair, pair, offset, None, valid2, left)
            rem[2 * u * rows : (2 * u + 2) * rows] = left - total
            acc[:, u * 128 : (u + 1) * 128] += jnp.where(
                first_half, pltpu.roll(o[:rows], 64, 1), o[rows:]
            )
        for u in range(kvb):
            base = kva * 128 + u * 256
            head = 2 * kva + u
            key = kvbuf[j, :, base : base + 128]
            value = kvbuf[j, :, base + 128 : base + 256]
            offset = offbuf[j, head : head + 1, :]
            left = rem[head * rows : (head + 1) * rows]
            query = qb_ref[:, u * 128 : (u + 1) * 128]
            o, total = unit(query, key, value, offset, 128**-0.5, valid1, left)
            rem[head * rows : (head + 1) * rows] = left - total
            c = (kva + u) * 128
            acc[:, c : c + 128] += o

    def sends(s):
        j0 = (z - s) * nx + x
        plan = [(z + 1 < nz, jnp.minimum(z + 1, nz - 1) * nx + x)]
        for d in range(1, nx):
            xo = lax.rem(x + d, nx)
            plan.append(((s > 0) | (x < xo), z * nx + xo))
        made = []
        for k, (cond, dest) in enumerate(plan):
            where = {"sp": dest, "tp": tp}
            made.append(
                (
                    cond,
                    remote(kvbuf.at[j0], kvbuf.at[j0], kv_send.at[s, k], kv_recv.at[j0], where),
                    remote(offbuf.at[j0], offbuf.at[j0], off_send.at[s, k], off_recv.at[j0], where),
                )
            )
        return made

    def wait_block(j):
        where = {"sp": sp, "tp": tp}
        remote(kvbuf.at[j], kvbuf.at[j], kv_send.at[0, 0], kv_recv.at[j], where).wait_recv()
        remote(offbuf.at[j], offbuf.at[j], off_send.at[0, 0], off_recv.at[j], where).wait_recv()

    loads[0].wait()
    loads[1].wait()
    loads[4].wait()

    def forward(s):
        @pl.when(s > 0)
        def _():
            wait_block((z - s) * nx + x)

        for cond, kv_copy, off_copy in sends(s):

            @pl.when(cond)
            def _(kv_copy=kv_copy, off_copy=off_copy):
                off_copy.start()
                kv_copy.start()

    forward(0)

    def level(s, carry):
        src = z - s

        @pl.when(s < z)
        def _():
            forward(s + 1)

        def across(i, inner):
            xo = nx - 1 - i

            @pl.when((s > 0) | (xo <= x))
            def _():
                @pl.when(xo != x)
                def _():
                    wait_block(src * nx + xo)

                block(src * nx + xo)

            return inner

        return lax.fori_loop(0, nx, across, carry)

    lax.fori_loop(0, z + 1, level, 0)
    early()

    wide = kva * 128
    aa = acc[:, :wide]
    ab = acc[:, wide:]
    stats_start(n_tp, sp, tp, lane_sums(aa * aa), lane_sums(ab * ab), stat1, s1_send, s1_recv)
    loads[2].wait()
    loads[3].wait()
    na = (aa * ga_ref[...]).astype(BF16)
    nb = (ab * gb_ref[...]).astype(BF16)
    for t in range(n_tp):
        ya[t] = jnp.dot(na, pa[:, t * cols : (t + 1) * cols], preferred_element_type=F32)
        yb[t] = jnp.dot(nb, pb[:, t * cols : (t + 1) * cols], preferred_element_type=F32)
    sq_a, sq_b = stats_finish(n_tp, sp, tp, stat1, s1_send, s1_recv, rows)
    scale_a = lax.rsqrt(sq_a / (wide * n_tp) + norm_eps)
    scale_b = lax.rsqrt(sq_b / (kvb * 128 * n_tp) + norm_eps)

    def part_copy(o):
        peer = lax.rem(tp + o, n_tp)
        return remote(
            part.at[peer], got.at[tp], part_send.at[o], part_recv.at[tp], {"sp": sp, "tp": peer}
        )

    for o in range(1, n_tp):
        peer = lax.rem(tp + o, n_tp)
        part[peer] = (ya[peer] * scale_a + yb[peer] * scale_b).astype(BF16)
        part_copy(o).start()
    total = (ya[tp] * scale_a + yb[tp] * scale_b).astype(BF16).astype(F32)
    for o in range(1, n_tp):
        peer = lax.rem(tp + o, n_tp)
        remote(
            part.at[peer], got.at[peer], part_send.at[o], part_recv.at[peer], {"sp": sp, "tp": peer}
        ).wait_recv()
        total = total + got[peer].astype(F32)
    mixed = total.astype(BF16).astype(F32)
    first = depth_scale * res_ref[...].astype(F32) + mixed
    stats_start(n_tp, sp, tp, lane_sums(first), lane_sums(first * first), stat2, s2_send, s2_recv)
    for o in range(1, n_tp):
        part_copy(o).wait_send()

    def drain(s, carry):
        for cond, kv_copy, off_copy in sends(s):

            @pl.when(cond)
            def _(kv_copy=kv_copy, off_copy=off_copy):
                off_copy.wait_send()
                kv_copy.wait_send()

        return carry

    lax.fori_loop(0, z + 1, drain, 0)
    one, two = stats_finish(n_tp, sp, tp, stat2, s2_send, s2_recv, rows)
    out_ref[...] = norm(first, one, two, gs_ref[...], bs_ref[...], cols * n_tp)


def plane_attend(
    early,
    n_sp,
    n_tp,
    nx,
    kva,
    kvb,
    qa_ref,
    qb_ref,
    pairs_a_hbm,
    pairs_b_hbm,
    offa_ref,
    offb_ref,
    res_ref,
    ga_ref,
    gb_ref,
    pa_hbm,
    pb_hbm,
    gs_ref,
    bs_ref,
    out_ref,
    raw_a,
    raw_b,
    wide_a,
    wide_b,
    own_a,
    own_b,
    own_off,
    qin,
    kin,
    oin,
    keys2,
    values2,
    left,
    acc,
    obuf,
    ain,
    pa,
    pb,
    ya,
    yb,
    part,
    got,
    stat1,
    stat2,
    load_sem,
    in_send,
    in_recv,
    o_send,
    o_recv,
    part_send,
    part_recv,
    s1_send,
    s1_recv,
    s2_send,
    s2_recv,
):
    sp = lax.axis_index("sp")
    tp = lax.axis_index("tp")
    nz = n_sp // nx
    z = sp // nx
    x = lax.rem(sp, nx)
    rows = qa_ref.shape[0]
    cols = out_ref.shape[1]
    tall = nx * rows

    def is_alpha(zz, xx):
        return lax.rem(zz + xx, 2) == 0

    loads = (
        pltpu.make_async_copy(pairs_a_hbm, raw_a, load_sem.at[0]),
        pltpu.make_async_copy(pairs_b_hbm, raw_b, load_sem.at[1]),
        pltpu.make_async_copy(pa_hbm, pa, load_sem.at[2]),
        pltpu.make_async_copy(pb_hbm, pb, load_sem.at[3]),
    )
    loads[0].start()
    loads[1].start()
    for u in range(nz):
        own_off[u, 0:2] = offa_ref[2 * u : 2 * u + 2]
        own_off[u, 2:3] = offb_ref[u : u + 1]
    greet(n_sp, n_tp, sp, tp)
    loads[0].wait()
    wide_a[...] = raw_a[...].astype(F32)
    for u in range(kva):
        own_a[u] = wide_a[pl.ds(u, rows, stride=kva), :].astype(BF16)
    loads[1].wait()
    wide_b[...] = raw_b[...].astype(F32)
    for u in range(kvb):
        for h in range(2):
            own_b[u, h] = wide_b[pl.ds(h * kvb + u, rows, stride=2 * kvb), :].astype(BF16)
    loads[2].start()
    loads[3].start()

    def in_copies(zz, xx, alpha):
        dest = zz * nx + xx
        where = {"sp": dest, "tp": tp}
        at = pl.ds(pl.multiple_of(zz * 128, 128), 128)
        q_ref = qa_ref if alpha else qb_ref
        kv = (own_a.at[zz], kin.at[0, sp]) if alpha else (own_b.at[zz], kin.at[:, sp])
        return (
            remote(own_off.at[zz], oin.at[sp], in_send.at[0, dest], in_recv.at[0, sp], where),
            remote(q_ref.at[:, at], qin.at[sp], in_send.at[1, dest], in_recv.at[1, sp], where),
            remote(*kv, in_send.at[2, dest], in_recv.at[2, sp], where),
        )

    def each_dest(act):
        def hop(t, carry):
            away = (t + 1) // 2
            zz = z + away * (2 * lax.rem(t, 2) - 1)
            for xx in range(nx):
                there = (zz >= 0) & (zz < nz) & ((zz != z) | (xx != x))
                for alpha in (True, False):

                    @pl.when(there & (is_alpha(zz, xx) == alpha))
                    def _(xx=xx, alpha=alpha):
                        for copy in in_copies(zz, xx, alpha):
                            act(copy)

            return carry

        lax.fori_loop(0, 2 * nz - 1, hop, 0)

    each_dest(lambda copy: copy.start())
    early()

    def o_copy(d):
        return remote(obuf.at[d], ain.at[sp], o_send.at[d], o_recv.at[sp], {"sp": d, "tp": tp})

    lane_t = lax.broadcasted_iota(jnp.int32, (tall, tall), 1)
    row_t = lax.broadcasted_iota(jnp.int32, (tall, tall), 0)
    lane = lax.broadcasted_iota(jnp.int32, (tall, 128), 1)
    tri = jnp.where(row_t > lane_t, 1.0, 0.0).astype(BF16)

    def attend(alpha):
        heads = 2 if alpha else 1
        scale = 64**-0.5 if alpha else 128**-0.5
        at = pl.ds(pl.multiple_of(z * 128, 128), 128)
        oin[sp] = own_off[z]
        if alpha:
            qin[sp] = qa_ref[:, at]
            kin[0, sp] = own_a[z]
        else:
            qin[sp] = qb_ref[:, at]
            kin[:, sp] = own_b[z]

        def arrive(p):
            for xx in range(nx):
                s = p * nx + xx

                @pl.when(s != sp)
                def _(s=s):
                    where = {"sp": sp, "tp": tp}
                    kv = kin.at[0, s] if alpha else kin.at[:, s]
                    remote(oin.at[s], oin.at[s], in_send.at[0, 0], in_recv.at[0, s], where).wait_recv()
                    remote(qin.at[s], qin.at[s], in_send.at[1, 0], in_recv.at[1, s], where).wait_recv()
                    remote(kv, kv, in_send.at[2, 0], in_recv.at[2, s], where).wait_recv()

            if alpha:
                pair = kin[0, pl.ds(p * nx, nx)].reshape(tall, 128).astype(F32)
                turned = pltpu.roll(pair, 64, 1)
                keys2[p, 0:tall] = jnp.where(lane < 64, pair, 0.0).astype(BF16)
                keys2[p, tall:] = jnp.where(lane < 64, 0.0, turned).astype(BF16)
                values2[p, 0:tall] = jnp.where(lane < 64, turned, 0.0).astype(BF16)
                values2[p, tall:] = jnp.where(lane < 64, 0.0, pair).astype(BF16)

        def step(r, c, diag):
            query = qin[pl.ds(r * nx, nx)].reshape(tall, 128)
            if alpha:
                key, value = keys2[c], values2[c]
            else:
                key = kin[0, pl.ds(c * nx, nx)].reshape(tall, 128)
                value = kin[1, pl.ds(c * nx, nx)].reshape(tall, 128)
            scores = lax.dot_general(query, key, (((1,), (1,)), ((), ())), preferred_element_type=F32)
            valid = lane_t < row_t
            ws = []
            for h in range(heads):
                row = h if alpha else 2
                offset = jnp.concatenate([oin[c * nx + i, row : row + 1, :] for i in range(nx)], axis=1)
                s = scores[:, h * tall : (h + 1) * tall] * scale + offset
                soft = jnp.maximum(s, 0.0) + jnp.log(1.0 + jnp.exp(-jnp.abs(s)))
                used = jnp.where(valid, soft, 0.0) if diag else soft
                sums = jnp.dot(used.astype(BF16), tri, preferred_element_type=F32)
                total = jnp.broadcast_to(sums[:, 0:1] + used[:, 0:1], (tall, 128))
                e = s - soft - sums
                if diag:
                    w = jnp.where(valid, jnp.exp(e), 0.0)
                    left[h, r] = -total
                else:
                    before = left[h, r]
                    w = jnp.exp(e + jnp.concatenate([before] * nx, axis=1))
                    left[h, r] = before - total
                ws.append(w.astype(BF16))
            w = ws[0] if heads == 1 else jnp.concatenate(ws, axis=1)
            o = jnp.dot(w, value, preferred_element_type=F32)
            o = o if diag else acc[r] + o
            acc[r] = o

            @pl.when(c == 0)
            def _():
                obuf[pl.ds(r * nx, nx)] = o.astype(BF16).reshape(nx, rows, 128)
                for xx in range(nx):
                    d = r * nx + xx

                    @pl.when(d != sp)
                    def _(d=d):
                        o_copy(d).start()

                    @pl.when(d == sp)
                    def _(d=d):
                        ain[sp] = obuf[d]

        def phase(k, span):
            low, high = span
            lower_half = z < nz // 2
            up = jnp.where(lower_half, low == 0, high < nz - 1).astype(jnp.int32)
            first = (k == 0).astype(jnp.int32)
            p = first * z + (1 - first) * (up * (high + 1) + (1 - up) * (low - 1))
            arrive(p)
            step(p, p, True)
            count = (1 - first) * (high - low + 1)

            def more(t, carry):
                step(p + t * (1 - up), p - t * up, False)
                return carry

            lax.fori_loop(1, count + 1, more, 0)
            return jnp.minimum(low, p), jnp.maximum(high, p)

        lax.fori_loop(0, nz, phase, (z, z))

    for alpha in (True, False):

        @pl.when(is_alpha(z, x) == alpha)
        def _(alpha=alpha):
            attend(alpha)

    def o_wait(j, carry):
        @pl.when(j != sp)
        def _():
            remote(obuf.at[j], ain.at[j], o_send.at[0], o_recv.at[j], {"sp": sp, "tp": tp}).wait_recv()

        return carry

    lax.fori_loop(0, n_sp, o_wait, 0)
    wide = kva * 128
    aa = jnp.concatenate([ain[k * nx + k % 2] for k in range(nz)], axis=1).astype(F32)
    ab = jnp.concatenate([ain[k * nx + 1 - k % 2] for k in range(nz)], axis=1).astype(F32)
    stats_start(n_tp, sp, tp, lane_sums(aa * aa), lane_sums(ab * ab), stat1, s1_send, s1_recv)
    loads[2].wait()
    loads[3].wait()
    na = (aa * ga_ref[...]).astype(BF16)
    nb = (ab * gb_ref[...]).astype(BF16)
    for t in range(n_tp):
        ya[t] = jnp.dot(na, pa[:, t * cols : (t + 1) * cols], preferred_element_type=F32)
        yb[t] = jnp.dot(nb, pb[:, t * cols : (t + 1) * cols], preferred_element_type=F32)
    sq_a, sq_b = stats_finish(n_tp, sp, tp, stat1, s1_send, s1_recv, rows)
    scale_a = lax.rsqrt(sq_a / (wide * n_tp) + norm_eps)
    scale_b = lax.rsqrt(sq_b / (kvb * 128 * n_tp) + norm_eps)

    def part_copy(o):
        peer = lax.rem(tp + o, n_tp)
        return remote(
            part.at[peer], got.at[tp], part_send.at[o], part_recv.at[tp], {"sp": sp, "tp": peer}
        )

    for o in range(1, n_tp):
        peer = lax.rem(tp + o, n_tp)
        part[peer] = (ya[peer] * scale_a + yb[peer] * scale_b).astype(BF16)
        part_copy(o).start()
    total = (ya[tp] * scale_a + yb[tp] * scale_b).astype(BF16).astype(F32)
    for o in range(1, n_tp):
        peer = lax.rem(tp + o, n_tp)
        remote(
            part.at[peer], got.at[peer], part_send.at[o], part_recv.at[peer], {"sp": sp, "tp": peer}
        ).wait_recv()
        total = total + got[peer].astype(F32)
    mixed = total.astype(BF16).astype(F32)
    first = depth_scale * res_ref[...].astype(F32) + mixed
    stats_start(n_tp, sp, tp, lane_sums(first), lane_sums(first * first), stat2, s2_send, s2_recv)
    for o in range(1, n_tp):
        part_copy(o).wait_send()

    each_dest(lambda copy: copy.wait_send())

    def o_drain(j, carry):
        @pl.when(j != sp)
        def _():
            o_copy(j).wait_send()

        return carry

    lax.fori_loop(0, n_sp, o_drain, 0)
    one, two = stats_finish(n_tp, sp, tp, stat2, s2_send, s2_recv, rows)
    out_ref[...] = norm(first, one, two, gs_ref[...], bs_ref[...], cols * n_tp)


def expert_kernel(
    attention,
    balanced,
    n_sp,
    n_tp,
    nx,
    cap,
    set_ref,
    ids_ref,
    wg_hbm,
    wu_hbm,
    wd_hbm,
    gf_ref,
    bf_ref,
    out_ref,
    wg,
    wu,
    wd,
    sendbuf,
    xbuf,
    gate,
    up,
    hid,
    away,
    arrived,
    home,
    pre,
    peers,
    outb,
    back,
    stat,
    load_sem,
    a_send,
    a_recv,
    x_send,
    x_recv,
    relay_send,
    d_send,
    d_recv,
    y_send,
    y_recv,
    b_send,
    b_recv,
    s_send,
    s_recv,
):
    sp = lax.axis_index("sp")
    tp = lax.axis_index("tp")
    rows, cols = set_ref.shape
    places = n_sp * cap
    ny = n_tp // 2
    y = tp // 2
    core = lax.rem(tp, 2)
    mate = y * 2 + 1 - core
    loads = (
        pltpu.make_async_copy(wg_hbm.at[0], wg, load_sem.at[0]),
        pltpu.make_async_copy(wu_hbm.at[0], wu, load_sem.at[1]),
        pltpu.make_async_copy(wd_hbm.at[0], wd, load_sem.at[2]),
    )

    def loop(low, high, fn):
        def step(i, carry):
            fn(i)
            return carry

        lax.fori_loop(low, high, step, 0)

    def x_copies(j):
        made = []
        for k in range(ny):
            dest = mate if k == 0 else lax.rem(y + k, ny) * 2 + core
            made.append(
                remote(
                    xbuf.at[tp, j], xbuf.at[tp, j], x_send.at[k, j], x_recv.at[tp, j], {"sp": sp, "tp": dest}
                )
            )
        return made

    def spread_out(j):
        @pl.when(j != sp)
        def _():
            remote(
                sendbuf.at[j], xbuf.at[tp, j], a_send.at[0], a_recv.at[j], {"sp": sp, "tp": tp}
            ).wait_recv()

        for copy in x_copies(j):
            copy.start()

    ahead = 0 if balanced else jnp.maximum(sp // nx - 1, 0) * nx

    def start_loads():
        for load in loads:
            load.start()

    if balanced:
        attention(start_loads)
    else:
        start_loads()
        attention(lambda: loop(0, ahead, spread_out))
    ids = ids_ref[...][:, 0:2]
    expert = lax.broadcasted_iota(jnp.int32, (rows, 128), 1).astype(F32)
    hot = [jnp.where(ids[:, k : k + 1] == expert, 1.0, 0.0) for k in range(2)]
    r = lax.broadcasted_iota(jnp.int32, (rows, rows), 0)
    c = lax.broadcasted_iota(jnp.int32, (rows, rows), 1)
    lower = jnp.where(c < r, 1.0, 0.0).astype(BF16)
    before = jnp.dot(lower, (hot[0] + hot[1]).astype(BF16), preferred_element_type=F32)
    seat = lax.broadcasted_iota(jnp.int32, (rows, places), 1).astype(F32)
    hits = []
    for k in range(2):
        slot = jnp.sum(before * hot[k], axis=1, keepdims=True)
        place = ids[:, k : k + 1] * cap + slot
        hits.append(jnp.where(place == seat, 1.0, 0.0))
    spread = jnp.transpose(hits[0] + hits[1]).astype(BF16)
    sent = jnp.dot(spread, set_ref[...], preferred_element_type=F32).astype(BF16)
    sendbuf[...] = sent.reshape(n_sp, cap, cols)

    def at_sp(o):
        return lax.rem(sp + o, n_sp)

    def a_copy(o):
        dest = at_sp(o)
        return remote(
            sendbuf.at[dest], xbuf.at[tp, sp], a_send.at[o], a_recv.at[sp], {"sp": dest, "tp": tp}
        )

    loop(1, n_sp, lambda o: a_copy(o).start())
    xbuf[tp, sp] = sendbuf[sp]

    def x_wait(t, j):
        remote(xbuf.at[t, j], xbuf.at[t, j], x_send.at[0, 0], x_recv.at[t, j], {"sp": sp, "tp": t}).wait_recv()

    loop(ahead, n_sp, spread_out)

    def relay_copy(k, o):
        t = lax.rem(y + k, ny) * 2 + core
        j = o
        return remote(
            xbuf.at[t, j], xbuf.at[t, j], relay_send.at[k, o], x_recv.at[t, j], {"sp": sp, "tp": mate}
        )

    def gather_dot(t, fresh):
        xs = xbuf[t].reshape(places, cols)
        at = pl.ds(pl.multiple_of(t * cols, 128), cols)
        g = jnp.dot(xs, wg[at, :], preferred_element_type=F32)
        u = jnp.dot(xs, wu[at, :], preferred_element_type=F32)
        if fresh:
            gate[...] = g
            up[...] = u
        else:
            gate[...] += g
            up[...] += u

    loads[0].wait()
    loads[1].wait()
    gather_dot(tp, True)

    def arrive_mate(o):
        x_wait(mate, o)

    loop(0, n_sp, arrive_mate)
    gather_dot(mate, False)

    def from_y(k):
        t = lax.rem(y + k, ny) * 2 + core
        other = lax.rem(y + k, ny) * 2 + 1 - core

        def pass_on(o):
            x_wait(t, o)
            relay_copy(k, o).start()

        loop(0, n_sp, pass_on)
        gather_dot(t, False)

        def arrive(o):
            x_wait(other, o)

        loop(0, n_sp, arrive)
        gather_dot(other, False)

    loop(1, ny, from_y)
    value = gate[...]
    hid[...] = (value / (1.0 + jnp.exp(-value)) * up[...]).astype(BF16)
    loads[2].wait()

    def down(t):
        at = pl.ds(pl.multiple_of(t * cols, 128), cols)
        result = jnp.dot(hid[...], wd[:, at], preferred_element_type=F32)
        return result.astype(BF16).reshape(n_sp, cap, cols)

    def d_copy(k):
        return remote(away.at[k], arrived.at[k], d_send.at[k], d_recv.at[k], {"sp": sp, "tp": mate})

    def down_away(i):
        k = lax.rem(i + 1, ny)
        away[k] = down(lax.rem(y + k, ny) * 2 + 1 - core)
        d_copy(k).start()

    loop(0, ny, down_away)

    def down_home(i):
        k = lax.rem(i + 1, ny)
        home[k] = down(lax.rem(y + k, ny) * 2 + core)

    loop(0, ny, down_home)

    def y_copy(k, o):
        j = at_sp(o)
        return remote(
            pre.at[k, j],
            peers.at[k, j],
            y_send.at[k, o],
            y_recv.at[k, j],
            {"sp": sp, "tp": lax.rem(y + k, ny) * 2 + core},
        )

    for i in range(ny):
        k = (i + 1) % ny
        d_copy(k).wait_recv()
        if k:

            def to_y(o, k=k):
                j = at_sp(o)
                pre[k, j] = (home[k, j].astype(F32) + arrived[k, j].astype(F32)).astype(BF16)
                y_copy(k, o).start()

            loop(1, n_sp, to_y)
            to_y(0)

    def b_copy(o):
        dest = at_sp(o)
        return remote(outb.at[dest], back.at[sp], b_send.at[o], b_recv.at[sp], {"sp": dest, "tp": tp})

    def settle(o):
        j = at_sp(o)
        total = home[0, j].astype(F32) + arrived[0, j].astype(F32)
        for k in range(1, ny):
            remote(
                pre.at[k, j], peers.at[k, j], y_send.at[k, 0], y_recv.at[k, j], {"sp": sp, "tp": mate}
            ).wait_recv()
            total = total + peers[k, j].astype(F32)
        return total.astype(BF16)

    def give_back(o):
        outb[at_sp(o)] = settle(o)
        b_copy(o).start()

    loop(1, n_sp, give_back)
    back[sp] = settle(0)

    def wait_back(o):
        j = lax.rem(sp - o + n_sp, n_sp)
        remote(outb.at[j], back.at[j], b_send.at[0], b_recv.at[j], {"sp": j, "tp": tp}).wait_recv()

    loop(1, n_sp, wait_back)
    flat = back[...].reshape(places, cols)
    weight = ids_ref[...][:, 2:4]
    routed = weight[:, 0:1] * jnp.dot(hits[0].astype(BF16), flat, preferred_element_type=F32)
    routed = routed + weight[:, 1:2] * jnp.dot(hits[1].astype(BF16), flat, preferred_element_type=F32)
    second = depth_scale * set_ref[...].astype(F32) + routed
    stats_start(n_tp, sp, tp, lane_sums(second), lane_sums(second * second), stat, s_send, s_recv)

    def drain(o):
        for copy in x_copies(o):
            copy.wait_send()
        for k in range(1, ny):
            relay_copy(k, o).wait_send()
            y_copy(k, o).wait_send()

    loop(0, n_sp, drain)

    def drain_sp(o):
        a_copy(o).wait_send()
        b_copy(o).wait_send()

    loop(1, n_sp, drain_sp)
    for k in range(ny):
        d_copy(k).wait_send()
    one, two = stats_finish(n_tp, sp, tp, stat, s_send, s_recv, rows)
    out_ref[...] = norm(second, one, two, gf_ref[...], bf_ref[...], cols * n_tp)


def body(
    residual_in,
    query_alpha,
    pairs_alpha,
    offset_alpha,
    gain_alpha,
    query_beta,
    pairs_beta,
    offset_beta,
    gain_beta,
    project_alpha,
    project_beta,
    gain_settle,
    bias_settle,
    expert_ids,
    route_weight,
    expert_gate,
    expert_up,
    expert_down,
    gain_final,
    bias_final,
):
    n_sp = lax.axis_size("sp")
    n_tp = lax.axis_size("tp")
    nx = 2 ** ((n_sp.bit_length() - 1) // 2)
    nz = n_sp // nx
    rows, cols = residual_in.shape
    kva = pairs_alpha.shape[1]
    kvb = pairs_beta.shape[1]
    heads = 2 * kva + kvb
    heads_pad = -(-heads // 8) * 8
    kv_cols = kva * 128 + kvb * 256
    inner = kva * 128
    inner_b = kvb * 128
    vm = pl.BlockSpec(memory_space=VMEM)
    hbm = pl.BlockSpec(memory_space=pl.ANY)
    row = lambda v: v.reshape(1, -1)
    cap = -(-(3 * rows // n_sp) // 16) * 16
    places = n_sp * cap
    ny = n_tp // 2
    width, units = expert_gate.shape[1:]
    attend_scratch = [
        VMEM((n_sp, rows, kv_cols), BF16),
        VMEM((n_sp, heads_pad, rows), F32),
        VMEM((kva, 2 * rows, 128), BF16),
        VMEM((rows, inner + inner_b), F32),
        VMEM((heads * rows, 128), F32),
        VMEM(project_alpha.shape, BF16),
        VMEM(project_beta.shape, BF16),
        VMEM((n_tp, rows, cols), F32),
        VMEM((n_tp, rows, cols), F32),
        VMEM((n_tp, rows, cols), BF16),
        VMEM((n_tp, rows, cols), BF16),
        VMEM((n_tp, 2, 8, rows), F32),
        VMEM((n_tp, 2, 8, rows), F32),
        DMA((5,)),
        DMA((nz, nx)),
        DMA((n_sp,)),
        DMA((nz, nx)),
        DMA((n_sp,)),
        DMA((n_tp,)),
        DMA((n_tp,)),
        DMA((n_tp,)),
        DMA((n_tp,)),
        DMA((n_tp,)),
        DMA((n_tp,)),
    ]
    balanced = nx == 2 and kva == nz and kvb == nz
    tall = nx * rows
    plane_scratch = [
        VMEM((rows * kva, 128), BF16),
        VMEM((rows * kvb * 2, 128), BF16),
        VMEM((rows * kva, 128), F32),
        VMEM((rows * kvb * 2, 128), F32),
        VMEM((kva, rows, 128), BF16),
        VMEM((kvb, 2, rows, 128), BF16),
        VMEM((nz, 8, 128), F32),
        VMEM((n_sp, rows, 128), BF16),
        VMEM((2, n_sp, rows, 128), BF16),
        VMEM((n_sp, 8, 128), F32),
        VMEM((nz, 2 * tall, 128), BF16),
        VMEM((nz, 2 * tall, 128), BF16),
        VMEM((2, nz, tall, 128), F32),
        VMEM((nz, tall, 128), F32),
        VMEM((n_sp, rows, 128), BF16),
        VMEM((n_sp, rows, 128), BF16),
        VMEM(project_alpha.shape, BF16),
        VMEM(project_beta.shape, BF16),
        VMEM((n_tp, rows, cols), F32),
        VMEM((n_tp, rows, cols), F32),
        VMEM((n_tp, rows, cols), BF16),
        VMEM((n_tp, rows, cols), BF16),
        VMEM((n_tp, 2, 8, rows), F32),
        VMEM((n_tp, 2, 8, rows), F32),
        DMA((4,)),
        DMA((3, n_sp)),
        DMA((3, n_sp)),
        DMA((n_sp,)),
        DMA((n_sp,)),
        DMA((n_tp,)),
        DMA((n_tp,)),
        DMA((n_tp,)),
        DMA((n_tp,)),
        DMA((n_tp,)),
        DMA((n_tp,)),
    ]
    if balanced:
        attend_scratch = plane_scratch
    expert_scratch = [
        VMEM((width, units), BF16),
        VMEM((width, units), BF16),
        VMEM((units, width), BF16),
        VMEM((n_sp, cap, cols), BF16),
        VMEM((n_tp, n_sp, cap, cols), BF16),
        VMEM((places, units), F32),
        VMEM((places, units), F32),
        VMEM((places, units), BF16),
        VMEM((ny, n_sp, cap, cols), BF16),
        VMEM((ny, n_sp, cap, cols), BF16),
        VMEM((ny, n_sp, cap, cols), BF16),
        VMEM((ny, n_sp, cap, cols), BF16),
        VMEM((ny, n_sp, cap, cols), BF16),
        VMEM((n_sp, cap, cols), BF16),
        VMEM((n_sp, cap, cols), BF16),
        VMEM((n_tp, 2, 8, rows), F32),
        DMA((3,)),
        DMA((n_sp,)),
        DMA((n_sp,)),
        DMA((ny, n_sp)),
        DMA((n_tp, n_sp)),
        DMA((ny, n_sp)),
        DMA((ny,)),
        DMA((ny,)),
        DMA((ny, n_sp)),
        DMA((ny, n_sp)),
        DMA((n_sp,)),
        DMA((n_sp,)),
        DMA((n_tp,)),
        DMA((n_tp,)),
    ]
    n_attend = len(attend_scratch)
    if balanced:
        halves = pairs_beta.reshape(rows, kvb, 2, 128).transpose(0, 2, 1, 3)
        keyed = [
            pairs_alpha.reshape(rows * kva, 128),
            halves.reshape(rows * kvb * 2, 128),
            offset_alpha.T,
            offset_beta.T,
        ]
        places_in = [vm, vm]
    else:
        off = jnp.transpose(jnp.concatenate([offset_alpha, offset_beta], axis=1))
        off = jnp.pad(off, ((0, heads_pad - heads), (0, 0)))
        keyed = [pairs_alpha.reshape(rows, -1), pairs_beta.reshape(rows, -1), off]
        places_in = [hbm]
    n_in = len(keyed) + 9

    def kernel(*refs):
        attend_in = refs[:n_in]
        expert_in = refs[n_in : n_in + 6]
        out_ref, settled = refs[n_in + 6 : n_in + 8]
        own = refs[n_in + 8 :]

        def attention(early):
            attend = plane_attend if balanced else attend_kernel
            attend(early, n_sp, n_tp, nx, kva, kvb, *attend_in, settled, *own[:n_attend])

        expert_kernel(attention, balanced, n_sp, n_tp, nx, cap, settled, *expert_in, out_ref, *own[n_attend:])

    return pl.pallas_call(
        kernel,
        out_shape=jax.ShapeDtypeStruct((rows, cols), BF16),
        in_specs=[vm, vm, hbm, hbm] + places_in + [vm, vm, vm, hbm, hbm, vm, vm, vm, hbm, hbm, hbm, vm, vm],
        out_specs=vm,
        scratch_shapes=[VMEM((rows, cols), BF16)] + attend_scratch + expert_scratch,
        compiler_params=pltpu.CompilerParams(
            collective_id=0, has_side_effects=True, vmem_limit_bytes=60 * 1024 * 1024
        ),
    )(
        query_alpha,
        query_beta,
        *keyed,
        residual_in,
        row(gain_alpha),
        row(gain_beta),
        project_alpha,
        project_beta,
        row(gain_settle),
        row(bias_settle),
        jnp.concatenate([expert_ids.astype(F32), route_weight], axis=1),
        expert_gate,
        expert_up,
        expert_down,
        row(gain_final),
        row(bias_final),
    )


def solution(mesh):
    in_specs = (
        P("sp", "tp"),
        P("sp", "tp"),
        P("sp", "tp", None),
        P("sp", "tp"),
        P("tp"),
        P("sp", "tp"),
        P("sp", "tp", None),
        P("sp", "tp"),
        P("tp"),
        P("tp", None),
        P("tp", None),
        P("tp"),
        P("tp"),
        P("sp", None),
        P("sp", None),
        P("sp", None, "tp"),
        P("sp", None, "tp"),
        P("sp", "tp", None),
        P("tp"),
        P("tp"),
    )
    out_specs = P("sp", "tp")
    return jax.shard_map(body, mesh=mesh, in_specs=in_specs, out_specs=out_specs, check_vma=False)
```

```python
import functools
import jax
import jax.numpy as jnp
from jax import lax
from jax.experimental import pallas as pl
from jax.experimental.pallas import tpu as pltpu
from jax.sharding import PartitionSpec as P

depth_scale = 2.0**0.5
norm_eps = 1e-05
F32 = jnp.float32
BF16 = jnp.bfloat16
VMEM = pltpu.VMEM
DMA = pltpu.SemaphoreType.DMA


def remote(src, dst, send, recv, where):
    return pltpu.make_async_remote_copy(
        src_ref=src,
        dst_ref=dst,
        send_sem=send,
        recv_sem=recv,
        device_id=where,
        device_id_type=pl.DeviceIdType.MESH,
    )


def greet(n_sp, n_tp, sp, tp):
    barrier = pltpu.get_barrier_semaphore()
    for o in range(1, n_sp):
        pl.semaphore_signal(
            barrier,
            inc=1,
            device_id={"sp": lax.rem(sp + o, n_sp), "tp": tp},
            device_id_type=pl.DeviceIdType.MESH,
        )
    for o in range(1, n_tp):
        pl.semaphore_signal(
            barrier,
            inc=1,
            device_id={"sp": sp, "tp": lax.rem(tp + o, n_tp)},
            device_id_type=pl.DeviceIdType.MESH,
        )
    pl.semaphore_wait(barrier, n_sp + n_tp - 2)


def split(x):
    high = x.astype(BF16)
    return high, (x - high.astype(F32)).astype(BF16)


def lane_sums(x):
    ones = jnp.ones((8, x.shape[1]), BF16)
    dims = (((1,), (1,)), ((), ()))
    high, low = split(x)
    return lax.dot_general(ones, high, dims, preferred_element_type=F32) + lax.dot_general(
        ones, low, dims, preferred_element_type=F32
    )


def column(row, rows):
    return jnp.transpose(jnp.broadcast_to(row[0:1, :], (rows, rows)))[:, 0:1]


def stats_start(n_tp, sp, tp, one, two, stat, send, recv):
    stat[tp, 0] = one
    stat[tp, 1] = two
    for o in range(1, n_tp):
        remote(
            stat.at[tp], stat.at[tp], send.at[o], recv.at[tp], {"sp": sp, "tp": lax.rem(tp + o, n_tp)}
        ).start()


def stats_finish(n_tp, sp, tp, stat, send, recv, rows):
    for o in range(1, n_tp):
        peer = lax.rem(tp + o, n_tp)
        remote(stat.at[peer], stat.at[peer], send.at[o], recv.at[peer], {"sp": sp, "tp": peer}).wait_recv()
    for o in range(1, n_tp):
        peer = lax.rem(tp + o, n_tp)
        remote(stat.at[tp], stat.at[tp], send.at[o], recv.at[tp], {"sp": sp, "tp": peer}).wait_send()
    total = stat[0]
    for t in range(1, n_tp):
        total = total + stat[t]
    return column(total[0], rows), column(total[1], rows)


def norm(total, one, two, gain, bias, columns):
    mean = one / columns
    var = two / columns - mean * mean
    return ((total - mean) * lax.rsqrt(var + norm_eps) * gain + bias).astype(BF16)


def attend_kernel(
    early,
    n_sp,
    n_tp,
    nx,
    kva,
    kvb,
    qa_ref,
    qb_ref,
    kva_hbm,
    kvb_hbm,
    off_hbm,
    res_ref,
    ga_ref,
    gb_ref,
    pa_hbm,
    pb_hbm,
    gs_ref,
    bs_ref,
    out_ref,
    kvbuf,
    offbuf,
    qs,
    acc,
    rem,
    pa,
    pb,
    ya,
    yb,
    part,
    got,
    stat1,
    stat2,
    load_sem,
    kv_send,
    kv_recv,
    off_send,
    off_recv,
    part_send,
    part_recv,
    s1_send,
    s1_recv,
    s2_send,
    s2_recv,
):
    sp = lax.axis_index("sp")
    tp = lax.axis_index("tp")
    nz = n_sp // nx
    z = sp // nx
    x = lax.rem(sp, nx)
    rows = qa_ref.shape[0]
    cols = out_ref.shape[1]
    loads = (
        pltpu.make_async_copy(kva_hbm, kvbuf.at[sp, :, 0 : kva * 128], load_sem.at[0]),
        pltpu.make_async_copy(off_hbm, offbuf.at[sp], load_sem.at[1]),
        pltpu.make_async_copy(pa_hbm, pa, load_sem.at[2]),
        pltpu.make_async_copy(pb_hbm, pb, load_sem.at[3]),
        pltpu.make_async_copy(kvb_hbm, kvbuf.at[sp, :, kva * 128 :], load_sem.at[4]),
    )
    for load in loads:
        load.start()
    greet(n_sp, n_tp, sp, tp)
    lane = lax.broadcasted_iota(jnp.int32, (rows, 128), 1)
    row_i = lax.broadcasted_iota(jnp.int32, (rows, 128), 0)
    first_half = lane < 64
    for u in range(kva):
        q32 = qa_ref[:, u * 128 : (u + 1) * 128].astype(F32) * (64**-0.5)
        qs[u, 0:rows] = jnp.where(first_half, q32, 0.0).astype(BF16)
        qs[u, rows : 2 * rows] = jnp.where(first_half, pltpu.roll(q32, 64, 1), 0.0).astype(BF16)
    acc[...] = jnp.zeros_like(acc)
    rem[...] = jnp.zeros_like(rem)
    tri_r = lax.broadcasted_iota(jnp.int32, (256, 256), 0) % 128
    tri_c = lax.broadcasted_iota(jnp.int32, (256, 256), 1)
    tri = jnp.where((tri_r > tri_c) | (tri_c >= 128), 1.0, 0.0).astype(BF16)

    def block(j):
        gap = (sp - j) * rows
        valid1 = lane < row_i + gap
        valid2 = jnp.concatenate([valid1.astype(F32)] * 2, axis=0) > 0.5

        def unit(query, key, value, offset, scale, valid, left):
            s = lax.dot_general(query, key, (((1,), (1,)), ((), ())), preferred_element_type=F32)
            s = (s if scale is None else s * scale) + offset
            soft = jnp.maximum(s, 0.0) + jnp.log(1.0 + jnp.exp(-jnp.abs(s)))
            used = jnp.where(valid, soft, 0.0)
            high, low = split(used)
            sums = jnp.dot(jnp.concatenate([high, low], axis=1), tri, preferred_element_type=F32)
            w = jnp.where(valid, jnp.exp(s - soft - sums[:, :128] + left), 0.0).astype(BF16)
            return jnp.dot(w, value, preferred_element_type=F32), sums[:, 128:]

        for u in range(kva):
            pair = kvbuf[j, :, u * 128 : (u + 1) * 128]
            offset = jnp.concatenate(
                [
                    jnp.broadcast_to(offbuf[j, 2 * u : 2 * u + 1, :], (rows, 128)),
                    jnp.broadcast_to(offbuf[j, 2 * u + 1 : 2 * u + 2, :], (rows, 128)),
                ],
                axis=0,
            )
            left = rem[2 * u * rows : (2 * u + 2) * rows]
            o, total = unit(qs[u], pair, pair, offset, None, valid2, left)
            rem[2 * u * rows : (2 * u + 2) * rows] = left - total
            acc[:, u * 128 : (u + 1) * 128] += jnp.where(
                first_half, pltpu.roll(o[:rows], 64, 1), o[rows:]
            )
        for u in range(kvb):
            base = kva * 128 + u * 256
            head = 2 * kva + u
            key = kvbuf[j, :, base : base + 128]
            value = kvbuf[j, :, base + 128 : base + 256]
            offset = offbuf[j, head : head + 1, :]
            left = rem[head * rows : (head + 1) * rows]
            query = qb_ref[:, u * 128 : (u + 1) * 128]
            o, total = unit(query, key, value, offset, 128**-0.5, valid1, left)
            rem[head * rows : (head + 1) * rows] = left - total
            c = (kva + u) * 128
            acc[:, c : c + 128] += o

    def sends(s):
        j0 = (z - s) * nx + x
        plan = [(z + 1 < nz, jnp.minimum(z + 1, nz - 1) * nx + x)]
        for d in range(1, nx):
            xo = lax.rem(x + d, nx)
            plan.append(((s > 0) | (x < xo), z * nx + xo))
        made = []
        for k, (cond, dest) in enumerate(plan):
            where = {"sp": dest, "tp": tp}
            made.append(
                (
                    cond,
                    remote(kvbuf.at[j0], kvbuf.at[j0], kv_send.at[s, k], kv_recv.at[j0], where),
                    remote(offbuf.at[j0], offbuf.at[j0], off_send.at[s, k], off_recv.at[j0], where),
                )
            )
        return made

    def wait_block(j):
        where = {"sp": sp, "tp": tp}
        remote(kvbuf.at[j], kvbuf.at[j], kv_send.at[0, 0], kv_recv.at[j], where).wait_recv()
        remote(offbuf.at[j], offbuf.at[j], off_send.at[0, 0], off_recv.at[j], where).wait_recv()

    loads[0].wait()
    loads[1].wait()
    loads[4].wait()

    def forward(s):
        @pl.when(s > 0)
        def _():
            wait_block((z - s) * nx + x)

        for cond, kv_copy, off_copy in sends(s):

            @pl.when(cond)
            def _(kv_copy=kv_copy, off_copy=off_copy):
                off_copy.start()
                kv_copy.start()

    forward(0)

    def level(s, carry):
        src = z - s

        @pl.when(s < z)
        def _():
            forward(s + 1)

        def across(i, inner):
            xo = nx - 1 - i

            @pl.when((s > 0) | (xo <= x))
            def _():
                @pl.when(xo != x)
                def _():
                    wait_block(src * nx + xo)

                block(src * nx + xo)

            return inner

        return lax.fori_loop(0, nx, across, carry)

    lax.fori_loop(0, z + 1, level, 0)
    early()

    wide = kva * 128
    aa = acc[:, :wide]
    ab = acc[:, wide:]
    stats_start(n_tp, sp, tp, lane_sums(aa * aa), lane_sums(ab * ab), stat1, s1_send, s1_recv)
    loads[2].wait()
    loads[3].wait()
    na = (aa * ga_ref[...]).astype(BF16)
    nb = (ab * gb_ref[...]).astype(BF16)
    for t in range(n_tp):
        ya[t] = jnp.dot(na, pa[:, t * cols : (t + 1) * cols], preferred_element_type=F32)
        yb[t] = jnp.dot(nb, pb[:, t * cols : (t + 1) * cols], preferred_element_type=F32)
    sq_a, sq_b = stats_finish(n_tp, sp, tp, stat1, s1_send, s1_recv, rows)
    scale_a = lax.rsqrt(sq_a / (wide * n_tp) + norm_eps)
    scale_b = lax.rsqrt(sq_b / (kvb * 128 * n_tp) + norm_eps)

    def part_copy(o):
        peer = lax.rem(tp + o, n_tp)
        return remote(
            part.at[peer], got.at[tp], part_send.at[o], part_recv.at[tp], {"sp": sp, "tp": peer}
        )

    for o in range(1, n_tp):
        peer = lax.rem(tp + o, n_tp)
        part[peer] = (ya[peer] * scale_a + yb[peer] * scale_b).astype(BF16)
        part_copy(o).start()
    total = (ya[tp] * scale_a + yb[tp] * scale_b).astype(BF16).astype(F32)
    for o in range(1, n_tp):
        peer = lax.rem(tp + o, n_tp)
        remote(
            part.at[peer], got.at[peer], part_send.at[o], part_recv.at[peer], {"sp": sp, "tp": peer}
        ).wait_recv()
        total = total + got[peer].astype(F32)
    mixed = total.astype(BF16).astype(F32)
    first = depth_scale * res_ref[...].astype(F32) + mixed
    stats_start(n_tp, sp, tp, lane_sums(first), lane_sums(first * first), stat2, s2_send, s2_recv)
    for o in range(1, n_tp):
        part_copy(o).wait_send()

    def drain(s, carry):
        for cond, kv_copy, off_copy in sends(s):

            @pl.when(cond)
            def _(kv_copy=kv_copy, off_copy=off_copy):
                off_copy.wait_send()
                kv_copy.wait_send()

        return carry

    lax.fori_loop(0, z + 1, drain, 0)
    one, two = stats_finish(n_tp, sp, tp, stat2, s2_send, s2_recv, rows)
    out_ref[...] = norm(first, one, two, gs_ref[...], bs_ref[...], cols * n_tp)


def plane_attend(
    early,
    between,
    n_sp,
    n_tp,
    nx,
    kva,
    kvb,
    qa_ref,
    qb_ref,
    pairs_a_hbm,
    pairs_b_hbm,
    offa_ref,
    offb_ref,
    res_ref,
    ga_ref,
    gb_ref,
    pa_hbm,
    pb_hbm,
    gs_ref,
    bs_ref,
    out_ref,
    raw_a,
    raw_b,
    wide_a,
    wide_b,
    own_a,
    own_b,
    own_off,
    qin,
    kin,
    oin,
    keys2,
    values2,
    left,
    acc,
    obuf,
    ain,
    pa,
    pb,
    ya,
    yb,
    part,
    got,
    stat1,
    stat2,
    load_sem,
    in_send,
    in_recv,
    o_send,
    o_recv,
    part_send,
    part_recv,
    s1_send,
    s1_recv,
    s2_send,
    s2_recv,
):
    sp = lax.axis_index("sp")
    tp = lax.axis_index("tp")
    nz = n_sp // nx
    z = sp // nx
    x = lax.rem(sp, nx)
    rows = qa_ref.shape[0]
    cols = out_ref.shape[1]
    tall = nx * rows

    def is_alpha(zz, xx):
        return lax.rem(zz + xx, 2) == 0

    loads = (
        pltpu.make_async_copy(pairs_a_hbm, raw_a, load_sem.at[0]),
        pltpu.make_async_copy(pairs_b_hbm, raw_b, load_sem.at[1]),
        pltpu.make_async_copy(pa_hbm, pa, load_sem.at[2]),
        pltpu.make_async_copy(pb_hbm, pb, load_sem.at[3]),
    )
    loads[0].start()
    loads[1].start()
    for u in range(nz):
        own_off[u, 0:2] = offa_ref[2 * u : 2 * u + 2]
        own_off[u, 2:3] = offb_ref[u : u + 1]
    greet(n_sp, n_tp, sp, tp)
    loads[0].wait()
    wide_a[...] = raw_a[...].astype(F32)
    for u in range(kva):
        own_a[u] = wide_a[pl.ds(u, rows, stride=kva), :].astype(BF16)
    loads[1].wait()
    wide_b[...] = raw_b[...].astype(F32)
    for u in range(kvb):
        for h in range(2):
            own_b[u, h] = wide_b[pl.ds(h * kvb + u, rows, stride=2 * kvb), :].astype(BF16)
    loads[2].start()
    loads[3].start()

    def in_copies(zz, xx, alpha):
        dest = zz * nx + xx
        where = {"sp": dest, "tp": tp}
        at = pl.ds(pl.multiple_of(zz * 128, 128), 128)
        q_ref = qa_ref if alpha else qb_ref
        kv = (own_a.at[zz], kin.at[0, sp]) if alpha else (own_b.at[zz], kin.at[:, sp])
        return (
            remote(own_off.at[zz], oin.at[sp], in_send.at[0, dest], in_recv.at[0, sp], where),
            remote(q_ref.at[:, at], qin.at[sp], in_send.at[1, dest], in_recv.at[1, sp], where),
            remote(*kv, in_send.at[2, dest], in_recv.at[2, sp], where),
        )

    def each_dest(act):
        def hop(t, carry):
            away = (t + 1) // 2
            zz = z + away * (2 * lax.rem(t, 2) - 1)
            for xx in range(nx):
                there = (zz >= 0) & (zz < nz) & ((zz != z) | (xx != x))
                for alpha in (True, False):

                    @pl.when(there & (is_alpha(zz, xx) == alpha))
                    def _(xx=xx, alpha=alpha):
                        for copy in in_copies(zz, xx, alpha):
                            act(copy)

            return carry

        lax.fori_loop(0, 2 * nz - 1, hop, 0)

    each_dest(lambda copy: copy.start())
    early()

    def o_copy(d):
        return remote(obuf.at[d], ain.at[sp], o_send.at[d], o_recv.at[sp], {"sp": d, "tp": tp})

    lane_t = lax.broadcasted_iota(jnp.int32, (tall, tall), 1)
    row_t = lax.broadcasted_iota(jnp.int32, (tall, tall), 0)
    lane = lax.broadcasted_iota(jnp.int32, (tall, 128), 1)
    tri = jnp.where(row_t > lane_t, 1.0, 0.0).astype(BF16)

    def attend(alpha):
        heads = 2 if alpha else 1
        scale = 64**-0.5 if alpha else 128**-0.5
        at = pl.ds(pl.multiple_of(z * 128, 128), 128)
        oin[sp] = own_off[z]
        if alpha:
            qin[sp] = qa_ref[:, at]
            kin[0, sp] = own_a[z]
        else:
            qin[sp] = qb_ref[:, at]
            kin[:, sp] = own_b[z]

        def arrive(p):
            for xx in range(nx):
                s = p * nx + xx

                @pl.when(s != sp)
                def _(s=s):
                    where = {"sp": sp, "tp": tp}
                    kv = kin.at[0, s] if alpha else kin.at[:, s]
                    remote(oin.at[s], oin.at[s], in_send.at[0, 0], in_recv.at[0, s], where).wait_recv()
                    remote(qin.at[s], qin.at[s], in_send.at[1, 0], in_recv.at[1, s], where).wait_recv()
                    remote(kv, kv, in_send.at[2, 0], in_recv.at[2, s], where).wait_recv()

            if alpha:
                pair = kin[0, pl.ds(p * nx, nx)].reshape(tall, 128).astype(F32)
                turned = pltpu.roll(pair, 64, 1)
                keys2[p, 0:tall] = jnp.where(lane < 64, pair, 0.0).astype(BF16)
                keys2[p, tall:] = jnp.where(lane < 64, 0.0, turned).astype(BF16)
                values2[p, 0:tall] = jnp.where(lane < 64, turned, 0.0).astype(BF16)
                values2[p, tall:] = jnp.where(lane < 64, 0.0, pair).astype(BF16)

        def step(r, c, diag):
            query = qin[pl.ds(r * nx, nx)].reshape(tall, 128)
            if alpha:
                key, value = keys2[c], values2[c]
            else:
                key = kin[0, pl.ds(c * nx, nx)].reshape(tall, 128)
                value = kin[1, pl.ds(c * nx, nx)].reshape(tall, 128)
            scores = lax.dot_general(query, key, (((1,), (1,)), ((), ())), preferred_element_type=F32)
            valid = lane_t < row_t
            ws = []
            for h in range(heads):
                row = h if alpha else 2
                offset = jnp.concatenate([oin[c * nx + i, row : row + 1, :] for i in range(nx)], axis=1)
                s = scores[:, h * tall : (h + 1) * tall] * scale + offset
                soft = jnp.maximum(s, 0.0) + jnp.log(1.0 + jnp.exp(-jnp.abs(s)))
                used = jnp.where(valid, soft, 0.0) if diag else soft
                sums = jnp.dot(used.astype(BF16), tri, preferred_element_type=F32)
                total = jnp.broadcast_to(sums[:, 0:1] + used[:, 0:1], (tall, 128))
                e = s - soft - sums
                if diag:
                    w = jnp.where(valid, jnp.exp(e), 0.0)
                    left[h, r] = -total
                else:
                    before = left[h, r]
                    w = jnp.exp(e + jnp.concatenate([before] * nx, axis=1))
                    left[h, r] = before - total
                ws.append(w.astype(BF16))
            w = ws[0] if heads == 1 else jnp.concatenate(ws, axis=1)
            o = jnp.dot(w, value, preferred_element_type=F32)
            o = o if diag else acc[r] + o
            acc[r] = o

            @pl.when(c == 0)
            def _():
                obuf[pl.ds(r * nx, nx)] = o.astype(BF16).reshape(nx, rows, 128)
                for xx in range(nx):
                    d = r * nx + xx

                    @pl.when(d != sp)
                    def _(d=d):
                        o_copy(d).start()

                    @pl.when(d == sp)
                    def _(d=d):
                        ain[sp] = obuf[d]

        def phase(k, span):
            low, high = span
            lower_half = z < nz // 2
            up = jnp.where(lower_half, low == 0, high < nz - 1).astype(jnp.int32)
            first = (k == 0).astype(jnp.int32)
            p = first * z + (1 - first) * (up * (high + 1) + (1 - up) * (low - 1))
            arrive(p)
            step(p, p, True)
            count = (1 - first) * (high - low + 1)

            def more(t, carry):
                step(p + t * (1 - up), p - t * up, False)
                return carry

            lax.fori_loop(1, count + 1, more, 0)
            return jnp.minimum(low, p), jnp.maximum(high, p)

        lax.fori_loop(0, nz, phase, (z, z))

    for alpha in (True, False):

        @pl.when(is_alpha(z, x) == alpha)
        def _(alpha=alpha):
            attend(alpha)

    between()

    def o_wait(j, carry):
        @pl.when(j != sp)
        def _():
            remote(obuf.at[j], ain.at[j], o_send.at[0], o_recv.at[j], {"sp": sp, "tp": tp}).wait_recv()

        return carry

    lax.fori_loop(0, n_sp, o_wait, 0)
    wide = kva * 128
    aa = jnp.concatenate([ain[k * nx + k % 2] for k in range(nz)], axis=1).astype(F32)
    ab = jnp.concatenate([ain[k * nx + 1 - k % 2] for k in range(nz)], axis=1).astype(F32)
    stats_start(n_tp, sp, tp, lane_sums(aa * aa), lane_sums(ab * ab), stat1, s1_send, s1_recv)
    loads[2].wait()
    loads[3].wait()
    na = (aa * ga_ref[...]).astype(BF16)
    nb = (ab * gb_ref[...]).astype(BF16)
    for t in range(n_tp):
        ya[t] = jnp.dot(na, pa[:, t * cols : (t + 1) * cols], preferred_element_type=F32)
        yb[t] = jnp.dot(nb, pb[:, t * cols : (t + 1) * cols], preferred_element_type=F32)
    sq_a, sq_b = stats_finish(n_tp, sp, tp, stat1, s1_send, s1_recv, rows)
    scale_a = lax.rsqrt(sq_a / (wide * n_tp) + norm_eps)
    scale_b = lax.rsqrt(sq_b / (kvb * 128 * n_tp) + norm_eps)

    def part_copy(o):
        peer = lax.rem(tp + o, n_tp)
        return remote(
            part.at[peer], got.at[tp], part_send.at[o], part_recv.at[tp], {"sp": sp, "tp": peer}
        )

    for o in range(1, n_tp):
        peer = lax.rem(tp + o, n_tp)
        part[peer] = (ya[peer] * scale_a + yb[peer] * scale_b).astype(BF16)
        part_copy(o).start()
    total = (ya[tp] * scale_a + yb[tp] * scale_b).astype(BF16).astype(F32)
    for o in range(1, n_tp):
        peer = lax.rem(tp + o, n_tp)
        remote(
            part.at[peer], got.at[peer], part_send.at[o], part_recv.at[peer], {"sp": sp, "tp": peer}
        ).wait_recv()
        total = total + got[peer].astype(F32)
    mixed = total.astype(BF16).astype(F32)
    first = depth_scale * res_ref[...].astype(F32) + mixed
    stats_start(n_tp, sp, tp, lane_sums(first), lane_sums(first * first), stat2, s2_send, s2_recv)
    for o in range(1, n_tp):
        part_copy(o).wait_send()

    each_dest(lambda copy: copy.wait_send())

    def o_drain(j, carry):
        @pl.when(j != sp)
        def _():
            o_copy(j).wait_send()

        return carry

    lax.fori_loop(0, n_sp, o_drain, 0)
    one, two = stats_finish(n_tp, sp, tp, stat2, s2_send, s2_recv, rows)
    out_ref[...] = norm(first, one, two, gs_ref[...], bs_ref[...], cols * n_tp)


def expert_kernel(
    attention,
    n_sp,
    n_tp,
    nx,
    cap,
    set_ref,
    ids_ref,
    wg_hbm,
    wu_hbm,
    wd_hbm,
    gf_ref,
    bf_ref,
    out_ref,
    wg,
    wu,
    wd,
    sendbuf,
    xbuf,
    gate,
    up,
    hid,
    away,
    arrived,
    home,
    pre,
    peers,
    outb,
    back,
    stat,
    load_sem,
    a_send,
    a_recv,
    x_send,
    x_recv,
    relay_send,
    d_send,
    d_recv,
    y_send,
    y_recv,
    b_send,
    b_recv,
    s_send,
    s_recv,
):
    sp = lax.axis_index("sp")
    tp = lax.axis_index("tp")
    rows, cols = set_ref.shape
    places = n_sp * cap
    ny = n_tp // 2
    y = tp // 2
    core = lax.rem(tp, 2)
    mate = y * 2 + 1 - core
    loads = (
        pltpu.make_async_copy(wg_hbm.at[0], wg, load_sem.at[0]),
        pltpu.make_async_copy(wu_hbm.at[0], wu, load_sem.at[1]),
        pltpu.make_async_copy(wd_hbm.at[0], wd, load_sem.at[2]),
    )

    def loop(low, high, fn):
        def step(i, carry):
            fn(i)
            return carry

        lax.fori_loop(low, high, step, 0)

    def x_copies(j):
        made = []
        for k in range(ny):
            dest = mate if k == 0 else lax.rem(y + k, ny) * 2 + core
            made.append(
                remote(
                    xbuf.at[tp, j], xbuf.at[tp, j], x_send.at[k, j], x_recv.at[tp, j], {"sp": sp, "tp": dest}
                )
            )
        return made

    def spread_out(j):
        @pl.when(j != sp)
        def _():
            remote(
                sendbuf.at[j], xbuf.at[tp, j], a_send.at[0], a_recv.at[j], {"sp": sp, "tp": tp}
            ).wait_recv()

        for copy in x_copies(j):
            copy.start()

    ahead = jnp.maximum(sp // nx - 1, 0) * nx

    for load in loads:
        load.start()
    attention(lambda: loop(0, ahead, spread_out))
    ids = ids_ref[...][:, 0:2]
    expert = lax.broadcasted_iota(jnp.int32, (rows, 128), 1).astype(F32)
    hot = [jnp.where(ids[:, k : k + 1] == expert, 1.0, 0.0) for k in range(2)]
    r = lax.broadcasted_iota(jnp.int32, (rows, rows), 0)
    c = lax.broadcasted_iota(jnp.int32, (rows, rows), 1)
    lower = jnp.where(c < r, 1.0, 0.0).astype(BF16)
    before = jnp.dot(lower, (hot[0] + hot[1]).astype(BF16), preferred_element_type=F32)
    seat = lax.broadcasted_iota(jnp.int32, (rows, places), 1).astype(F32)
    hits = []
    for k in range(2):
        slot = jnp.sum(before * hot[k], axis=1, keepdims=True)
        place = ids[:, k : k + 1] * cap + slot
        hits.append(jnp.where(place == seat, 1.0, 0.0))
    spread = jnp.transpose(hits[0] + hits[1]).astype(BF16)
    sent = jnp.dot(spread, set_ref[...], preferred_element_type=F32).astype(BF16)
    sendbuf[...] = sent.reshape(n_sp, cap, cols)

    def at_sp(o):
        return lax.rem(sp + o, n_sp)

    def a_copy(o):
        dest = at_sp(o)
        return remote(
            sendbuf.at[dest], xbuf.at[tp, sp], a_send.at[o], a_recv.at[sp], {"sp": dest, "tp": tp}
        )

    loop(1, n_sp, lambda o: a_copy(o).start())
    xbuf[tp, sp] = sendbuf[sp]

    def x_wait(t, j):
        remote(xbuf.at[t, j], xbuf.at[t, j], x_send.at[0, 0], x_recv.at[t, j], {"sp": sp, "tp": t}).wait_recv()

    loop(ahead, n_sp, spread_out)

    def relay_copy(k, o):
        t = lax.rem(y + k, ny) * 2 + core
        j = o
        return remote(
            xbuf.at[t, j], xbuf.at[t, j], relay_send.at[k, o], x_recv.at[t, j], {"sp": sp, "tp": mate}
        )

    def gather_dot(t, fresh):
        xs = xbuf[t].reshape(places, cols)
        at = pl.ds(pl.multiple_of(t * cols, 128), cols)
        g = jnp.dot(xs, wg[at, :], preferred_element_type=F32)
        u = jnp.dot(xs, wu[at, :], preferred_element_type=F32)
        if fresh:
            gate[...] = g
            up[...] = u
        else:
            gate[...] += g
            up[...] += u

    loads[0].wait()
    loads[1].wait()
    gather_dot(tp, True)

    def arrive_mate(o):
        x_wait(mate, o)

    loop(0, n_sp, arrive_mate)
    gather_dot(mate, False)

    def from_y(k):
        t = lax.rem(y + k, ny) * 2 + core
        other = lax.rem(y + k, ny) * 2 + 1 - core

        def pass_on(o):
            x_wait(t, o)
            relay_copy(k, o).start()

        loop(0, n_sp, pass_on)
        gather_dot(t, False)

        def arrive(o):
            x_wait(other, o)

        loop(0, n_sp, arrive)
        gather_dot(other, False)

    loop(1, ny, from_y)
    value = gate[...]
    hid[...] = (value / (1.0 + jnp.exp(-value)) * up[...]).astype(BF16)
    loads[2].wait()

    def down(t):
        at = pl.ds(pl.multiple_of(t * cols, 128), cols)
        result = jnp.dot(hid[...], wd[:, at], preferred_element_type=F32)
        return result.astype(BF16).reshape(n_sp, cap, cols)

    def d_copy(k):
        return remote(away.at[k], arrived.at[k], d_send.at[k], d_recv.at[k], {"sp": sp, "tp": mate})

    def down_away(i):
        k = lax.rem(i + 1, ny)
        away[k] = down(lax.rem(y + k, ny) * 2 + 1 - core)
        d_copy(k).start()

    loop(0, ny, down_away)

    def down_home(i):
        k = lax.rem(i + 1, ny)
        home[k] = down(lax.rem(y + k, ny) * 2 + core)

    loop(0, ny, down_home)

    def y_copy(k, o):
        j = at_sp(o)
        return remote(
            pre.at[k, j],
            peers.at[k, j],
            y_send.at[k, o],
            y_recv.at[k, j],
            {"sp": sp, "tp": lax.rem(y + k, ny) * 2 + core},
        )

    for i in range(ny):
        k = (i + 1) % ny
        d_copy(k).wait_recv()
        if k:

            def to_y(o, k=k):
                j = at_sp(o)
                pre[k, j] = (home[k, j].astype(F32) + arrived[k, j].astype(F32)).astype(BF16)
                y_copy(k, o).start()

            loop(1, n_sp, to_y)
            to_y(0)

    def b_copy(o):
        dest = at_sp(o)
        return remote(outb.at[dest], back.at[sp], b_send.at[o], b_recv.at[sp], {"sp": dest, "tp": tp})

    def settle(o):
        j = at_sp(o)
        total = home[0, j].astype(F32) + arrived[0, j].astype(F32)
        for k in range(1, ny):
            remote(
                pre.at[k, j], peers.at[k, j], y_send.at[k, 0], y_recv.at[k, j], {"sp": sp, "tp": mate}
            ).wait_recv()
            total = total + peers[k, j].astype(F32)
        return total.astype(BF16)

    def give_back(o):
        outb[at_sp(o)] = settle(o)
        b_copy(o).start()

    loop(1, n_sp, give_back)
    back[sp] = settle(0)

    def wait_back(o):
        j = lax.rem(sp - o + n_sp, n_sp)
        remote(outb.at[j], back.at[j], b_send.at[0], b_recv.at[j], {"sp": j, "tp": tp}).wait_recv()

    loop(1, n_sp, wait_back)
    flat = back[...].reshape(places, cols)
    weight = ids_ref[...][:, 2:4]
    routed = weight[:, 0:1] * jnp.dot(hits[0].astype(BF16), flat, preferred_element_type=F32)
    routed = routed + weight[:, 1:2] * jnp.dot(hits[1].astype(BF16), flat, preferred_element_type=F32)
    second = depth_scale * set_ref[...].astype(F32) + routed
    stats_start(n_tp, sp, tp, lane_sums(second), lane_sums(second * second), stat, s_send, s_recv)

    def drain(o):
        for copy in x_copies(o):
            copy.wait_send()
        for k in range(1, ny):
            relay_copy(k, o).wait_send()
            y_copy(k, o).wait_send()

    loop(0, n_sp, drain)

    def drain_sp(o):
        a_copy(o).wait_send()
        b_copy(o).wait_send()

    loop(1, n_sp, drain_sp)
    for k in range(ny):
        d_copy(k).wait_send()
    one, two = stats_finish(n_tp, sp, tp, stat, s_send, s_recv, rows)
    out_ref[...] = norm(second, one, two, gf_ref[...], bf_ref[...], cols * n_tp)


def plane_expert(
    attention,
    n_sp,
    n_tp,
    nx,
    cap,
    set_ref,
    ids_ref,
    weight_ref,
    wg_hbm,
    wu_hbm,
    wd_hbm,
    gf_ref,
    bf_ref,
    out_ref,
    wg,
    wu,
    wd,
    hits,
    wpack,
    wrecv,
    wcol,
    packed,
    xbuf,
    gate,
    up,
    hid,
    away,
    arrived,
    home,
    mid,
    midx,
    midy,
    gotd,
    gotx,
    goty,
    outb,
    back,
    stat,
    load_sem,
    w_send,
    w_recv,
    a_send,
    a_recv,
    x_send,
    x_recv,
    d_send,
    d_recv,
    m_send,
    m_recv,
    b_send,
    b_recv,
    s_send,
    s_recv,
):
    sp = lax.axis_index("sp")
    tp = lax.axis_index("tp")
    rows, cols = set_ref.shape
    nz = n_sp // nx
    z = sp // nx
    x = lax.rem(sp, nx)
    core = lax.rem(tp, 2)
    y = tp // 2
    mate = y * 2 + 1 - core
    far = (1 - y) * 2 + core
    far_mate = (1 - y) * 2 + 1 - core
    to_mate = {"sp": sp, "tp": mate}
    to_x = {"sp": z * nx + 1 - x, "tp": tp}
    to_y = {"sp": sp, "tp": far}
    table = [sorted(range(nz), key=lambda g: (abs(g - a), (g - a) * (1 if a < nz // 2 else -1))) for a in range(nz)]

    def near(i):
        pick = table[0][i]
        for a in range(1, nz):
            pick = jnp.where(z == a, table[a][i], pick)
        return pick

    loads = (
        pltpu.make_async_copy(wg_hbm.at[0], wg, load_sem.at[0]),
        pltpu.make_async_copy(wu_hbm.at[0], wu, load_sem.at[1]),
        pltpu.make_async_copy(wd_hbm.at[0], wd, load_sem.at[2]),
    )

    def w_copy(d):
        return remote(wpack.at[d // nx], wrecv.at[sp], w_send.at[d], w_recv.at[sp], {"sp": d, "tp": tp})

    def others(fn):
        def one(d, carry):
            @pl.when(d != sp)
            def _():
                fn(d)

            return carry

        lax.fori_loop(0, n_sp, one, 0)

    def early():
        for load in loads:
            load.start()
        ids = [ids_ref[k : k + 1, :] for k in range(2)]
        r = lax.broadcasted_iota(jnp.int32, (rows, rows), 0)
        c = lax.broadcasted_iota(jnp.int32, (rows, rows), 1)
        upper = jnp.where(r < c, 1.0, 0.0).astype(BF16)
        group = lax.broadcasted_iota(jnp.int32, (8, rows), 0) * nx
        hot = jnp.where((ids[0] >= group) & (ids[0] < group + nx), 1.0, 0.0)
        before = jnp.dot(hot.astype(BF16), upper, preferred_element_type=F32)
        seat = lax.broadcasted_iota(jnp.int32, (cap, rows), 0).astype(F32)
        for g in range(nz):
            match = jnp.where(seat == before[g : g + 1], hot[g : g + 1], 0.0).astype(BF16)
            hits[g * cap : (g + 1) * cap] = match
            share = [
                jnp.where(ids[0] == g * nx + e, weight_ref[0:1, :], 0.0)
                + jnp.where(ids[1] == g * nx + e, weight_ref[1:2, :], 0.0)
                for e in range(nx)
            ]
            line = lax.broadcasted_iota(jnp.int32, (8, rows), 0)
            both = jnp.where(line == 0, share[0], jnp.where(line == 1, share[1], 0.0))
            high, low = split(both)
            dims = (((1,), (1,)), ((), ()))
            wpack[g] = jnp.zeros((8, 128), F32)
            wpack[g, :, 0:cap] = lax.dot_general(high, match, dims, preferred_element_type=F32) + lax.dot_general(
                low, match, dims, preferred_element_type=F32
            )
        others(lambda d: w_copy(d).start())
        wrecv[sp] = wpack[z]

    def between():
        def spread(j, carry):
            @pl.when(j != sp)
            def _():
                remote(wrecv.at[j], wrecv.at[j], w_send.at[0], w_recv.at[j], {"sp": sp, "tp": tp}).wait_recv()

            wide = jnp.transpose(jnp.broadcast_to(wrecv[j, pl.ds(x, 1), :], (128, 128)))
            wcol[lax.rem(j, nx), j // nx] = wide[0:cap]
            return carry

        lax.fori_loop(0, n_sp, spread, 0)

    attention(early, between)

    sent = jnp.dot(hits[...], set_ref[...], preferred_element_type=F32).astype(BF16)
    packed[...] = sent.reshape(nz, cap, cols)

    def a_copy(i):
        g = near(i)
        return remote(packed.at[g], xbuf.at[tp, x, z], a_send.at[i], a_recv.at[z], {"sp": g * nx + x, "tp": tp})

    for i in range(1, nz):
        a_copy(i).start()
    xbuf[tp, x, z] = packed[z]

    def x_copy(kind, t, xs, g, where):
        block = xbuf.at[t, xs, g]
        return remote(block, block, x_send.at[kind, g], x_recv.at[t, xs, g], where)

    def x_wait(t, xs, g):
        block = xbuf.at[t, xs, g]
        remote(block, block, x_send.at[0, 0], x_recv.at[t, xs, g], to_mate).wait_recv()

    def when_x_first(g, fn):
        pl.when(lax.rem(g, 2) == 0)(fn)

    def when_y_first(g, fn):
        pl.when(lax.rem(g, 2) == 1)(fn)

    def own_out(i):
        g = near(i)
        if i:
            remote(packed.at[g], xbuf.at[tp, x, g], a_send.at[0], a_recv.at[g], to_mate).wait_recv()
        x_copy(1, tp, x, g, to_x).start()
        x_copy(2, tp, x, g, to_y).start()
        x_copy(0, tp, x, g, to_mate).start()

    def pass_on(i):
        g = near(i)
        x_wait(tp, 1 - x, g)
        when_x_first(g, lambda: x_copy(4, tp, 1 - x, g, to_y).start())
        x_copy(3, tp, 1 - x, g, to_mate).start()
        x_wait(far, x, g)
        when_y_first(g, lambda: x_copy(6, far, x, g, to_x).start())
        x_copy(5, far, x, g, to_mate).start()

    def pass_diag(i):
        g = near(i)
        x_wait(far, 1 - x, g)
        x_copy(7, far, 1 - x, g, to_mate).start()

    def piece(t, xs, fresh):
        block = xbuf[t, xs].reshape(nz * cap, cols)
        at = pl.ds(pl.multiple_of(t * cols, 128), cols)
        g = jnp.dot(block, wg[at, :], preferred_element_type=F32)
        u = jnp.dot(block, wu[at, :], preferred_element_type=F32)
        if fresh:
            gate[xs] = g
            up[xs] = u
        else:
            gate[xs] += g
            up[xs] += u

    def all_in(t, xs):
        def one(g, carry):
            x_wait(t, xs, g)
            return carry

        lax.fori_loop(0, nz, one, 0)

    for i in range(nz + 2):
        if i < nz:
            own_out(i)
        if 1 <= i <= nz:
            pass_on(i - 1)
        if i >= 2:
            pass_diag(i - 2)
        if i == nz - 1:
            loads[0].wait()
            loads[1].wait()
            piece(tp, x, True)
        if i == nz:
            all_in(mate, x)
            piece(mate, x, False)
            piece(tp, 1 - x, True)
    piece(far, x, False)
    all_in(far_mate, x)
    piece(far_mate, x, False)
    all_in(mate, 1 - x)
    piece(mate, 1 - x, False)
    piece(far, 1 - x, False)
    all_in(far_mate, 1 - x)
    piece(far_mate, 1 - x, False)
    for xs in range(nx):
        value = gate[xs]
        weight = jnp.concatenate([wcol[xs].reshape(nz * cap, 128)] * (value.shape[1] // 128), axis=1)
        hid[xs * nz * cap : (xs + 1) * nz * cap] = (value / (1.0 + jnp.exp(-value)) * up[xs] * weight).astype(BF16)
    loads[2].wait()

    def down(t):
        at = pl.ds(pl.multiple_of(t * cols, 128), cols)
        result = jnp.dot(hid[...], wd[:, at], preferred_element_type=F32)
        return result.astype(BF16).reshape(nx, nz, cap, cols)

    def d_copy(k, xs):
        return remote(away.at[k, xs], arrived.at[k, xs], d_send.at[k, xs], d_recv.at[k, xs], to_mate)

    away[1] = down(far_mate)
    d_copy(1, 1 - x).start()
    d_copy(1, x).start()
    away[0] = down(mate)
    d_copy(0, 1 - x).start()
    d_copy(0, x).start()
    home[1] = down(far)

    def pair(k, xs, g):
        return home[k, xs, g].astype(F32) + arrived[k, xs, g].astype(F32)

    def m_copy(kind, src, dst, g, where):
        return remote(src.at[g], dst.at[g], m_send.at[kind, g], m_recv.at[kind, g], where)

    def diag_copy(g, where):
        return m_copy(0, mid, gotd, g, where)

    def x_send_copy(g):
        return m_copy(1, midx, gotx, g, to_x)

    def y_send_copy(g):
        return m_copy(2, midy, goty, g, to_y)

    order = range(nz - 1, -1, -1)
    d_copy(1, 1 - x).wait_recv()
    for i in order:
        g = near(i)
        mid[g] = pair(1, 1 - x, g).astype(BF16)
        when_x_first(g, lambda g=g: diag_copy(g, to_x).start())
        when_y_first(g, lambda g=g: diag_copy(g, to_y).start())
    home[0] = down(tp)
    d_copy(1, x).wait_recv()
    d_copy(0, 1 - x).wait_recv()
    for i in order:
        g = near(i)

        def plain_x(g=g):
            midx[g] = pair(0, 1 - x, g).astype(BF16)
            x_send_copy(g).start()

        def plain_y(g=g):
            midy[g] = pair(1, x, g).astype(BF16)
            y_send_copy(g).start()

        when_x_first(g, plain_x)
        when_y_first(g, plain_y)
    for i in order:
        g = near(i)
        diag_copy(g, to_mate).wait_recv()

        def joined_y(g=g):
            midy[g] = (pair(1, x, g) + gotd[g].astype(F32)).astype(BF16)
            y_send_copy(g).start()

        def joined_x(g=g):
            midx[g] = (pair(0, 1 - x, g) + gotd[g].astype(F32)).astype(BF16)
            x_send_copy(g).start()

        when_x_first(g, joined_y)
        when_y_first(g, joined_x)

    def b_copy(i):
        g = near(i)
        return remote(outb.at[g], back.at[z], b_send.at[i], b_recv.at[z], {"sp": g * nx + x, "tp": tp})

    d_copy(0, x).wait_recv()
    for i in order:
        g = near(i)
        x_send_copy(g).wait_recv()
        y_send_copy(g).wait_recv()
        total = (pair(0, x, g) + gotx[g].astype(F32) + goty[g].astype(F32)).astype(BF16)
        if i:
            outb[g] = total
            b_copy(i).start()
        else:
            back[z] = total
    for i in range(1, nz):
        g = near(i)
        remote(outb.at[g], back.at[g], b_send.at[0], b_recv.at[g], to_mate).wait_recv()
    flat = back[...].reshape(nz * cap, cols)
    routed = lax.dot_general(hits[...], flat, (((0,), (0,)), ((), ())), preferred_element_type=F32)
    second = depth_scale * set_ref[...].astype(F32) + routed
    stats_start(n_tp, sp, tp, lane_sums(second), lane_sums(second * second), stat, s_send, s_recv)
    others(lambda d: w_copy(d).wait_send())
    for i in range(nz):
        g = near(i)
        if i:
            a_copy(i).wait_send()
            b_copy(i).wait_send()
        x_copy(1, tp, x, g, to_x).wait_send()
        x_copy(2, tp, x, g, to_y).wait_send()
        for kind in (0, 3, 5, 7):
            x_copy(kind, tp, x, g, to_mate).wait_send()
        when_x_first(g, lambda g=g: x_copy(4, tp, 1 - x, g, to_y).wait_send())
        when_y_first(g, lambda g=g: x_copy(6, far, x, g, to_x).wait_send())
        diag_copy(g, to_mate).wait_send()
        x_send_copy(g).wait_send()
        y_send_copy(g).wait_send()
    for k in range(2):
        d_copy(k, 0).wait_send()
        d_copy(k, 1).wait_send()
    one, two = stats_finish(n_tp, sp, tp, stat, s_send, s_recv, rows)
    out_ref[...] = norm(second, one, two, gf_ref[...], bf_ref[...], cols * n_tp)


def body(
    residual_in,
    query_alpha,
    pairs_alpha,
    offset_alpha,
    gain_alpha,
    query_beta,
    pairs_beta,
    offset_beta,
    gain_beta,
    project_alpha,
    project_beta,
    gain_settle,
    bias_settle,
    expert_ids,
    route_weight,
    expert_gate,
    expert_up,
    expert_down,
    gain_final,
    bias_final,
):
    n_sp = lax.axis_size("sp")
    n_tp = lax.axis_size("tp")
    nx = 2 ** ((n_sp.bit_length() - 1) // 2)
    nz = n_sp // nx
    rows, cols = residual_in.shape
    kva = pairs_alpha.shape[1]
    kvb = pairs_beta.shape[1]
    heads = 2 * kva + kvb
    heads_pad = -(-heads // 8) * 8
    kv_cols = kva * 128 + kvb * 256
    inner = kva * 128
    inner_b = kvb * 128
    vm = pl.BlockSpec(memory_space=VMEM)
    hbm = pl.BlockSpec(memory_space=pl.ANY)
    row = lambda v: v.reshape(1, -1)
    cap = -(-(3 * rows // n_sp) // 16) * 16
    places = n_sp * cap
    ny = n_tp // 2
    width, units = expert_gate.shape[1:]
    attend_scratch = [
        VMEM((n_sp, rows, kv_cols), BF16),
        VMEM((n_sp, heads_pad, rows), F32),
        VMEM((kva, 2 * rows, 128), BF16),
        VMEM((rows, inner + inner_b), F32),
        VMEM((heads * rows, 128), F32),
        VMEM(project_alpha.shape, BF16),
        VMEM(project_beta.shape, BF16),
        VMEM((n_tp, rows, cols), F32),
        VMEM((n_tp, rows, cols), F32),
        VMEM((n_tp, rows, cols), BF16),
        VMEM((n_tp, rows, cols), BF16),
        VMEM((n_tp, 2, 8, rows), F32),
        VMEM((n_tp, 2, 8, rows), F32),
        DMA((5,)),
        DMA((nz, nx)),
        DMA((n_sp,)),
        DMA((nz, nx)),
        DMA((n_sp,)),
        DMA((n_tp,)),
        DMA((n_tp,)),
        DMA((n_tp,)),
        DMA((n_tp,)),
        DMA((n_tp,)),
        DMA((n_tp,)),
    ]
    balanced = nx == 2 and ny == 2 and kva == nz and kvb == nz and cap % 16 == 0
    tall = nx * rows
    plane_scratch = [
        VMEM((rows * kva, 128), BF16),
        VMEM((rows * kvb * 2, 128), BF16),
        VMEM((rows * kva, 128), F32),
        VMEM((rows * kvb * 2, 128), F32),
        VMEM((kva, rows, 128), BF16),
        VMEM((kvb, 2, rows, 128), BF16),
        VMEM((nz, 8, 128), F32),
        VMEM((n_sp, rows, 128), BF16),
        VMEM((2, n_sp, rows, 128), BF16),
        VMEM((n_sp, 8, 128), F32),
        VMEM((nz, 2 * tall, 128), BF16),
        VMEM((nz, 2 * tall, 128), BF16),
        VMEM((2, nz, tall, 128), F32),
        VMEM((nz, tall, 128), F32),
        VMEM((n_sp, rows, 128), BF16),
        VMEM((n_sp, rows, 128), BF16),
        VMEM(project_alpha.shape, BF16),
        VMEM(project_beta.shape, BF16),
        VMEM((n_tp, rows, cols), F32),
        VMEM((n_tp, rows, cols), F32),
        VMEM((n_tp, rows, cols), BF16),
        VMEM((n_tp, rows, cols), BF16),
        VMEM((n_tp, 2, 8, rows), F32),
        VMEM((n_tp, 2, 8, rows), F32),
        DMA((4,)),
        DMA((3, n_sp)),
        DMA((3, n_sp)),
        DMA((n_sp,)),
        DMA((n_sp,)),
        DMA((n_tp,)),
        DMA((n_tp,)),
        DMA((n_tp,)),
        DMA((n_tp,)),
        DMA((n_tp,)),
        DMA((n_tp,)),
    ]
    expert_scratch = [
        VMEM((width, units), BF16),
        VMEM((width, units), BF16),
        VMEM((units, width), BF16),
        VMEM((n_sp, cap, cols), BF16),
        VMEM((n_tp, n_sp, cap, cols), BF16),
        VMEM((places, units), F32),
        VMEM((places, units), F32),
        VMEM((places, units), BF16),
        VMEM((ny, n_sp, cap, cols), BF16),
        VMEM((ny, n_sp, cap, cols), BF16),
        VMEM((ny, n_sp, cap, cols), BF16),
        VMEM((ny, n_sp, cap, cols), BF16),
        VMEM((ny, n_sp, cap, cols), BF16),
        VMEM((n_sp, cap, cols), BF16),
        VMEM((n_sp, cap, cols), BF16),
        VMEM((n_tp, 2, 8, rows), F32),
        DMA((3,)),
        DMA((n_sp,)),
        DMA((n_sp,)),
        DMA((ny, n_sp)),
        DMA((n_tp, n_sp)),
        DMA((ny, n_sp)),
        DMA((ny,)),
        DMA((ny,)),
        DMA((ny, n_sp)),
        DMA((ny, n_sp)),
        DMA((n_sp,)),
        DMA((n_sp,)),
        DMA((n_tp,)),
        DMA((n_tp,)),
    ]
    block = (nz, cap, cols)
    grouped_scratch = [
        VMEM((width, units), BF16),
        VMEM((width, units), BF16),
        VMEM((units, width), BF16),
        VMEM((nz * cap, rows), BF16),
        VMEM((nz, 8, 128), F32),
        VMEM((n_sp, 8, 128), F32),
        VMEM((nx, nz, cap, 128), F32),
        VMEM(block, BF16),
        VMEM((n_tp, nx) + block, BF16),
        VMEM((nx, nz * cap, units), F32),
        VMEM((nx, nz * cap, units), F32),
        VMEM((places, units), BF16),
        VMEM((ny, nx) + block, BF16),
        VMEM((ny, nx) + block, BF16),
        VMEM((ny, nx) + block, BF16),
        VMEM(block, BF16),
        VMEM(block, BF16),
        VMEM(block, BF16),
        VMEM(block, BF16),
        VMEM(block, BF16),
        VMEM(block, BF16),
        VMEM(block, BF16),
        VMEM(block, BF16),
        VMEM((n_tp, 2, 8, rows), F32),
        DMA((3,)),
        DMA((n_sp,)),
        DMA((n_sp,)),
        DMA((nz,)),
        DMA((nz,)),
        DMA((8, nz)),
        DMA((n_tp, nx, nz)),
        DMA((ny, nx)),
        DMA((ny, nx)),
        DMA((3, nz)),
        DMA((3, nz)),
        DMA((nz,)),
        DMA((nz,)),
        DMA((n_tp,)),
        DMA((n_tp,)),
    ]
    if balanced:
        attend_scratch, expert_scratch = plane_scratch, grouped_scratch
    n_attend = len(attend_scratch)
    if balanced:
        halves = pairs_beta.reshape(rows, kvb, 2, 128).transpose(0, 2, 1, 3)
        keyed = [
            pairs_alpha.reshape(rows * kva, 128),
            halves.reshape(rows * kvb * 2, 128),
            offset_alpha.T,
            offset_beta.T,
        ]
        places_in = [vm, vm]
        routes = [expert_ids.T, route_weight.T]
    else:
        off = jnp.transpose(jnp.concatenate([offset_alpha, offset_beta], axis=1))
        off = jnp.pad(off, ((0, heads_pad - heads), (0, 0)))
        keyed = [pairs_alpha.reshape(rows, -1), pairs_beta.reshape(rows, -1), off]
        places_in = [hbm]
        routes = [jnp.concatenate([expert_ids.astype(F32), route_weight], axis=1)]
    n_in = len(keyed) + 9
    n_all = n_in + len(routes) + 5

    def kernel(*refs):
        attend_in = refs[:n_in]
        out_ref, settled = refs[n_all : n_all + 2]
        expert_in = refs[n_in:n_all]
        own = refs[n_all + 2 :]

        def attention(*hooks):
            attend = plane_attend if balanced else attend_kernel
            attend(*hooks, n_sp, n_tp, nx, kva, kvb, *attend_in, settled, *own[:n_attend])

        expert = plane_expert if balanced else expert_kernel
        expert(attention, n_sp, n_tp, nx, cap, settled, *expert_in, out_ref, *own[n_attend:])

    return pl.pallas_call(
        kernel,
        out_shape=jax.ShapeDtypeStruct((rows, cols), BF16),
        in_specs=[vm, vm, hbm, hbm] + places_in + [vm] * 3 + [hbm] * 2 + [vm] * (2 + len(routes)) + [hbm] * 3 + [vm] * 2,
        out_specs=vm,
        scratch_shapes=[VMEM((rows, cols), BF16)] + attend_scratch + expert_scratch,
        compiler_params=pltpu.CompilerParams(
            collective_id=0, has_side_effects=True, vmem_limit_bytes=60 * 1024 * 1024
        ),
    )(
        query_alpha,
        query_beta,
        *keyed,
        residual_in,
        row(gain_alpha),
        row(gain_beta),
        project_alpha,
        project_beta,
        row(gain_settle),
        row(bias_settle),
        *routes,
        expert_gate,
        expert_up,
        expert_down,
        row(gain_final),
        row(bias_final),
    )


def solution(mesh):
    in_specs = (
        P("sp", "tp"),
        P("sp", "tp"),
        P("sp", "tp", None),
        P("sp", "tp"),
        P("tp"),
        P("sp", "tp"),
        P("sp", "tp", None),
        P("sp", "tp"),
        P("tp"),
        P("tp", None),
        P("tp", None),
        P("tp"),
        P("tp"),
        P("sp", None),
        P("sp", None),
        P("sp", None, "tp"),
        P("sp", None, "tp"),
        P("sp", "tp", None),
        P("tp"),
        P("tp"),
    )
    out_specs = P("sp", "tp")
    return jax.shard_map(body, mesh=mesh, in_specs=in_specs, out_specs=out_specs, check_vma=False)
```

```python
import functools
import jax
import jax.numpy as jnp
from jax import lax
from jax.experimental import pallas as pl
from jax.experimental.pallas import tpu as pltpu
from jax.sharding import PartitionSpec as P

depth_scale = 2.0**0.5
norm_eps = 1e-05
F32 = jnp.float32
BF16 = jnp.bfloat16
VMEM = pltpu.VMEM
DMA = pltpu.SemaphoreType.DMA


def remote(src, dst, send, recv, where):
    return pltpu.make_async_remote_copy(
        src_ref=src,
        dst_ref=dst,
        send_sem=send,
        recv_sem=recv,
        device_id=where,
        device_id_type=pl.DeviceIdType.MESH,
    )


def greet(n_sp, n_tp, sp, tp):
    barrier = pltpu.get_barrier_semaphore()
    for o in range(1, n_sp):
        pl.semaphore_signal(
            barrier,
            inc=1,
            device_id={"sp": lax.rem(sp + o, n_sp), "tp": tp},
            device_id_type=pl.DeviceIdType.MESH,
        )
    for o in range(1, n_tp):
        pl.semaphore_signal(
            barrier,
            inc=1,
            device_id={"sp": sp, "tp": lax.rem(tp + o, n_tp)},
            device_id_type=pl.DeviceIdType.MESH,
        )
    pl.semaphore_wait(barrier, n_sp + n_tp - 2)


def split(x):
    high = x.astype(BF16)
    return high, (x - high.astype(F32)).astype(BF16)


def lane_sums(x):
    ones = jnp.ones((8, x.shape[1]), BF16)
    dims = (((1,), (1,)), ((), ()))
    high, low = split(x)
    return lax.dot_general(ones, high, dims, preferred_element_type=F32) + lax.dot_general(
        ones, low, dims, preferred_element_type=F32
    )


def column(row, rows):
    return jnp.transpose(jnp.broadcast_to(row[0:1, :], (rows, rows)))[:, 0:1]


def stats_start(n_tp, sp, tp, one, two, stat, send, recv):
    stat[tp, 0] = one
    stat[tp, 1] = two
    for o in range(1, n_tp):
        remote(
            stat.at[tp], stat.at[tp], send.at[o], recv.at[tp], {"sp": sp, "tp": lax.rem(tp + o, n_tp)}
        ).start()


def stats_rows(n_tp, sp, tp, stat, send, recv):
    for o in range(1, n_tp):
        peer = lax.rem(tp + o, n_tp)
        remote(stat.at[peer], stat.at[peer], send.at[o], recv.at[peer], {"sp": sp, "tp": peer}).wait_recv()
    for o in range(1, n_tp):
        peer = lax.rem(tp + o, n_tp)
        remote(stat.at[tp], stat.at[tp], send.at[o], recv.at[tp], {"sp": sp, "tp": peer}).wait_send()
    total = stat[0]
    for t in range(1, n_tp):
        total = total + stat[t]
    return total[0], total[1]


def stats_finish(n_tp, sp, tp, stat, send, recv, rows):
    one, two = stats_rows(n_tp, sp, tp, stat, send, recv)
    return column(one, rows), column(two, rows)


def norm(total, one, two, gain, bias, columns):
    mean = one / columns
    var = two / columns - mean * mean
    return ((total - mean) * lax.rsqrt(var + norm_eps) * gain + bias).astype(BF16)


def attend_kernel(
    early,
    n_sp,
    n_tp,
    nx,
    kva,
    kvb,
    qa_ref,
    qb_ref,
    kva_hbm,
    kvb_hbm,
    off_hbm,
    res_ref,
    ga_ref,
    gb_ref,
    pa_hbm,
    pb_hbm,
    gs_ref,
    bs_ref,
    out_ref,
    kvbuf,
    offbuf,
    qs,
    acc,
    rem,
    pa,
    pb,
    ya,
    yb,
    part,
    got,
    stat1,
    stat2,
    load_sem,
    kv_send,
    kv_recv,
    off_send,
    off_recv,
    part_send,
    part_recv,
    s1_send,
    s1_recv,
    s2_send,
    s2_recv,
):
    sp = lax.axis_index("sp")
    tp = lax.axis_index("tp")
    nz = n_sp // nx
    z = sp // nx
    x = lax.rem(sp, nx)
    rows = qa_ref.shape[0]
    cols = out_ref.shape[1]
    loads = (
        pltpu.make_async_copy(kva_hbm, kvbuf.at[sp, :, 0 : kva * 128], load_sem.at[0]),
        pltpu.make_async_copy(off_hbm, offbuf.at[sp], load_sem.at[1]),
        pltpu.make_async_copy(pa_hbm, pa, load_sem.at[2]),
        pltpu.make_async_copy(pb_hbm, pb, load_sem.at[3]),
        pltpu.make_async_copy(kvb_hbm, kvbuf.at[sp, :, kva * 128 :], load_sem.at[4]),
    )
    for load in loads:
        load.start()
    greet(n_sp, n_tp, sp, tp)
    lane = lax.broadcasted_iota(jnp.int32, (rows, 128), 1)
    row_i = lax.broadcasted_iota(jnp.int32, (rows, 128), 0)
    first_half = lane < 64
    for u in range(kva):
        q32 = qa_ref[:, u * 128 : (u + 1) * 128].astype(F32) * (64**-0.5)
        qs[u, 0:rows] = jnp.where(first_half, q32, 0.0).astype(BF16)
        qs[u, rows : 2 * rows] = jnp.where(first_half, pltpu.roll(q32, 64, 1), 0.0).astype(BF16)
    acc[...] = jnp.zeros_like(acc)
    rem[...] = jnp.zeros_like(rem)
    tri_r = lax.broadcasted_iota(jnp.int32, (256, 256), 0) % 128
    tri_c = lax.broadcasted_iota(jnp.int32, (256, 256), 1)
    tri = jnp.where((tri_r > tri_c) | (tri_c >= 128), 1.0, 0.0).astype(BF16)

    def block(j):
        gap = (sp - j) * rows
        valid1 = lane < row_i + gap
        valid2 = jnp.concatenate([valid1.astype(F32)] * 2, axis=0) > 0.5

        def unit(query, key, value, offset, scale, valid, left):
            s = lax.dot_general(query, key, (((1,), (1,)), ((), ())), preferred_element_type=F32)
            s = (s if scale is None else s * scale) + offset
            soft = jnp.maximum(s, 0.0) + jnp.log(1.0 + jnp.exp(-jnp.abs(s)))
            used = jnp.where(valid, soft, 0.0)
            high, low = split(used)
            sums = jnp.dot(jnp.concatenate([high, low], axis=1), tri, preferred_element_type=F32)
            w = jnp.where(valid, jnp.exp(s - soft - sums[:, :128] + left), 0.0).astype(BF16)
            return jnp.dot(w, value, preferred_element_type=F32), sums[:, 128:]

        for u in range(kva):
            pair = kvbuf[j, :, u * 128 : (u + 1) * 128]
            offset = jnp.concatenate(
                [
                    jnp.broadcast_to(offbuf[j, 2 * u : 2 * u + 1, :], (rows, 128)),
                    jnp.broadcast_to(offbuf[j, 2 * u + 1 : 2 * u + 2, :], (rows, 128)),
                ],
                axis=0,
            )
            left = rem[2 * u * rows : (2 * u + 2) * rows]
            o, total = unit(qs[u], pair, pair, offset, None, valid2, left)
            rem[2 * u * rows : (2 * u + 2) * rows] = left - total
            acc[:, u * 128 : (u + 1) * 128] += jnp.where(
                first_half, pltpu.roll(o[:rows], 64, 1), o[rows:]
            )
        for u in range(kvb):
            base = kva * 128 + u * 256
            head = 2 * kva + u
            key = kvbuf[j, :, base : base + 128]
            value = kvbuf[j, :, base + 128 : base + 256]
            offset = offbuf[j, head : head + 1, :]
            left = rem[head * rows : (head + 1) * rows]
            query = qb_ref[:, u * 128 : (u + 1) * 128]
            o, total = unit(query, key, value, offset, 128**-0.5, valid1, left)
            rem[head * rows : (head + 1) * rows] = left - total
            c = (kva + u) * 128
            acc[:, c : c + 128] += o

    def sends(s):
        j0 = (z - s) * nx + x
        plan = [(z + 1 < nz, jnp.minimum(z + 1, nz - 1) * nx + x)]
        for d in range(1, nx):
            xo = lax.rem(x + d, nx)
            plan.append(((s > 0) | (x < xo), z * nx + xo))
        made = []
        for k, (cond, dest) in enumerate(plan):
            where = {"sp": dest, "tp": tp}
            made.append(
                (
                    cond,
                    remote(kvbuf.at[j0], kvbuf.at[j0], kv_send.at[s, k], kv_recv.at[j0], where),
                    remote(offbuf.at[j0], offbuf.at[j0], off_send.at[s, k], off_recv.at[j0], where),
                )
            )
        return made

    def wait_block(j):
        where = {"sp": sp, "tp": tp}
        remote(kvbuf.at[j], kvbuf.at[j], kv_send.at[0, 0], kv_recv.at[j], where).wait_recv()
        remote(offbuf.at[j], offbuf.at[j], off_send.at[0, 0], off_recv.at[j], where).wait_recv()

    loads[0].wait()
    loads[1].wait()
    loads[4].wait()

    def forward(s):
        @pl.when(s > 0)
        def _():
            wait_block((z - s) * nx + x)

        for cond, kv_copy, off_copy in sends(s):

            @pl.when(cond)
            def _(kv_copy=kv_copy, off_copy=off_copy):
                off_copy.start()
                kv_copy.start()

    forward(0)

    def level(s, carry):
        src = z - s

        @pl.when(s < z)
        def _():
            forward(s + 1)

        def across(i, inner):
            xo = nx - 1 - i

            @pl.when((s > 0) | (xo <= x))
            def _():
                @pl.when(xo != x)
                def _():
                    wait_block(src * nx + xo)

                block(src * nx + xo)

            return inner

        return lax.fori_loop(0, nx, across, carry)

    lax.fori_loop(0, z + 1, level, 0)
    early()

    wide = kva * 128
    aa = acc[:, :wide]
    ab = acc[:, wide:]
    stats_start(n_tp, sp, tp, lane_sums(aa * aa), lane_sums(ab * ab), stat1, s1_send, s1_recv)
    loads[2].wait()
    loads[3].wait()
    na = (aa * ga_ref[...]).astype(BF16)
    nb = (ab * gb_ref[...]).astype(BF16)
    for t in range(n_tp):
        ya[t] = jnp.dot(na, pa[:, t * cols : (t + 1) * cols], preferred_element_type=F32)
        yb[t] = jnp.dot(nb, pb[:, t * cols : (t + 1) * cols], preferred_element_type=F32)
    sq_a, sq_b = stats_finish(n_tp, sp, tp, stat1, s1_send, s1_recv, rows)
    scale_a = lax.rsqrt(sq_a / (wide * n_tp) + norm_eps)
    scale_b = lax.rsqrt(sq_b / (kvb * 128 * n_tp) + norm_eps)

    def part_copy(o):
        peer = lax.rem(tp + o, n_tp)
        return remote(
            part.at[peer], got.at[tp], part_send.at[o], part_recv.at[tp], {"sp": sp, "tp": peer}
        )

    for o in range(1, n_tp):
        peer = lax.rem(tp + o, n_tp)
        part[peer] = (ya[peer] * scale_a + yb[peer] * scale_b).astype(BF16)
        part_copy(o).start()
    total = (ya[tp] * scale_a + yb[tp] * scale_b).astype(BF16).astype(F32)
    for o in range(1, n_tp):
        peer = lax.rem(tp + o, n_tp)
        remote(
            part.at[peer], got.at[peer], part_send.at[o], part_recv.at[peer], {"sp": sp, "tp": peer}
        ).wait_recv()
        total = total + got[peer].astype(F32)
    mixed = total.astype(BF16).astype(F32)
    first = depth_scale * res_ref[...].astype(F32) + mixed
    stats_start(n_tp, sp, tp, lane_sums(first), lane_sums(first * first), stat2, s2_send, s2_recv)
    for o in range(1, n_tp):
        part_copy(o).wait_send()

    def drain(s, carry):
        for cond, kv_copy, off_copy in sends(s):

            @pl.when(cond)
            def _(kv_copy=kv_copy, off_copy=off_copy):
                off_copy.wait_send()
                kv_copy.wait_send()

        return carry

    lax.fori_loop(0, z + 1, drain, 0)
    one, two = stats_finish(n_tp, sp, tp, stat2, s2_send, s2_recv, rows)
    out_ref[...] = norm(first, one, two, gs_ref[...], bs_ref[...], cols * n_tp)


def plane_attend(
    early,
    send_rows,
    send_scales,
    n_sp,
    n_tp,
    nx,
    kva,
    kvb,
    qa_ref,
    qb_ref,
    pairs_a_hbm,
    pairs_b_hbm,
    offa_ref,
    offb_ref,
    res_ref,
    ga_ref,
    gb_ref,
    pa_hbm,
    pb_hbm,
    gs_ref,
    bs_ref,
    out_ref,
    raw_a,
    raw_b,
    wide_a,
    wide_b,
    own_a,
    own_b,
    own_off,
    qin,
    kin,
    oin,
    keys2,
    values2,
    left,
    acc,
    obuf,
    ain,
    pa,
    pb,
    ya,
    yb,
    part,
    got,
    across,
    stat1,
    stat2,
    load_sem,
    in_send,
    in_recv,
    o_send,
    o_recv,
    part_send,
    part_recv,
    s1_send,
    s1_recv,
    s2_send,
    s2_recv,
):
    sp = lax.axis_index("sp")
    tp = lax.axis_index("tp")
    nz = n_sp // nx
    z = sp // nx
    x = lax.rem(sp, nx)
    rows = qa_ref.shape[0]
    cols = out_ref.shape[1]
    tall = nx * rows

    def is_alpha(zz, xx):
        return lax.rem(zz + xx, 2) == 0

    loads = (
        pltpu.make_async_copy(pairs_a_hbm, raw_a, load_sem.at[0]),
        pltpu.make_async_copy(pairs_b_hbm, raw_b, load_sem.at[1]),
        pltpu.make_async_copy(pa_hbm, pa, load_sem.at[2]),
        pltpu.make_async_copy(pb_hbm, pb, load_sem.at[3]),
    )
    loads[0].start()
    loads[1].start()
    for u in range(nz):
        own_off[u, 0:2] = offa_ref[2 * u : 2 * u + 2]
        own_off[u, 2:3] = offb_ref[u : u + 1]
    greet(n_sp, n_tp, sp, tp)
    loads[0].wait()
    wide_a[...] = raw_a[...].astype(F32)
    for u in range(kva):
        own_a[u] = wide_a[pl.ds(u, rows, stride=kva), :].astype(BF16)
    loads[1].wait()
    wide_b[...] = raw_b[...].astype(F32)
    for u in range(kvb):
        for h in range(2):
            own_b[u, h] = wide_b[pl.ds(h * kvb + u, rows, stride=2 * kvb), :].astype(BF16)
    loads[2].start()
    loads[3].start()

    def in_copies(zz, xx, alpha):
        dest = zz * nx + xx
        where = {"sp": dest, "tp": tp}
        at = pl.ds(pl.multiple_of(zz * 128, 128), 128)
        q_ref = qa_ref if alpha else qb_ref
        kv = (own_a.at[zz], kin.at[0, sp]) if alpha else (own_b.at[zz], kin.at[:, sp])
        return (
            remote(own_off.at[zz], oin.at[sp], in_send.at[0, dest], in_recv.at[0, sp], where),
            remote(q_ref.at[:, at], qin.at[sp], in_send.at[1, dest], in_recv.at[1, sp], where),
            remote(*kv, in_send.at[2, dest], in_recv.at[2, sp], where),
        )

    def each_dest(act, low, high):
        def hop(t, carry):
            away = (t + 1) // 2
            zz = z + away * (2 * lax.rem(t, 2) - 1) * (1 - 2 * lax.rem(tp, 2))
            for xx in range(nx):
                there = (zz >= 0) & (zz < nz) & ((zz != z) | (xx != x))
                for alpha in (True, False):

                    @pl.when(there & (is_alpha(zz, xx) == alpha))
                    def _(xx=xx, alpha=alpha):
                        for copy in in_copies(zz, xx, alpha):
                            act(copy)

            return carry

        lax.fori_loop(low, high, hop, 0)

    hops = 2 * nz - 1
    outer = ((z == 0) | (z == nz - 1)).astype(jnp.int32)
    held = hops + 0 * outer
    each_dest(lambda copy: copy.start(), 0, held)
    early()

    def o_copy(d):
        return remote(obuf.at[d], ain.at[sp], o_send.at[d], o_recv.at[sp], {"sp": d, "tp": tp})

    lane_t = lax.broadcasted_iota(jnp.int32, (tall, tall), 1)
    row_t = lax.broadcasted_iota(jnp.int32, (tall, tall), 0)
    lane = lax.broadcasted_iota(jnp.int32, (tall, 128), 1)
    tri = jnp.where(row_t > lane_t, 1.0, 0.0).astype(BF16)

    def attend(alpha):
        heads = 2 if alpha else 1
        scale = 64**-0.5 if alpha else 128**-0.5
        at = pl.ds(pl.multiple_of(z * 128, 128), 128)
        oin[sp] = own_off[z]
        if alpha:
            qin[sp] = qa_ref[:, at]
            kin[0, sp] = own_a[z]
        else:
            qin[sp] = qb_ref[:, at]
            kin[:, sp] = own_b[z]

        def arrive(p):
            for xx in range(nx):
                s = p * nx + xx

                @pl.when(s != sp)
                def _(s=s):
                    where = {"sp": sp, "tp": tp}
                    kv = kin.at[0, s] if alpha else kin.at[:, s]
                    remote(oin.at[s], oin.at[s], in_send.at[0, 0], in_recv.at[0, s], where).wait_recv()
                    remote(qin.at[s], qin.at[s], in_send.at[1, 0], in_recv.at[1, s], where).wait_recv()
                    remote(kv, kv, in_send.at[2, 0], in_recv.at[2, s], where).wait_recv()

            if alpha:
                pair = kin[0, pl.ds(p * nx, nx)].reshape(tall, 128).astype(F32)
                turned = pltpu.roll(pair, 64, 1)
                keys2[p, 0:tall] = jnp.where(lane < 64, pair, 0.0).astype(BF16)
                keys2[p, tall:] = jnp.where(lane < 64, 0.0, turned).astype(BF16)
                values2[p, 0:tall] = jnp.where(lane < 64, turned, 0.0).astype(BF16)
                values2[p, tall:] = jnp.where(lane < 64, 0.0, pair).astype(BF16)

        def step(r, c, diag):
            query = qin[pl.ds(r * nx, nx)].reshape(tall, 128)
            if alpha:
                key, value = keys2[c], values2[c]
            else:
                key = kin[0, pl.ds(c * nx, nx)].reshape(tall, 128)
                value = kin[1, pl.ds(c * nx, nx)].reshape(tall, 128)
            scores = lax.dot_general(query, key, (((1,), (1,)), ((), ())), preferred_element_type=F32)
            valid = lane_t < row_t
            ws = []
            for h in range(heads):
                row = h if alpha else 2
                offset = jnp.concatenate([oin[c * nx + i, row : row + 1, :] for i in range(nx)], axis=1)
                s = scores[:, h * tall : (h + 1) * tall] * scale + offset
                soft = jnp.maximum(s, 0.0) + jnp.log(1.0 + jnp.exp(-jnp.abs(s)))
                used = jnp.where(valid, soft, 0.0) if diag else soft
                sums = jnp.dot(used.astype(BF16), tri, preferred_element_type=F32)
                total = jnp.broadcast_to(sums[:, 0:1] + used[:, 0:1], (tall, 128))
                e = s - soft - sums
                if diag:
                    w = jnp.where(valid, jnp.exp(e), 0.0)
                    left[h, r] = -total
                else:
                    before = left[h, r]
                    w = jnp.exp(e + jnp.concatenate([before] * nx, axis=1))
                    left[h, r] = before - total
                ws.append(w.astype(BF16))
            w = ws[0] if heads == 1 else jnp.concatenate(ws, axis=1)
            o = jnp.dot(w, value, preferred_element_type=F32)
            o = o if diag else acc[r] + o
            acc[r] = o

            @pl.when(c == 0)
            def _():
                obuf[pl.ds(r * nx, nx)] = o.astype(BF16).reshape(nx, rows, 128)
                for xx in range(nx):
                    d = r * nx + xx

                    @pl.when(d != sp)
                    def _(d=d):
                        o_copy(d).start()

                    @pl.when(d == sp)
                    def _(d=d):
                        ain[sp] = obuf[d]

        def phase(k, span):
            low, high = span
            lower_half = z < nz // 2
            up = jnp.where(lower_half, low == 0, high < nz - 1).astype(jnp.int32)
            first = (k == 0).astype(jnp.int32)
            p = first * z + (1 - first) * (up * (high + 1) + (1 - up) * (low - 1))

            arrive(p)

            @pl.when(k == 1)
            def _():
                each_dest(lambda copy: copy.start(), held, hops)

            step(p, p, True)
            count = (1 - first) * (high - low + 1)

            def more(t, carry):
                step(p + t * (1 - up), p - t * up, False)
                return carry

            lax.fori_loop(1, count + 1, more, 0)
            return jnp.minimum(low, p), jnp.maximum(high, p)

        lax.fori_loop(0, nz, phase, (z, z))

    for alpha in (True, False):

        @pl.when(is_alpha(z, x) == alpha)
        def _(alpha=alpha):
            attend(alpha)

    def o_wait(j, carry):
        @pl.when(j != sp)
        def _():
            remote(obuf.at[j], ain.at[j], o_send.at[0], o_recv.at[j], {"sp": sp, "tp": tp}).wait_recv()

        return carry

    lax.fori_loop(0, n_sp, o_wait, 0)
    wide = kva * 128
    aa = jnp.concatenate([ain[k * nx + k % 2] for k in range(nz)], axis=1).astype(F32)
    ab = jnp.concatenate([ain[k * nx + 1 - k % 2] for k in range(nz)], axis=1).astype(F32)
    stats_start(n_tp, sp, tp, lane_sums(aa * aa), lane_sums(ab * ab), stat1, s1_send, s1_recv)
    loads[2].wait()
    loads[3].wait()
    core = lax.rem(tp, 2)
    y = tp // 2
    sides = ((1 - y) * 2, y * 2)
    to_mate = {"sp": sp, "tp": y * 2 + 1 - core}
    to_far = {"sp": sp, "tp": (1 - y) * 2 + core}
    na = (aa * ga_ref[...]).astype(BF16)
    nb = (ab * gb_ref[...]).astype(BF16)

    def project(t):
        at = pl.ds(pl.multiple_of(t * cols, 128), cols)
        return (
            jnp.dot(na, pa[:, at], preferred_element_type=F32),
            jnp.dot(nb, pb[:, at], preferred_element_type=F32),
        )

    def mate_copy(k):
        return remote(part.at[k], got.at[k], part_send.at[k], part_recv.at[k], to_mate)

    for k in range(2):
        a, b = project(sides[k] + 1 - core)
        part[k, 0] = a.astype(BF16)
        part[k, 1] = b.astype(BF16)
        mate_copy(k).start()
    for k in range(2):
        ya[k], yb[k] = project(sides[k] + core)
    sq_a, sq_b = stats_finish(n_tp, sp, tp, stat1, s1_send, s1_recv, rows)
    scale_a = lax.rsqrt(sq_a / (wide * n_tp) + norm_eps)
    scale_b = lax.rsqrt(sq_b / (kvb * 128 * n_tp) + norm_eps)

    def chip_sum(k):
        mate_copy(k).wait_recv()
        return (ya[k] + got[k, 0].astype(F32)) * scale_a + (yb[k] + got[k, 1].astype(F32)) * scale_b

    far_copy = remote(across.at[0], across.at[1], part_send.at[2], part_recv.at[2], to_far)
    across[0] = chip_sum(0).astype(BF16)
    far_copy.start()
    total = chip_sum(1)
    residual = depth_scale * res_ref[...].astype(F32)
    far_copy.wait_recv()
    mixed = (total + across[1].astype(F32)).astype(BF16).astype(F32)
    first = residual + mixed
    sums = lane_sums(first)
    stats_start(n_tp, sp, tp, sums, lane_sums(first * first), stat2, s2_send, s2_recv)
    centre = sums / cols
    send_rows((first - column(centre, rows)).astype(BF16))
    far_copy.wait_send()
    for k in range(2):
        mate_copy(k).wait_send()
    each_dest(lambda copy: copy.wait_send(), 0, hops)

    def o_drain(j, carry):
        @pl.when(j != sp)
        def _():
            o_copy(j).wait_send()

        return carry

    lax.fori_loop(0, n_sp, o_drain, 0)
    one, two = stats_rows(n_tp, sp, tp, stat2, s2_send, s2_recv)
    mean = one / (cols * n_tp)
    factor = lax.rsqrt(two / (cols * n_tp) - mean * mean + norm_eps)
    shifts = [(stat2[t, 0] / cols - mean) * factor for t in range(n_tp)]
    send_scales([factor] + shifts)
    flat = (first - column(mean, rows)) * column(factor, rows)
    out_ref[...] = (flat * gs_ref[...] + bs_ref[...]).astype(BF16)


def expert_kernel(
    attention,
    n_sp,
    n_tp,
    nx,
    cap,
    set_ref,
    ids_ref,
    wg_hbm,
    wu_hbm,
    wd_hbm,
    gf_ref,
    bf_ref,
    out_ref,
    wg,
    wu,
    wd,
    sendbuf,
    xbuf,
    gate,
    up,
    hid,
    away,
    arrived,
    home,
    pre,
    peers,
    outb,
    back,
    stat,
    load_sem,
    a_send,
    a_recv,
    x_send,
    x_recv,
    relay_send,
    d_send,
    d_recv,
    y_send,
    y_recv,
    b_send,
    b_recv,
    s_send,
    s_recv,
):
    sp = lax.axis_index("sp")
    tp = lax.axis_index("tp")
    rows, cols = set_ref.shape
    places = n_sp * cap
    ny = n_tp // 2
    y = tp // 2
    core = lax.rem(tp, 2)
    mate = y * 2 + 1 - core
    loads = (
        pltpu.make_async_copy(wg_hbm.at[0], wg, load_sem.at[0]),
        pltpu.make_async_copy(wu_hbm.at[0], wu, load_sem.at[1]),
        pltpu.make_async_copy(wd_hbm.at[0], wd, load_sem.at[2]),
    )

    def loop(low, high, fn):
        def step(i, carry):
            fn(i)
            return carry

        lax.fori_loop(low, high, step, 0)

    def x_copies(j):
        made = []
        for k in range(ny):
            dest = mate if k == 0 else lax.rem(y + k, ny) * 2 + core
            made.append(
                remote(
                    xbuf.at[tp, j], xbuf.at[tp, j], x_send.at[k, j], x_recv.at[tp, j], {"sp": sp, "tp": dest}
                )
            )
        return made

    def spread_out(j):
        @pl.when(j != sp)
        def _():
            remote(
                sendbuf.at[j], xbuf.at[tp, j], a_send.at[0], a_recv.at[j], {"sp": sp, "tp": tp}
            ).wait_recv()

        for copy in x_copies(j):
            copy.start()

    ahead = jnp.maximum(sp // nx - 1, 0) * nx

    for load in loads:
        load.start()
    attention(lambda: loop(0, ahead, spread_out))
    ids = ids_ref[...][:, 0:2]
    expert = lax.broadcasted_iota(jnp.int32, (rows, 128), 1).astype(F32)
    hot = [jnp.where(ids[:, k : k + 1] == expert, 1.0, 0.0) for k in range(2)]
    r = lax.broadcasted_iota(jnp.int32, (rows, rows), 0)
    c = lax.broadcasted_iota(jnp.int32, (rows, rows), 1)
    lower = jnp.where(c < r, 1.0, 0.0).astype(BF16)
    before = jnp.dot(lower, (hot[0] + hot[1]).astype(BF16), preferred_element_type=F32)
    seat = lax.broadcasted_iota(jnp.int32, (rows, places), 1).astype(F32)
    hits = []
    for k in range(2):
        slot = jnp.sum(before * hot[k], axis=1, keepdims=True)
        place = ids[:, k : k + 1] * cap + slot
        hits.append(jnp.where(place == seat, 1.0, 0.0))
    spread = jnp.transpose(hits[0] + hits[1]).astype(BF16)
    sent = jnp.dot(spread, set_ref[...], preferred_element_type=F32).astype(BF16)
    sendbuf[...] = sent.reshape(n_sp, cap, cols)

    def at_sp(o):
        return lax.rem(sp + o, n_sp)

    def a_copy(o):
        dest = at_sp(o)
        return remote(
            sendbuf.at[dest], xbuf.at[tp, sp], a_send.at[o], a_recv.at[sp], {"sp": dest, "tp": tp}
        )

    loop(1, n_sp, lambda o: a_copy(o).start())
    xbuf[tp, sp] = sendbuf[sp]

    def x_wait(t, j):
        remote(xbuf.at[t, j], xbuf.at[t, j], x_send.at[0, 0], x_recv.at[t, j], {"sp": sp, "tp": t}).wait_recv()

    loop(ahead, n_sp, spread_out)

    def relay_copy(k, o):
        t = lax.rem(y + k, ny) * 2 + core
        j = o
        return remote(
            xbuf.at[t, j], xbuf.at[t, j], relay_send.at[k, o], x_recv.at[t, j], {"sp": sp, "tp": mate}
        )

    def gather_dot(t, fresh):
        xs = xbuf[t].reshape(places, cols)
        at = pl.ds(pl.multiple_of(t * cols, 128), cols)
        g = jnp.dot(xs, wg[at, :], preferred_element_type=F32)
        u = jnp.dot(xs, wu[at, :], preferred_element_type=F32)
        if fresh:
            gate[...] = g
            up[...] = u
        else:
            gate[...] += g
            up[...] += u

    loads[0].wait()
    loads[1].wait()
    gather_dot(tp, True)

    def arrive_mate(o):
        x_wait(mate, o)

    loop(0, n_sp, arrive_mate)
    gather_dot(mate, False)

    def from_y(k):
        t = lax.rem(y + k, ny) * 2 + core
        other = lax.rem(y + k, ny) * 2 + 1 - core

        def pass_on(o):
            x_wait(t, o)
            relay_copy(k, o).start()

        loop(0, n_sp, pass_on)
        gather_dot(t, False)

        def arrive(o):
            x_wait(other, o)

        loop(0, n_sp, arrive)
        gather_dot(other, False)

    loop(1, ny, from_y)
    value = gate[...]
    hid[...] = (value / (1.0 + jnp.exp(-value)) * up[...]).astype(BF16)
    loads[2].wait()

    def down(t):
        at = pl.ds(pl.multiple_of(t * cols, 128), cols)
        result = jnp.dot(hid[...], wd[:, at], preferred_element_type=F32)
        return result.astype(BF16).reshape(n_sp, cap, cols)

    def d_copy(k):
        return remote(away.at[k], arrived.at[k], d_send.at[k], d_recv.at[k], {"sp": sp, "tp": mate})

    def down_away(i):
        k = lax.rem(i + 1, ny)
        away[k] = down(lax.rem(y + k, ny) * 2 + 1 - core)
        d_copy(k).start()

    loop(0, ny, down_away)

    def down_home(i):
        k = lax.rem(i + 1, ny)
        home[k] = down(lax.rem(y + k, ny) * 2 + core)

    loop(0, ny, down_home)

    def y_copy(k, o):
        j = at_sp(o)
        return remote(
            pre.at[k, j],
            peers.at[k, j],
            y_send.at[k, o],
            y_recv.at[k, j],
            {"sp": sp, "tp": lax.rem(y + k, ny) * 2 + core},
        )

    for i in range(ny):
        k = (i + 1) % ny
        d_copy(k).wait_recv()
        if k:

            def to_y(o, k=k):
                j = at_sp(o)
                pre[k, j] = (home[k, j].astype(F32) + arrived[k, j].astype(F32)).astype(BF16)
                y_copy(k, o).start()

            loop(1, n_sp, to_y)
            to_y(0)

    def b_copy(o):
        dest = at_sp(o)
        return remote(outb.at[dest], back.at[sp], b_send.at[o], b_recv.at[sp], {"sp": dest, "tp": tp})

    def settle(o):
        j = at_sp(o)
        total = home[0, j].astype(F32) + arrived[0, j].astype(F32)
        for k in range(1, ny):
            remote(
                pre.at[k, j], peers.at[k, j], y_send.at[k, 0], y_recv.at[k, j], {"sp": sp, "tp": mate}
            ).wait_recv()
            total = total + peers[k, j].astype(F32)
        return total.astype(BF16)

    def give_back(o):
        outb[at_sp(o)] = settle(o)
        b_copy(o).start()

    loop(1, n_sp, give_back)
    back[sp] = settle(0)

    def wait_back(o):
        j = lax.rem(sp - o + n_sp, n_sp)
        remote(outb.at[j], back.at[j], b_send.at[0], b_recv.at[j], {"sp": j, "tp": tp}).wait_recv()

    loop(1, n_sp, wait_back)
    flat = back[...].reshape(places, cols)
    weight = ids_ref[...][:, 2:4]
    routed = weight[:, 0:1] * jnp.dot(hits[0].astype(BF16), flat, preferred_element_type=F32)
    routed = routed + weight[:, 1:2] * jnp.dot(hits[1].astype(BF16), flat, preferred_element_type=F32)
    second = depth_scale * set_ref[...].astype(F32) + routed
    stats_start(n_tp, sp, tp, lane_sums(second), lane_sums(second * second), stat, s_send, s_recv)

    def drain(o):
        for copy in x_copies(o):
            copy.wait_send()
        for k in range(1, ny):
            relay_copy(k, o).wait_send()
            y_copy(k, o).wait_send()

    loop(0, n_sp, drain)

    def drain_sp(o):
        a_copy(o).wait_send()
        b_copy(o).wait_send()

    loop(1, n_sp, drain_sp)
    for k in range(ny):
        d_copy(k).wait_send()
    one, two = stats_finish(n_tp, sp, tp, stat, s_send, s_recv, rows)
    out_ref[...] = norm(second, one, two, gf_ref[...], bf_ref[...], cols * n_tp)


def plane_expert(
    attention,
    n_sp,
    n_tp,
    nx,
    cap,
    set_ref,
    gs_ref,
    bs_ref,
    ids_ref,
    weight_ref,
    wg_hbm,
    wu_hbm,
    wd_hbm,
    gf_ref,
    bf_ref,
    out_ref,
    wg,
    wu,
    wd,
    hits,
    packed,
    scales,
    scaled,
    affine,
    xbuf,
    gate,
    up,
    hid,
    away,
    arrived,
    home,
    mid,
    midx,
    midy,
    gotd,
    gotx,
    goty,
    outb,
    back,
    stat,
    load_sem,
    a_send,
    a_recv,
    t_send,
    t_recv,
    g_send,
    g_recv,
    x_send,
    x_recv,
    d_send,
    d_recv,
    m_send,
    m_recv,
    b_send,
    b_recv,
    s_send,
    s_recv,
):
    sp = lax.axis_index("sp")
    tp = lax.axis_index("tp")
    rows, cols = set_ref.shape
    nz = n_sp // nx
    z = sp // nx
    x = lax.rem(sp, nx)
    core = lax.rem(tp, 2)
    y = tp // 2
    mate = y * 2 + 1 - core
    far = (1 - y) * 2 + core
    far_mate = (1 - y) * 2 + 1 - core
    to_mate = {"sp": sp, "tp": mate}
    to_x = {"sp": z * nx + 1 - x, "tp": tp}
    to_y = {"sp": sp, "tp": far}
    table = [sorted(range(nz), key=lambda g: (abs(g - a), (g - a) * (1 if a < nz // 2 else -1))) for a in range(nz)]

    def near(i):
        pick = table[0][i]
        for a in range(1, nz):
            pick = jnp.where(z == a, table[a][i], pick)
        return pick

    loads = (
        pltpu.make_async_copy(wg_hbm.at[0], wg, load_sem.at[0]),
        pltpu.make_async_copy(wu_hbm.at[0], wu, load_sem.at[1]),
        pltpu.make_async_copy(wd_hbm.at[0], wd, load_sem.at[2]),
    )

    def g_copy(o):
        where = {"sp": sp, "tp": lax.rem(tp + o, n_tp)}
        return remote(affine.at[tp], affine.at[tp], g_send.at[o], g_recv.at[tp], where)

    def others(fn):
        def one(d, carry):
            @pl.when(d != sp)
            def _():
                fn(d)

            return carry

        lax.fori_loop(0, n_sp, one, 0)

    def early():
        for load in loads:
            load.start()
        affine[tp, 0:1] = gs_ref[...]
        affine[tp, 1:2] = bs_ref[...]
        for o in range(1, n_tp):
            g_copy(o).start()
        ids = [ids_ref[k : k + 1, :] for k in range(2)]
        r = lax.broadcasted_iota(jnp.int32, (rows, rows), 0)
        c = lax.broadcasted_iota(jnp.int32, (rows, rows), 1)
        upper = jnp.where(r < c, 1.0, 0.0).astype(BF16)
        group = lax.broadcasted_iota(jnp.int32, (8, rows), 0) * nx
        hot = jnp.where((ids[0] >= group) & (ids[0] < group + nx), 1.0, 0.0)
        before = jnp.dot(hot.astype(BF16), upper, preferred_element_type=F32)
        seat = lax.broadcasted_iota(jnp.int32, (cap, rows), 0).astype(F32)
        for g in range(nz):
            match = jnp.where(seat == before[g : g + 1], hot[g : g + 1], 0.0).astype(BF16)
            hits[g * cap : (g + 1) * cap] = match
            scales[g] = jnp.zeros((8, 128), F32)

    def a_copy(i):
        g = near(i)
        return remote(packed.at[g], xbuf.at[tp, x, z], a_send.at[i], a_recv.at[z], {"sp": g * nx + x, "tp": tp})

    def t_copy(d):
        return remote(scales.at[d // nx], scaled.at[sp], t_send.at[d], t_recv.at[sp], {"sp": d, "tp": tp})

    def send_rows(part):
        sent = jnp.dot(hits[...], part, preferred_element_type=F32).astype(BF16)
        packed[...] = sent.reshape(nz, cap, cols)
        for i in range(1, nz):
            a_copy(i).start()
        xbuf[tp, x, z] = packed[z]

    def compact(lines, g):
        line = lax.broadcasted_iota(jnp.int32, (8, rows), 0)
        tile = jnp.zeros((8, rows), F32)
        for k, value in enumerate(lines):
            tile = jnp.where(line == k, value, tile)
        high, low = split(tile)
        dims = (((1,), (1,)), ((), ()))
        match = hits[g * cap : (g + 1) * cap]
        return lax.dot_general(high, match, dims, preferred_element_type=F32) + lax.dot_general(
            low, match, dims, preferred_element_type=F32
        )

    def send_scales(lines):
        for g in range(nz):
            share = []
            for e in range(nx):
                chosen = [
                    jnp.where(ids_ref[k : k + 1, :] == g * nx + e, weight_ref[k : k + 1, :], 0.0) for k in range(2)
                ]
                share.append(chosen[0] + chosen[1])
            scales[g, :, 0:cap] = compact(lines + share, g)
        others(lambda d: t_copy(d).start())
        scaled[sp] = scales[z]

    def x_copy(kind, t, xs, g, where):
        block = xbuf.at[t, xs, g]
        return remote(block, block, x_send.at[kind, g], x_recv.at[t, xs, g], where)

    def x_wait(t, xs, g):
        block = xbuf.at[t, xs, g]
        remote(block, block, x_send.at[0, 0], x_recv.at[t, xs, g], to_mate).wait_recv()

    def when_x_first(g, fn):
        pl.when(lax.rem(g, 2) == 0)(fn)

    def when_y_first(g, fn):
        pl.when(lax.rem(g, 2) == 1)(fn)

    def own_out(i):
        g = near(i)
        if i:
            remote(packed.at[g], xbuf.at[tp, x, g], a_send.at[0], a_recv.at[g], to_mate).wait_recv()
        x_copy(1, tp, x, g, to_x).start()
        x_copy(2, tp, x, g, to_y).start()
        x_copy(0, tp, x, g, to_mate).start()

    def pass_on(i):
        g = near(i)
        x_wait(tp, 1 - x, g)
        when_x_first(g, lambda: x_copy(4, tp, 1 - x, g, to_y).start())
        x_copy(3, tp, 1 - x, g, to_mate).start()
        x_wait(far, x, g)
        when_y_first(g, lambda: x_copy(6, far, x, g, to_x).start())
        x_copy(5, far, x, g, to_mate).start()

    def pass_diag(i):
        g = near(i)
        x_wait(far, 1 - x, g)
        x_copy(7, far, 1 - x, g, to_mate).start()

    def t_wait(j):
        remote(scaled.at[j], scaled.at[j], t_send.at[0], t_recv.at[j], to_mate).wait_recv()

    def piece(t, xs, fresh):
        factor, shift = [], []
        for g in range(nz):
            j = g * nx + xs
            factor.append(scaled[j, 0:1, :])
            shift.append(scaled[j, pl.ds(1 + t, 1), :])
        turned = jnp.transpose(jnp.concatenate(factor + shift, axis=0))
        gain, bias = affine[t, 0:1, :], affine[t, 1:2, :]
        block = jnp.concatenate(
            [
                (
                    (xbuf[t, xs, g].astype(F32) * turned[0:cap, g : g + 1] + turned[0:cap, nz + g : nz + g + 1]) * gain
                    + bias
                ).astype(BF16)
                for g in range(nz)
            ],
            axis=0,
        )
        at = pl.ds(pl.multiple_of(t * cols, 128), cols)
        g = jnp.dot(block, wg[at, :], preferred_element_type=F32)
        u = jnp.dot(block, wu[at, :], preferred_element_type=F32)
        if fresh:
            gate[xs] = g
            up[xs] = u
        else:
            gate[xs] += g
            up[xs] += u

    def all_in(t, xs):
        def one(g, carry):
            x_wait(t, xs, g)
            return carry

        lax.fori_loop(0, nz, one, 0)

    def exchange(i):
        if i < nz:
            own_out(i)
        if 1 <= i <= nz:
            pass_on(i - 1)
        if i >= 2:
            pass_diag(i - 2)

    def first_rows(part):
        send_rows(part)
        exchange(0)
        exchange(1)

    attention(early, first_rows, send_scales)
    for i in range(2, nz + 2):
        exchange(i)
        if i == nz - 1:
            loads[0].wait()
            loads[1].wait()
            others(t_wait)
            for o in range(1, n_tp):
                peer = lax.rem(tp + o, n_tp)
                remote(affine.at[peer], affine.at[peer], g_send.at[0], g_recv.at[peer], to_mate).wait_recv()
            piece(tp, x, True)
        if i == nz:
            all_in(mate, x)
            piece(mate, x, False)
            piece(far, x, False)
            piece(tp, 1 - x, True)
    all_in(far_mate, x)
    piece(far_mate, x, False)
    all_in(mate, 1 - x)
    piece(mate, 1 - x, False)
    piece(far, 1 - x, False)
    all_in(far_mate, 1 - x)
    piece(far_mate, 1 - x, False)
    for xs in range(nx):
        value = gate[xs]
        line = [scaled[g * nx + xs, pl.ds(1 + n_tp + x, 1), :] for g in range(nz)]
        turned = jnp.transpose(jnp.concatenate(line + line, axis=0))
        weight = jnp.concatenate([turned[0:cap, g : g + 1] for g in range(nz)], axis=0)
        hid[xs * nz * cap : (xs + 1) * nz * cap] = (value / (1.0 + jnp.exp(-value)) * up[xs] * weight).astype(BF16)
    loads[2].wait()

    def down(t):
        at = pl.ds(pl.multiple_of(t * cols, 128), cols)
        result = jnp.dot(hid[...], wd[:, at], preferred_element_type=F32)
        return result.astype(BF16).reshape(nx, nz, cap, cols)

    def d_copy(k, xs):
        return remote(away.at[k, xs], arrived.at[k, xs], d_send.at[k, xs], d_recv.at[k, xs], to_mate)

    away[1] = down(far_mate)
    d_copy(1, 1 - x).start()
    d_copy(1, x).start()
    away[0] = down(mate)
    d_copy(0, 1 - x).start()
    d_copy(0, x).start()
    home[1] = down(far)

    def pair(k, xs, g):
        return home[k, xs, g].astype(F32) + arrived[k, xs, g].astype(F32)

    def m_copy(kind, src, dst, g, where):
        return remote(src.at[g], dst.at[g], m_send.at[kind, g], m_recv.at[kind, g], where)

    def diag_copy(g, where):
        return m_copy(0, mid, gotd, g, where)

    def x_send_copy(g):
        return m_copy(1, midx, gotx, g, to_x)

    def y_send_copy(g):
        return m_copy(2, midy, goty, g, to_y)

    order = range(nz - 1, -1, -1)
    late = order[nz // 2 :]

    def plain(i):
        g = near(i)

        def plain_x():
            midx[g] = pair(0, 1 - x, g).astype(BF16)
            x_send_copy(g).start()

        def plain_y():
            midy[g] = pair(1, x, g).astype(BF16)
            y_send_copy(g).start()

        when_x_first(g, plain_x)
        when_y_first(g, plain_y)

    def joined(i):
        g = near(i)
        diag_copy(g, to_mate).wait_recv()

        def joined_y():
            midy[g] = (pair(1, x, g) + gotd[g].astype(F32)).astype(BF16)
            y_send_copy(g).start()

        def joined_x():
            midx[g] = (pair(0, 1 - x, g) + gotd[g].astype(F32)).astype(BF16)
            x_send_copy(g).start()

        when_x_first(g, joined_y)
        when_y_first(g, joined_x)

    def diagonal(i):
        g = near(i)
        mid[g] = pair(1, 1 - x, g).astype(BF16)
        when_x_first(g, lambda: diag_copy(g, to_x).start())
        when_y_first(g, lambda: diag_copy(g, to_y).start())

    d_copy(1, 1 - x).wait_recv()
    for i in order:
        diagonal(i)
    home[0] = down(tp)
    d_copy(1, x).wait_recv()
    d_copy(0, 1 - x).wait_recv()
    for i in order[: nz // 2]:
        plain(i)
    for i in order[: nz // 2]:
        joined(i)
    for i in late:
        plain(i)
    for i in late:
        joined(i)

    def b_copy(i):
        g = near(i)
        return remote(outb.at[g], back.at[z], b_send.at[i], b_recv.at[z], {"sp": g * nx + x, "tp": tp})

    d_copy(0, x).wait_recv()
    for i in order:
        g = near(i)
        x_send_copy(g).wait_recv()
        y_send_copy(g).wait_recv()
        total = (pair(0, x, g) + gotx[g].astype(F32) + goty[g].astype(F32)).astype(BF16)
        if i:
            outb[g] = total
            b_copy(i).start()
        else:
            back[z] = total
    for i in range(1, nz):
        g = near(i)
        remote(outb.at[g], back.at[g], b_send.at[0], b_recv.at[g], to_mate).wait_recv()
    flat = back[...].reshape(nz * cap, cols)
    routed = lax.dot_general(hits[...], flat, (((0,), (0,)), ((), ())), preferred_element_type=F32)
    second = depth_scale * set_ref[...].astype(F32) + routed
    stats_start(n_tp, sp, tp, lane_sums(second), lane_sums(second * second), stat, s_send, s_recv)
    others(lambda d: t_copy(d).wait_send())
    for o in range(1, n_tp):
        g_copy(o).wait_send()
    for i in range(nz):
        g = near(i)
        if i:
            a_copy(i).wait_send()
            b_copy(i).wait_send()
        x_copy(1, tp, x, g, to_x).wait_send()
        x_copy(2, tp, x, g, to_y).wait_send()
        for kind in (0, 3, 5, 7):
            x_copy(kind, tp, x, g, to_mate).wait_send()
        when_x_first(g, lambda g=g: x_copy(4, tp, 1 - x, g, to_y).wait_send())
        when_y_first(g, lambda g=g: x_copy(6, far, x, g, to_x).wait_send())
        diag_copy(g, to_mate).wait_send()
        x_send_copy(g).wait_send()
        y_send_copy(g).wait_send()
    for k in range(2):
        d_copy(k, 0).wait_send()
        d_copy(k, 1).wait_send()
    one, two = stats_finish(n_tp, sp, tp, stat, s_send, s_recv, rows)
    out_ref[...] = norm(second, one, two, gf_ref[...], bf_ref[...], cols * n_tp)


def body(
    residual_in,
    query_alpha,
    pairs_alpha,
    offset_alpha,
    gain_alpha,
    query_beta,
    pairs_beta,
    offset_beta,
    gain_beta,
    project_alpha,
    project_beta,
    gain_settle,
    bias_settle,
    expert_ids,
    route_weight,
    expert_gate,
    expert_up,
    expert_down,
    gain_final,
    bias_final,
):
    n_sp = lax.axis_size("sp")
    n_tp = lax.axis_size("tp")
    nx = 2 ** ((n_sp.bit_length() - 1) // 2)
    nz = n_sp // nx
    rows, cols = residual_in.shape
    kva = pairs_alpha.shape[1]
    kvb = pairs_beta.shape[1]
    heads = 2 * kva + kvb
    heads_pad = -(-heads // 8) * 8
    kv_cols = kva * 128 + kvb * 256
    inner = kva * 128
    inner_b = kvb * 128
    vm = pl.BlockSpec(memory_space=VMEM)
    hbm = pl.BlockSpec(memory_space=pl.ANY)
    row = lambda v: v.reshape(1, -1)
    cap = -(-(3 * rows // n_sp) // 16) * 16
    places = n_sp * cap
    ny = n_tp // 2
    width, units = expert_gate.shape[1:]
    attend_scratch = [
        VMEM((n_sp, rows, kv_cols), BF16),
        VMEM((n_sp, heads_pad, rows), F32),
        VMEM((kva, 2 * rows, 128), BF16),
        VMEM((rows, inner + inner_b), F32),
        VMEM((heads * rows, 128), F32),
        VMEM(project_alpha.shape, BF16),
        VMEM(project_beta.shape, BF16),
        VMEM((n_tp, rows, cols), F32),
        VMEM((n_tp, rows, cols), F32),
        VMEM((n_tp, rows, cols), BF16),
        VMEM((n_tp, rows, cols), BF16),
        VMEM((n_tp, 2, 8, rows), F32),
        VMEM((n_tp, 2, 8, rows), F32),
        DMA((5,)),
        DMA((nz, nx)),
        DMA((n_sp,)),
        DMA((nz, nx)),
        DMA((n_sp,)),
        DMA((n_tp,)),
        DMA((n_tp,)),
        DMA((n_tp,)),
        DMA((n_tp,)),
        DMA((n_tp,)),
        DMA((n_tp,)),
    ]
    balanced = (nx, ny, kva, kvb) == (2, 2, nz, nz)
    tall = nx * rows
    plane_scratch = [
        VMEM((rows * kva, 128), BF16),
        VMEM((rows * kvb * 2, 128), BF16),
        VMEM((rows * kva, 128), F32),
        VMEM((rows * kvb * 2, 128), F32),
        VMEM((kva, rows, 128), BF16),
        VMEM((kvb, 2, rows, 128), BF16),
        VMEM((nz, 8, 128), F32),
        VMEM((n_sp, rows, 128), BF16),
        VMEM((2, n_sp, rows, 128), BF16),
        VMEM((n_sp, 8, 128), F32),
        VMEM((nz, 2 * tall, 128), BF16),
        VMEM((nz, 2 * tall, 128), BF16),
        VMEM((2, nz, tall, 128), F32),
        VMEM((nz, tall, 128), F32),
        VMEM((n_sp, rows, 128), BF16),
        VMEM((n_sp, rows, 128), BF16),
        VMEM(project_alpha.shape, BF16),
        VMEM(project_beta.shape, BF16),
        VMEM((ny, rows, cols), F32),
        VMEM((ny, rows, cols), F32),
        VMEM((ny, 2, rows, cols), BF16),
        VMEM((ny, 2, rows, cols), BF16),
        VMEM((2, rows, cols), BF16),
        VMEM((n_tp, 2, 8, rows), F32),
        VMEM((n_tp, 2, 8, rows), F32),
        DMA((4,)),
        DMA((3, n_sp)),
        DMA((3, n_sp)),
        DMA((n_sp,)),
        DMA((n_sp,)),
        DMA((n_tp,)),
        DMA((n_tp,)),
        DMA((n_tp,)),
        DMA((n_tp,)),
        DMA((n_tp,)),
        DMA((n_tp,)),
    ]
    expert_scratch = [
        VMEM((width, units), BF16),
        VMEM((width, units), BF16),
        VMEM((units, width), BF16),
        VMEM((n_sp, cap, cols), BF16),
        VMEM((n_tp, n_sp, cap, cols), BF16),
        VMEM((places, units), F32),
        VMEM((places, units), F32),
        VMEM((places, units), BF16),
        VMEM((ny, n_sp, cap, cols), BF16),
        VMEM((ny, n_sp, cap, cols), BF16),
        VMEM((ny, n_sp, cap, cols), BF16),
        VMEM((ny, n_sp, cap, cols), BF16),
        VMEM((ny, n_sp, cap, cols), BF16),
        VMEM((n_sp, cap, cols), BF16),
        VMEM((n_sp, cap, cols), BF16),
        VMEM((n_tp, 2, 8, rows), F32),
        DMA((3,)),
        DMA((n_sp,)),
        DMA((n_sp,)),
        DMA((ny, n_sp)),
        DMA((n_tp, n_sp)),
        DMA((ny, n_sp)),
        DMA((ny,)),
        DMA((ny,)),
        DMA((ny, n_sp)),
        DMA((ny, n_sp)),
        DMA((n_sp,)),
        DMA((n_sp,)),
        DMA((n_tp,)),
        DMA((n_tp,)),
    ]
    block = (nz, cap, cols)
    grouped_scratch = [
        VMEM((width, units), BF16),
        VMEM((width, units), BF16),
        VMEM((units, width), BF16),
        VMEM((nz * cap, rows), BF16),
        VMEM(block, BF16),
        VMEM((nz, 8, 128), F32),
        VMEM((n_sp, 8, 128), F32),
        VMEM((n_tp, 8, cols), F32),
        VMEM((n_tp, nx) + block, BF16),
        VMEM((nx, nz * cap, units), F32),
        VMEM((nx, nz * cap, units), F32),
        VMEM((places, units), BF16),
        VMEM((ny, nx) + block, BF16),
        VMEM((ny, nx) + block, BF16),
        VMEM((ny, nx) + block, BF16),
        VMEM(block, BF16),
        VMEM(block, BF16),
        VMEM(block, BF16),
        VMEM(block, BF16),
        VMEM(block, BF16),
        VMEM(block, BF16),
        VMEM(block, BF16),
        VMEM(block, BF16),
        VMEM((n_tp, 2, 8, rows), F32),
        DMA((3,)),
        DMA((nz,)),
        DMA((nz,)),
        DMA((n_sp,)),
        DMA((n_sp,)),
        DMA((n_tp,)),
        DMA((n_tp,)),
        DMA((8, nz)),
        DMA((n_tp, nx, nz)),
        DMA((ny, nx)),
        DMA((ny, nx)),
        DMA((3, nz)),
        DMA((3, nz)),
        DMA((nz,)),
        DMA((nz,)),
        DMA((n_tp,)),
        DMA((n_tp,)),
    ]
    if balanced:
        attend_scratch, expert_scratch = plane_scratch, grouped_scratch
    n_attend = len(attend_scratch)
    if balanced:
        halves = pairs_beta.reshape(rows, kvb, 2, 128).transpose(0, 2, 1, 3)
        keyed = [
            pairs_alpha.reshape(rows * kva, 128),
            halves.reshape(rows * kvb * 2, 128),
            offset_alpha.T,
            offset_beta.T,
        ]
        places_in = [vm, vm]
        routes = [expert_ids.T, route_weight.T]
    else:
        off = jnp.transpose(jnp.concatenate([offset_alpha, offset_beta], axis=1))
        off = jnp.pad(off, ((0, heads_pad - heads), (0, 0)))
        keyed = [pairs_alpha.reshape(rows, -1), pairs_beta.reshape(rows, -1), off]
        places_in = [hbm]
        routes = [jnp.concatenate([expert_ids.astype(F32), route_weight], axis=1)]
    n_in = len(keyed) + 9
    n_all = n_in + len(routes) + 5

    def kernel(*refs):
        attend_in = refs[:n_in]
        out_ref, settled = refs[n_all : n_all + 2]
        expert_in = refs[n_in:n_all]
        own = refs[n_all + 2 :]

        def attention(*hooks):
            attend = plane_attend if balanced else attend_kernel
            attend(*hooks, n_sp, n_tp, nx, kva, kvb, *attend_in, settled, *own[:n_attend])

        if balanced:
            expert_in = attend_in[-2:] + expert_in
        expert = plane_expert if balanced else expert_kernel
        expert(attention, n_sp, n_tp, nx, cap, settled, *expert_in, out_ref, *own[n_attend:])

    return pl.pallas_call(
        kernel,
        out_shape=jax.ShapeDtypeStruct((rows, cols), BF16),
        in_specs=[vm, vm, hbm, hbm] + places_in + [vm] * 3 + [hbm] * 2 + [vm] * (2 + len(routes)) + [hbm] * 3 + [vm] * 2,
        out_specs=vm,
        scratch_shapes=[VMEM((rows, cols), BF16)] + attend_scratch + expert_scratch,
        compiler_params=pltpu.CompilerParams(
            collective_id=0, has_side_effects=True, vmem_limit_bytes=60 * 1024 * 1024
        ),
    )(
        query_alpha,
        query_beta,
        *keyed,
        residual_in,
        row(gain_alpha),
        row(gain_beta),
        project_alpha,
        project_beta,
        row(gain_settle),
        row(bias_settle),
        *routes,
        expert_gate,
        expert_up,
        expert_down,
        row(gain_final),
        row(bias_final),
    )


def solution(mesh):
    in_specs = (
        P("sp", "tp"),
        P("sp", "tp"),
        P("sp", "tp", None),
        P("sp", "tp"),
        P("tp"),
        P("sp", "tp"),
        P("sp", "tp", None),
        P("sp", "tp"),
        P("tp"),
        P("tp", None),
        P("tp", None),
        P("tp"),
        P("tp"),
        P("sp", None),
        P("sp", None),
        P("sp", None, "tp"),
        P("sp", None, "tp"),
        P("sp", "tp", None),
        P("tp"),
        P("tp"),
    )
    out_specs = P("sp", "tp")
    return jax.shard_map(body, mesh=mesh, in_specs=in_specs, out_specs=out_specs, check_vma=False)
```

```python
import functools
import jax
import jax.numpy as jnp
from jax import lax
from jax.experimental import pallas as pl
from jax.experimental.pallas import tpu as pltpu
from jax.sharding import PartitionSpec as P

depth_scale = 2.0**0.5
norm_eps = 1e-05
F32 = jnp.float32
BF16 = jnp.bfloat16
VMEM = pltpu.VMEM
DMA = pltpu.SemaphoreType.DMA


def remote(src, dst, send, recv, where):
    return pltpu.make_async_remote_copy(
        src_ref=src,
        dst_ref=dst,
        send_sem=send,
        recv_sem=recv,
        device_id=where,
        device_id_type=pl.DeviceIdType.MESH,
    )


def greet(n_sp, n_tp, sp, tp):
    barrier = pltpu.get_barrier_semaphore()
    for o in range(1, n_sp):
        pl.semaphore_signal(
            barrier,
            inc=1,
            device_id={"sp": lax.rem(sp + o, n_sp), "tp": tp},
            device_id_type=pl.DeviceIdType.MESH,
        )
    for o in range(1, n_tp):
        pl.semaphore_signal(
            barrier,
            inc=1,
            device_id={"sp": sp, "tp": lax.rem(tp + o, n_tp)},
            device_id_type=pl.DeviceIdType.MESH,
        )
    pl.semaphore_wait(barrier, n_sp + n_tp - 2)


def split(x):
    high = x.astype(BF16)
    return high, (x - high.astype(F32)).astype(BF16)


def lane_sums(x):
    ones = jnp.ones((8, x.shape[1]), BF16)
    dims = (((1,), (1,)), ((), ()))
    high, low = split(x)
    return lax.dot_general(ones, high, dims, preferred_element_type=F32) + lax.dot_general(
        ones, low, dims, preferred_element_type=F32
    )


def column(row, rows):
    return jnp.transpose(jnp.broadcast_to(row[0:1, :], (rows, rows)))[:, 0:1]


def stats_start(n_tp, sp, tp, one, two, stat, send, recv, *more):
    for k, value in enumerate((one, two) + more):
        stat[tp, k] = value
    for o in range(1, n_tp):
        remote(
            stat.at[tp], stat.at[tp], send.at[o], recv.at[tp], {"sp": sp, "tp": lax.rem(tp + o, n_tp)}
        ).start()


def stats_rows(n_tp, sp, tp, stat, send, recv):
    for o in range(1, n_tp):
        peer = lax.rem(tp + o, n_tp)
        remote(stat.at[peer], stat.at[peer], send.at[o], recv.at[peer], {"sp": sp, "tp": peer}).wait_recv()
    for o in range(1, n_tp):
        peer = lax.rem(tp + o, n_tp)
        remote(stat.at[tp], stat.at[tp], send.at[o], recv.at[tp], {"sp": sp, "tp": peer}).wait_send()
    total = stat[0]
    for t in range(1, n_tp):
        total = total + stat[t]
    return total[0], total[1]


def stats_finish(n_tp, sp, tp, stat, send, recv, rows):
    one, two = stats_rows(n_tp, sp, tp, stat, send, recv)
    return column(one, rows), column(two, rows)


def norm(total, one, two, gain, bias, columns):
    mean = one / columns
    var = two / columns - mean * mean
    return ((total - mean) * lax.rsqrt(var + norm_eps) * gain + bias).astype(BF16)


def attend_kernel(
    early,
    n_sp,
    n_tp,
    nx,
    kva,
    kvb,
    qa_ref,
    qb_ref,
    kva_hbm,
    kvb_hbm,
    off_hbm,
    res_ref,
    ga_ref,
    gb_ref,
    pa_hbm,
    pb_hbm,
    gs_ref,
    bs_ref,
    out_ref,
    kvbuf,
    offbuf,
    qs,
    acc,
    rem,
    pa,
    pb,
    ya,
    yb,
    part,
    got,
    stat1,
    stat2,
    load_sem,
    kv_send,
    kv_recv,
    off_send,
    off_recv,
    part_send,
    part_recv,
    s1_send,
    s1_recv,
    s2_send,
    s2_recv,
):
    sp = lax.axis_index("sp")
    tp = lax.axis_index("tp")
    nz = n_sp // nx
    z = sp // nx
    x = lax.rem(sp, nx)
    rows = qa_ref.shape[0]
    cols = out_ref.shape[1]
    loads = (
        pltpu.make_async_copy(kva_hbm, kvbuf.at[sp, :, 0 : kva * 128], load_sem.at[0]),
        pltpu.make_async_copy(off_hbm, offbuf.at[sp], load_sem.at[1]),
        pltpu.make_async_copy(pa_hbm, pa, load_sem.at[2]),
        pltpu.make_async_copy(pb_hbm, pb, load_sem.at[3]),
        pltpu.make_async_copy(kvb_hbm, kvbuf.at[sp, :, kva * 128 :], load_sem.at[4]),
    )
    for load in loads:
        load.start()
    greet(n_sp, n_tp, sp, tp)
    lane = lax.broadcasted_iota(jnp.int32, (rows, 128), 1)
    row_i = lax.broadcasted_iota(jnp.int32, (rows, 128), 0)
    first_half = lane < 64
    for u in range(kva):
        q32 = qa_ref[:, u * 128 : (u + 1) * 128].astype(F32) * (64**-0.5)
        qs[u, 0:rows] = jnp.where(first_half, q32, 0.0).astype(BF16)
        qs[u, rows : 2 * rows] = jnp.where(first_half, pltpu.roll(q32, 64, 1), 0.0).astype(BF16)
    acc[...] = jnp.zeros_like(acc)
    rem[...] = jnp.zeros_like(rem)
    tri_r = lax.broadcasted_iota(jnp.int32, (256, 256), 0) % 128
    tri_c = lax.broadcasted_iota(jnp.int32, (256, 256), 1)
    tri = jnp.where((tri_r > tri_c) | (tri_c >= 128), 1.0, 0.0).astype(BF16)

    def block(j):
        gap = (sp - j) * rows
        valid1 = lane < row_i + gap
        valid2 = jnp.concatenate([valid1.astype(F32)] * 2, axis=0) > 0.5

        def unit(query, key, value, offset, scale, valid, left):
            s = lax.dot_general(query, key, (((1,), (1,)), ((), ())), preferred_element_type=F32)
            s = (s if scale is None else s * scale) + offset
            soft = jnp.maximum(s, 0.0) + jnp.log(1.0 + jnp.exp(-jnp.abs(s)))
            used = jnp.where(valid, soft, 0.0)
            high, low = split(used)
            sums = jnp.dot(jnp.concatenate([high, low], axis=1), tri, preferred_element_type=F32)
            w = jnp.where(valid, jnp.exp(s - soft - sums[:, :128] + left), 0.0).astype(BF16)
            return jnp.dot(w, value, preferred_element_type=F32), sums[:, 128:]

        for u in range(kva):
            pair = kvbuf[j, :, u * 128 : (u + 1) * 128]
            offset = jnp.concatenate(
                [
                    jnp.broadcast_to(offbuf[j, 2 * u : 2 * u + 1, :], (rows, 128)),
                    jnp.broadcast_to(offbuf[j, 2 * u + 1 : 2 * u + 2, :], (rows, 128)),
                ],
                axis=0,
            )
            left = rem[2 * u * rows : (2 * u + 2) * rows]
            o, total = unit(qs[u], pair, pair, offset, None, valid2, left)
            rem[2 * u * rows : (2 * u + 2) * rows] = left - total
            acc[:, u * 128 : (u + 1) * 128] += jnp.where(
                first_half, pltpu.roll(o[:rows], 64, 1), o[rows:]
            )
        for u in range(kvb):
            base = kva * 128 + u * 256
            head = 2 * kva + u
            key = kvbuf[j, :, base : base + 128]
            value = kvbuf[j, :, base + 128 : base + 256]
            offset = offbuf[j, head : head + 1, :]
            left = rem[head * rows : (head + 1) * rows]
            query = qb_ref[:, u * 128 : (u + 1) * 128]
            o, total = unit(query, key, value, offset, 128**-0.5, valid1, left)
            rem[head * rows : (head + 1) * rows] = left - total
            c = (kva + u) * 128
            acc[:, c : c + 128] += o

    def sends(s):
        j0 = (z - s) * nx + x
        plan = [(z + 1 < nz, jnp.minimum(z + 1, nz - 1) * nx + x)]
        for d in range(1, nx):
            xo = lax.rem(x + d, nx)
            plan.append(((s > 0) | (x < xo), z * nx + xo))
        made = []
        for k, (cond, dest) in enumerate(plan):
            where = {"sp": dest, "tp": tp}
            made.append(
                (
                    cond,
                    remote(kvbuf.at[j0], kvbuf.at[j0], kv_send.at[s, k], kv_recv.at[j0], where),
                    remote(offbuf.at[j0], offbuf.at[j0], off_send.at[s, k], off_recv.at[j0], where),
                )
            )
        return made

    def wait_block(j):
        where = {"sp": sp, "tp": tp}
        remote(kvbuf.at[j], kvbuf.at[j], kv_send.at[0, 0], kv_recv.at[j], where).wait_recv()
        remote(offbuf.at[j], offbuf.at[j], off_send.at[0, 0], off_recv.at[j], where).wait_recv()

    loads[0].wait()
    loads[1].wait()
    loads[4].wait()

    def forward(s):
        @pl.when(s > 0)
        def _():
            wait_block((z - s) * nx + x)

        for cond, kv_copy, off_copy in sends(s):

            @pl.when(cond)
            def _(kv_copy=kv_copy, off_copy=off_copy):
                off_copy.start()
                kv_copy.start()

    forward(0)

    def level(s, carry):
        src = z - s

        @pl.when(s < z)
        def _():
            forward(s + 1)

        def across(i, inner):
            xo = nx - 1 - i

            @pl.when((s > 0) | (xo <= x))
            def _():
                @pl.when(xo != x)
                def _():
                    wait_block(src * nx + xo)

                block(src * nx + xo)

            return inner

        return lax.fori_loop(0, nx, across, carry)

    lax.fori_loop(0, z + 1, level, 0)
    early()

    wide = kva * 128
    aa = acc[:, :wide]
    ab = acc[:, wide:]
    stats_start(n_tp, sp, tp, lane_sums(aa * aa), lane_sums(ab * ab), stat1, s1_send, s1_recv)
    loads[2].wait()
    loads[3].wait()
    na = (aa * ga_ref[...]).astype(BF16)
    nb = (ab * gb_ref[...]).astype(BF16)
    for t in range(n_tp):
        ya[t] = jnp.dot(na, pa[:, t * cols : (t + 1) * cols], preferred_element_type=F32)
        yb[t] = jnp.dot(nb, pb[:, t * cols : (t + 1) * cols], preferred_element_type=F32)
    sq_a, sq_b = stats_finish(n_tp, sp, tp, stat1, s1_send, s1_recv, rows)
    scale_a = lax.rsqrt(sq_a / (wide * n_tp) + norm_eps)
    scale_b = lax.rsqrt(sq_b / (kvb * 128 * n_tp) + norm_eps)

    def part_copy(o):
        peer = lax.rem(tp + o, n_tp)
        return remote(
            part.at[peer], got.at[tp], part_send.at[o], part_recv.at[tp], {"sp": sp, "tp": peer}
        )

    for o in range(1, n_tp):
        peer = lax.rem(tp + o, n_tp)
        part[peer] = (ya[peer] * scale_a + yb[peer] * scale_b).astype(BF16)
        part_copy(o).start()
    total = (ya[tp] * scale_a + yb[tp] * scale_b).astype(BF16).astype(F32)
    for o in range(1, n_tp):
        peer = lax.rem(tp + o, n_tp)
        remote(
            part.at[peer], got.at[peer], part_send.at[o], part_recv.at[peer], {"sp": sp, "tp": peer}
        ).wait_recv()
        total = total + got[peer].astype(F32)
    mixed = total.astype(BF16).astype(F32)
    first = depth_scale * res_ref[...].astype(F32) + mixed
    stats_start(n_tp, sp, tp, lane_sums(first), lane_sums(first * first), stat2, s2_send, s2_recv)
    for o in range(1, n_tp):
        part_copy(o).wait_send()

    def drain(s, carry):
        for cond, kv_copy, off_copy in sends(s):

            @pl.when(cond)
            def _(kv_copy=kv_copy, off_copy=off_copy):
                off_copy.wait_send()
                kv_copy.wait_send()

        return carry

    lax.fori_loop(0, z + 1, drain, 0)
    one, two = stats_finish(n_tp, sp, tp, stat2, s2_send, s2_recv, rows)
    out_ref[...] = norm(first, one, two, gs_ref[...], bs_ref[...], cols * n_tp)


def plane_attend(
    early,
    send_rows,
    send_scales,
    small_loads,
    n_sp,
    n_tp,
    nx,
    kva,
    kvb,
    qa_ref,
    qb_ref,
    pairs_a_hbm,
    pairs_b_hbm,
    offa_ref,
    offb_ref,
    res_ref,
    ga_ref,
    gb_ref,
    pa_hbm,
    pb_hbm,
    gs_ref,
    bs_ref,
    out_ref,
    raw_a,
    raw_b,
    wide_a,
    wide_b,
    own_a,
    own_b,
    own_off,
    qin,
    kin,
    oin,
    keys2,
    values2,
    left,
    acc,
    obuf,
    ain,
    pa,
    pb,
    ya,
    yb,
    part,
    got,
    across,
    stat1,
    stat2,
    load_sem,
    in_send,
    in_recv,
    o_send,
    o_recv,
    part_send,
    part_recv,
    s1_send,
    s1_recv,
    s2_send,
    s2_recv,
):
    sp = lax.axis_index("sp")
    tp = lax.axis_index("tp")
    nz = n_sp // nx
    z = sp // nx
    x = lax.rem(sp, nx)
    rows = qa_ref.shape[0]
    cols = out_ref.shape[1]
    tall = nx * rows

    def is_alpha(zz, xx):
        return lax.rem(zz + xx, 2) == 0

    loads = (
        pltpu.make_async_copy(pairs_a_hbm, raw_a, load_sem.at[0]),
        pltpu.make_async_copy(pairs_b_hbm, raw_b, load_sem.at[1]),
        pltpu.make_async_copy(pa_hbm, pa, load_sem.at[2]),
        pltpu.make_async_copy(pb_hbm, pb, load_sem.at[3]),
    )
    loads[0].start()
    loads[1].start()
    for load in small_loads:
        load.start()
    greet(n_sp, n_tp, sp, tp)
    for load in small_loads:
        load.wait()
    for u in range(nz):
        own_off[0, u] = offa_ref[2 * u : 2 * u + 2]
        own_off[1, u] = jnp.broadcast_to(offb_ref[u : u + 1], (2, 128))
    loads[0].wait()
    wide_a[...] = raw_a[...].astype(F32)
    for u in range(kva):
        own_a[u] = wide_a[pl.ds(u, rows, stride=kva), :].astype(BF16)
    loads[1].wait()
    wide_b[...] = raw_b[...].astype(F32)
    for u in range(kvb):
        for h in range(2):
            own_b[u, h] = wide_b[pl.ds(h * kvb + u, rows, stride=2 * kvb), :].astype(BF16)
    loads[2].start()
    loads[3].start()

    def in_copies(zz, xx, alpha):
        dest = zz * nx + xx
        where = {"sp": dest, "tp": tp}
        at = pl.ds(pl.multiple_of(zz * 128, 128), 128)
        q_ref = qa_ref if alpha else qb_ref
        kv = (own_a.at[zz], kin.at[0, sp]) if alpha else (own_b.at[zz], kin.at[:, sp])
        return (
            remote(own_off.at[0 if alpha else 1, zz], oin.at[sp], in_send.at[0, dest], in_recv.at[0, sp], where),
            remote(q_ref.at[:, at], qin.at[sp], in_send.at[1, dest], in_recv.at[1, sp], where),
            remote(*kv, in_send.at[2, dest], in_recv.at[2, sp], where),
        )

    def each_dest(act, low, high):
        def hop(t, carry):
            away = (t + 1) // 2
            zz = z + away * (2 * lax.rem(t, 2) - 1) * (1 - 2 * lax.rem(tp, 2))
            for xx in range(nx):
                there = (zz >= 0) & (zz < nz) & ((zz != z) | (xx != x))
                for alpha in (True, False):

                    @pl.when(there & (is_alpha(zz, xx) == alpha))
                    def _(xx=xx, alpha=alpha):
                        for copy in in_copies(zz, xx, alpha):
                            act(copy)

            return carry

        lax.fori_loop(low, high, hop, 0)

    hops = 2 * nz - 1
    each_dest(lambda copy: copy.start(), 0, hops)
    early()

    def o_copy(d):
        return remote(obuf.at[d], ain.at[sp], o_send.at[d], o_recv.at[sp], {"sp": d, "tp": tp})

    lane_t = lax.broadcasted_iota(jnp.int32, (tall, tall), 1)
    row_t = lax.broadcasted_iota(jnp.int32, (tall, tall), 0)
    lane = lax.broadcasted_iota(jnp.int32, (tall, 128), 1)
    tri = jnp.where(row_t > lane_t, 1.0, 0.0).astype(BF16)

    def attend(alpha):
        heads = 2 if alpha else 1
        scale = 64**-0.5 if alpha else 128**-0.5
        at = pl.ds(pl.multiple_of(z * 128, 128), 128)
        oin[sp] = own_off[0 if alpha else 1, z]
        if alpha:
            qin[sp] = qa_ref[:, at]
            kin[0, sp] = own_a[z]
        else:
            qin[sp] = qb_ref[:, at]
            kin[:, sp] = own_b[z]

        def arrive(p):
            for xx in range(nx):
                s = p * nx + xx

                @pl.when(s != sp)
                def _(s=s):
                    where = {"sp": sp, "tp": tp}
                    kv = kin.at[0, s] if alpha else kin.at[:, s]
                    remote(oin.at[s], oin.at[s], in_send.at[0, 0], in_recv.at[0, s], where).wait_recv()
                    remote(qin.at[s], qin.at[s], in_send.at[1, 0], in_recv.at[1, s], where).wait_recv()
                    remote(kv, kv, in_send.at[2, 0], in_recv.at[2, s], where).wait_recv()

            if alpha:
                pair = kin[0, pl.ds(p * nx, nx)].reshape(tall, 128).astype(F32)
                turned = pltpu.roll(pair, 64, 1)
                keys2[p, 0:tall] = jnp.where(lane < 64, pair, 0.0).astype(BF16)
                keys2[p, tall:] = jnp.where(lane < 64, 0.0, turned).astype(BF16)
                values2[p, 0:tall] = jnp.where(lane < 64, turned, 0.0).astype(BF16)
                values2[p, tall:] = jnp.where(lane < 64, 0.0, pair).astype(BF16)

        def step(r, c, diag):
            query = qin[pl.ds(r * nx, nx)].reshape(tall, 128)
            if alpha:
                key, value = keys2[c], values2[c]
            else:
                key = kin[0, pl.ds(c * nx, nx)].reshape(tall, 128)
                value = kin[1, pl.ds(c * nx, nx)].reshape(tall, 128)
            scores = lax.dot_general(query, key, (((1,), (1,)), ((), ())), preferred_element_type=F32)
            valid = lane_t < row_t
            ws = []
            for h in range(heads):
                row = h
                offset = jnp.concatenate([oin[c * nx + i, row : row + 1, :] for i in range(nx)], axis=1)
                s = scores[:, h * tall : (h + 1) * tall] * scale + offset
                soft = jnp.maximum(s, 0.0) + jnp.log(1.0 + jnp.exp(-jnp.abs(s)))
                used = jnp.where(valid, soft, 0.0) if diag else soft
                sums = jnp.dot(used.astype(BF16), tri, preferred_element_type=F32)
                total = jnp.broadcast_to(sums[:, 0:1] + used[:, 0:1], (tall, 128))
                e = s - soft - sums
                if diag:
                    w = jnp.where(valid, jnp.exp(e), 0.0)
                    left[h, r] = -total
                else:
                    before = left[h, r]
                    w = jnp.exp(e + jnp.concatenate([before] * nx, axis=1))
                    left[h, r] = before - total
                ws.append(w.astype(BF16))
            w = ws[0] if heads == 1 else jnp.concatenate(ws, axis=1)
            o = jnp.dot(w, value, preferred_element_type=F32)
            o = o if diag else acc[r] + o
            acc[r] = o

        def finish(r, c):
            @pl.when(c == 0)
            def _():
                obuf[pl.ds(r * nx, nx)] = acc[r].astype(BF16).reshape(nx, rows, 128)
                for xx in range(nx):
                    d = r * nx + xx

                    @pl.when(d != sp)
                    def _(d=d):
                        o_copy(d).start()

                    @pl.when(d == sp)
                    def _(d=d):
                        ain[sp] = obuf[d]

        def phase(k, span):
            low, high = span
            lower_half = z < nz // 2
            up = jnp.where(lower_half, low == 0, high < nz - 1).astype(jnp.int32)
            first = (k == 0).astype(jnp.int32)
            p = first * z + (1 - first) * (up * (high + 1) + (1 - up) * (low - 1))

            arrive(p)


            def at(t):
                return p + t * (1 - up), p - t * up

            @pl.when(k == 0)
            def _():
                step(p, p, True)
                finish(p, p)

            @pl.when(k > 0)
            def _():
                step(p, p, True)
                step(*at(1), False)
                finish(p, p)
                finish(*at(1))

            def two(i, carry):
                step(*at(2 * i), False)
                step(*at(2 * i + 1), False)
                finish(*at(2 * i))
                finish(*at(2 * i + 1))
                return carry

            lax.fori_loop(1, (k + 1) // 2, two, 0)

            @pl.when((k > 0) & (lax.rem(k, 2) == 0))
            def _():
                step(*at(k), False)
                finish(*at(k))

            return jnp.minimum(low, p), jnp.maximum(high, p)

        lax.fori_loop(0, nz, phase, (z, z))

    for alpha in (True, False):

        @pl.when(is_alpha(z, x) == alpha)
        def _(alpha=alpha):
            attend(alpha)

    def o_wait(j, carry):
        @pl.when(j != sp)
        def _():
            remote(obuf.at[j], ain.at[j], o_send.at[0], o_recv.at[j], {"sp": sp, "tp": tp}).wait_recv()

        return carry

    lax.fori_loop(0, n_sp, o_wait, 0)
    wide = kva * 128
    aa = jnp.concatenate([ain[k * nx + k % 2] for k in range(nz)], axis=1).astype(F32)
    ab = jnp.concatenate([ain[k * nx + 1 - k % 2] for k in range(nz)], axis=1).astype(F32)
    stats_start(n_tp, sp, tp, lane_sums(aa * aa), lane_sums(ab * ab), stat1, s1_send, s1_recv)
    loads[2].wait()
    loads[3].wait()
    core = lax.rem(tp, 2)
    y = tp // 2
    sides = ((1 - y) * 2, y * 2)
    to_mate = {"sp": sp, "tp": y * 2 + 1 - core}
    to_far = {"sp": sp, "tp": (1 - y) * 2 + core}
    na = (aa * ga_ref[...]).astype(BF16)
    nb = (ab * gb_ref[...]).astype(BF16)

    def project(t):
        at = pl.ds(pl.multiple_of(t * cols, 128), cols)
        return (
            jnp.dot(na, pa[:, at], preferred_element_type=F32),
            jnp.dot(nb, pb[:, at], preferred_element_type=F32),
        )

    def mate_copy(k):
        return remote(part.at[k], got.at[k], part_send.at[k], part_recv.at[k], to_mate)

    for k in range(2):
        a, b = project(sides[k] + 1 - core)
        part[k, 0] = a.astype(BF16)
        part[k, 1] = b.astype(BF16)
        mate_copy(k).start()
    for k in range(2):
        ya[k], yb[k] = project(sides[k] + core)
    sq_a, sq_b = stats_finish(n_tp, sp, tp, stat1, s1_send, s1_recv, rows)
    scale_a = lax.rsqrt(sq_a / (wide * n_tp) + norm_eps)
    scale_b = lax.rsqrt(sq_b / (kvb * 128 * n_tp) + norm_eps)

    def chip_sum(k):
        mate_copy(k).wait_recv()
        return (ya[k] + got[k, 0].astype(F32)) * scale_a + (yb[k] + got[k, 1].astype(F32)) * scale_b

    half = cols // 2
    across[0] = chip_sum(0).astype(BF16)

    def far_copy(k):
        at = slice(k * half, (k + 1) * half)
        return remote(
            across.at[0, :, at], across.at[1, :, at], part_send.at[2 + k], part_recv.at[2 + k], to_far
        )

    far_copy(0).start()
    far_copy(1).start()
    total = chip_sum(1)
    residual = depth_scale * res_ref[...].astype(F32)
    firsts, sums, squares = [], [], []
    for k in range(2):
        at = slice(k * half, (k + 1) * half)
        far_copy(k).wait_recv()
        mixed = (total[:, at] + across[1, :, at].astype(F32)).astype(BF16).astype(F32)
        firsts.append(residual[:, at] + mixed)
        sums.append(lane_sums(firsts[k]))
        squares.append(lane_sums(firsts[k] * firsts[k]))
        if k == 0:
            centre = sums[0] / half
            middle = column(centre, rows)
        else:
            stats_start(n_tp, sp, tp, sums[0] + sums[1], squares[0] + squares[1], stat2, s2_send, s2_recv, centre)
        send_rows((firsts[k] - middle).astype(BF16), k)
    first = jnp.concatenate(firsts, axis=1)
    for k in range(2):
        far_copy(k).wait_send()
        mate_copy(k).wait_send()
    each_dest(lambda copy: copy.wait_send(), 0, hops)

    def o_drain(j, carry):
        @pl.when(j != sp)
        def _():
            o_copy(j).wait_send()

        return carry

    lax.fori_loop(0, n_sp, o_drain, 0)
    one, two = stats_rows(n_tp, sp, tp, stat2, s2_send, s2_recv)
    mean = one / (cols * n_tp)
    factor = lax.rsqrt(two / (cols * n_tp) - mean * mean + norm_eps)
    centres = [stat2[t, 2] for t in range(n_tp)]
    shifts = [(centres[t] - mean) * factor for t in range(n_tp)]
    send_scales([factor] + shifts)
    flat = (first - column(mean, rows)) * column(factor, rows)
    out_ref[...] = (flat * gs_ref[...] + bs_ref[...]).astype(BF16)


def expert_kernel(
    attention,
    n_sp,
    n_tp,
    nx,
    cap,
    set_ref,
    ids_ref,
    wg_hbm,
    wu_hbm,
    wd_hbm,
    gf_ref,
    bf_ref,
    out_ref,
    wg,
    wu,
    wd,
    sendbuf,
    xbuf,
    gate,
    up,
    hid,
    away,
    arrived,
    home,
    pre,
    peers,
    outb,
    back,
    stat,
    load_sem,
    a_send,
    a_recv,
    x_send,
    x_recv,
    relay_send,
    d_send,
    d_recv,
    y_send,
    y_recv,
    b_send,
    b_recv,
    s_send,
    s_recv,
):
    sp = lax.axis_index("sp")
    tp = lax.axis_index("tp")
    rows, cols = set_ref.shape
    places = n_sp * cap
    ny = n_tp // 2
    y = tp // 2
    core = lax.rem(tp, 2)
    mate = y * 2 + 1 - core
    loads = (
        pltpu.make_async_copy(wg_hbm.at[0], wg, load_sem.at[0]),
        pltpu.make_async_copy(wu_hbm.at[0], wu, load_sem.at[1]),
        pltpu.make_async_copy(wd_hbm.at[0], wd, load_sem.at[2]),
    )

    def loop(low, high, fn):
        def step(i, carry):
            fn(i)
            return carry

        lax.fori_loop(low, high, step, 0)

    def x_copies(j):
        made = []
        for k in range(ny):
            dest = mate if k == 0 else lax.rem(y + k, ny) * 2 + core
            made.append(
                remote(
                    xbuf.at[tp, j], xbuf.at[tp, j], x_send.at[k, j], x_recv.at[tp, j], {"sp": sp, "tp": dest}
                )
            )
        return made

    def spread_out(j):
        @pl.when(j != sp)
        def _():
            remote(
                sendbuf.at[j], xbuf.at[tp, j], a_send.at[0], a_recv.at[j], {"sp": sp, "tp": tp}
            ).wait_recv()

        for copy in x_copies(j):
            copy.start()

    ahead = jnp.maximum(sp // nx - 1, 0) * nx

    for load in loads:
        load.start()
    attention(lambda: loop(0, ahead, spread_out))
    ids = ids_ref[...][:, 0:2]
    expert = lax.broadcasted_iota(jnp.int32, (rows, 128), 1).astype(F32)
    hot = [jnp.where(ids[:, k : k + 1] == expert, 1.0, 0.0) for k in range(2)]
    r = lax.broadcasted_iota(jnp.int32, (rows, rows), 0)
    c = lax.broadcasted_iota(jnp.int32, (rows, rows), 1)
    lower = jnp.where(c < r, 1.0, 0.0).astype(BF16)
    before = jnp.dot(lower, (hot[0] + hot[1]).astype(BF16), preferred_element_type=F32)
    seat = lax.broadcasted_iota(jnp.int32, (rows, places), 1).astype(F32)
    hits = []
    for k in range(2):
        slot = jnp.sum(before * hot[k], axis=1, keepdims=True)
        place = ids[:, k : k + 1] * cap + slot
        hits.append(jnp.where(place == seat, 1.0, 0.0))
    spread = jnp.transpose(hits[0] + hits[1]).astype(BF16)
    sent = jnp.dot(spread, set_ref[...], preferred_element_type=F32).astype(BF16)
    sendbuf[...] = sent.reshape(n_sp, cap, cols)

    def at_sp(o):
        return lax.rem(sp + o, n_sp)

    def a_copy(o):
        dest = at_sp(o)
        return remote(
            sendbuf.at[dest], xbuf.at[tp, sp], a_send.at[o], a_recv.at[sp], {"sp": dest, "tp": tp}
        )

    loop(1, n_sp, lambda o: a_copy(o).start())
    xbuf[tp, sp] = sendbuf[sp]

    def x_wait(t, j):
        remote(xbuf.at[t, j], xbuf.at[t, j], x_send.at[0, 0], x_recv.at[t, j], {"sp": sp, "tp": t}).wait_recv()

    loop(ahead, n_sp, spread_out)

    def relay_copy(k, o):
        t = lax.rem(y + k, ny) * 2 + core
        j = o
        return remote(
            xbuf.at[t, j], xbuf.at[t, j], relay_send.at[k, o], x_recv.at[t, j], {"sp": sp, "tp": mate}
        )

    def gather_dot(t, fresh):
        xs = xbuf[t].reshape(places, cols)
        at = pl.ds(pl.multiple_of(t * cols, 128), cols)
        g = jnp.dot(xs, wg[at, :], preferred_element_type=F32)
        u = jnp.dot(xs, wu[at, :], preferred_element_type=F32)
        if fresh:
            gate[...] = g
            up[...] = u
        else:
            gate[...] += g
            up[...] += u

    loads[0].wait()
    loads[1].wait()
    gather_dot(tp, True)

    def arrive_mate(o):
        x_wait(mate, o)

    loop(0, n_sp, arrive_mate)
    gather_dot(mate, False)

    def from_y(k):
        t = lax.rem(y + k, ny) * 2 + core
        other = lax.rem(y + k, ny) * 2 + 1 - core

        def pass_on(o):
            x_wait(t, o)
            relay_copy(k, o).start()

        loop(0, n_sp, pass_on)
        gather_dot(t, False)

        def arrive(o):
            x_wait(other, o)

        loop(0, n_sp, arrive)
        gather_dot(other, False)

    loop(1, ny, from_y)
    value = gate[...]
    hid[...] = (value / (1.0 + jnp.exp(-value)) * up[...]).astype(BF16)
    loads[2].wait()

    def down(t):
        at = pl.ds(pl.multiple_of(t * cols, 128), cols)
        result = jnp.dot(hid[...], wd[:, at], preferred_element_type=F32)
        return result.astype(BF16).reshape(n_sp, cap, cols)

    def d_copy(k):
        return remote(away.at[k], arrived.at[k], d_send.at[k], d_recv.at[k], {"sp": sp, "tp": mate})

    def down_away(i):
        k = lax.rem(i + 1, ny)
        away[k] = down(lax.rem(y + k, ny) * 2 + 1 - core)
        d_copy(k).start()

    loop(0, ny, down_away)

    def down_home(i):
        k = lax.rem(i + 1, ny)
        home[k] = down(lax.rem(y + k, ny) * 2 + core)

    loop(0, ny, down_home)

    def y_copy(k, o):
        j = at_sp(o)
        return remote(
            pre.at[k, j],
            peers.at[k, j],
            y_send.at[k, o],
            y_recv.at[k, j],
            {"sp": sp, "tp": lax.rem(y + k, ny) * 2 + core},
        )

    for i in range(ny):
        k = (i + 1) % ny
        d_copy(k).wait_recv()
        if k:

            def to_y(o, k=k):
                j = at_sp(o)
                pre[k, j] = (home[k, j].astype(F32) + arrived[k, j].astype(F32)).astype(BF16)
                y_copy(k, o).start()

            loop(1, n_sp, to_y)
            to_y(0)

    def b_copy(o):
        dest = at_sp(o)
        return remote(outb.at[dest], back.at[sp], b_send.at[o], b_recv.at[sp], {"sp": dest, "tp": tp})

    def settle(o):
        j = at_sp(o)
        total = home[0, j].astype(F32) + arrived[0, j].astype(F32)
        for k in range(1, ny):
            remote(
                pre.at[k, j], peers.at[k, j], y_send.at[k, 0], y_recv.at[k, j], {"sp": sp, "tp": mate}
            ).wait_recv()
            total = total + peers[k, j].astype(F32)
        return total.astype(BF16)

    def give_back(o):
        outb[at_sp(o)] = settle(o)
        b_copy(o).start()

    loop(1, n_sp, give_back)
    back[sp] = settle(0)

    def wait_back(o):
        j = lax.rem(sp - o + n_sp, n_sp)
        remote(outb.at[j], back.at[j], b_send.at[0], b_recv.at[j], {"sp": j, "tp": tp}).wait_recv()

    loop(1, n_sp, wait_back)
    flat = back[...].reshape(places, cols)
    weight = ids_ref[...][:, 2:4]
    routed = weight[:, 0:1] * jnp.dot(hits[0].astype(BF16), flat, preferred_element_type=F32)
    routed = routed + weight[:, 1:2] * jnp.dot(hits[1].astype(BF16), flat, preferred_element_type=F32)
    second = depth_scale * set_ref[...].astype(F32) + routed
    stats_start(n_tp, sp, tp, lane_sums(second), lane_sums(second * second), stat, s_send, s_recv)

    def drain(o):
        for copy in x_copies(o):
            copy.wait_send()
        for k in range(1, ny):
            relay_copy(k, o).wait_send()
            y_copy(k, o).wait_send()

    loop(0, n_sp, drain)

    def drain_sp(o):
        a_copy(o).wait_send()
        b_copy(o).wait_send()

    loop(1, n_sp, drain_sp)
    for k in range(ny):
        d_copy(k).wait_send()
    one, two = stats_finish(n_tp, sp, tp, stat, s_send, s_recv, rows)
    out_ref[...] = norm(second, one, two, gf_ref[...], bf_ref[...], cols * n_tp)


def plane_expert(
    attention,
    n_sp,
    n_tp,
    nx,
    cap,
    set_ref,
    gs_ref,
    bs_ref,
    ids_ref,
    weight_ref,
    wg_hbm,
    wu_hbm,
    wd_hbm,
    gf_ref,
    bf_ref,
    out_ref,
    wg,
    wu,
    wd,
    hits,
    packed,
    scales,
    scaled,
    affine,
    xbuf,
    gate,
    up,
    hid,
    away,
    arrived,
    home,
    mid,
    midx,
    midy,
    gotd,
    gotx,
    goty,
    outb,
    back,
    stat,
    load_sem,
    a_send,
    a_recv,
    t_send,
    t_recv,
    g_send,
    g_recv,
    x_send,
    x_recv,
    d_send,
    d_recv,
    m_send,
    m_recv,
    b_send,
    b_recv,
    s_send,
    s_recv,
):
    sp = lax.axis_index("sp")
    tp = lax.axis_index("tp")
    rows, cols = set_ref.shape
    nz = n_sp // nx
    z = sp // nx
    x = lax.rem(sp, nx)
    core = lax.rem(tp, 2)
    y = tp // 2
    mate = y * 2 + 1 - core
    far = (1 - y) * 2 + core
    far_mate = (1 - y) * 2 + 1 - core
    to_mate = {"sp": sp, "tp": mate}
    to_x = {"sp": z * nx + 1 - x, "tp": tp}
    to_y = {"sp": sp, "tp": far}
    table = [sorted(range(nz), key=lambda g: (abs(g - a), (g - a) * (1 if a < nz // 2 else -1))) for a in range(nz)]

    def near(i):
        pick = table[0][i]
        for a in range(1, nz):
            pick = jnp.where(z == a, table[a][i], pick)
        return pick

    loads = (
        pltpu.make_async_copy(wg_hbm.at[0], wg, load_sem.at[0]),
        pltpu.make_async_copy(wu_hbm.at[0], wu, load_sem.at[1]),
        pltpu.make_async_copy(wd_hbm.at[0], wd, load_sem.at[2]),
    )

    def g_copy(o):
        where = {"sp": sp, "tp": lax.rem(tp + o, n_tp)}
        return remote(affine.at[tp], affine.at[tp], g_send.at[o], g_recv.at[tp], where)

    def others(fn):
        def one(d, carry):
            @pl.when(d != sp)
            def _():
                fn(d)

            return carry

        lax.fori_loop(0, n_sp, one, 0)

    def early():
        for load in loads:
            load.start()
        affine[tp, 0:1] = gs_ref[...]
        affine[tp, 1:2] = bs_ref[...]
        for o in range(1, n_tp):
            g_copy(o).start()
        ids = [ids_ref[k : k + 1, :] for k in range(2)]
        r = lax.broadcasted_iota(jnp.int32, (rows, rows), 0)
        c = lax.broadcasted_iota(jnp.int32, (rows, rows), 1)
        upper = jnp.where(r < c, 1.0, 0.0).astype(BF16)
        group = lax.broadcasted_iota(jnp.int32, (8, rows), 0) * nx
        hot = jnp.where((ids[0] >= group) & (ids[0] < group + nx), 1.0, 0.0)
        before = jnp.dot(hot.astype(BF16), upper, preferred_element_type=F32)
        seat = lax.broadcasted_iota(jnp.int32, (cap, rows), 0).astype(F32)
        for g in range(nz):
            match = jnp.where(seat == before[g : g + 1], hot[g : g + 1], 0.0).astype(BF16)
            hits[g * cap : (g + 1) * cap] = match
            scales[g] = jnp.zeros((8, 128), F32)

    def a_copy(i, k):
        g = near(i)
        at = slice(k * half, (k + 1) * half)
        return remote(
            packed.at[g, :, at],
            xbuf.at[tp, x, z, :, at],
            a_send.at[k, i],
            a_recv.at[k, z],
            {"sp": g * nx + x, "tp": tp},
        )

    def t_copy(d):
        return remote(scales.at[d // nx], scaled.at[sp], t_send.at[d], t_recv.at[sp], {"sp": d, "tp": tp})

    half = cols // 2

    def send_rows(part, k):
        sent = jnp.dot(hits[...], part, preferred_element_type=F32).astype(BF16)
        at = slice(k * half, (k + 1) * half)
        packed[:, :, at] = sent.reshape(nz, cap, half)
        for i in range(1, nz):
            a_copy(i, k).start()
        xbuf[tp, x, z, :, at] = packed[z, :, at]

    def compact(lines, g):
        line = lax.broadcasted_iota(jnp.int32, (8, rows), 0)
        tile = jnp.zeros((8, rows), F32)
        for k, value in enumerate(lines):
            tile = jnp.where(line == k, value, tile)
        high, low = split(tile)
        dims = (((1,), (1,)), ((), ()))
        match = hits[g * cap : (g + 1) * cap]
        return lax.dot_general(high, match, dims, preferred_element_type=F32) + lax.dot_general(
            low, match, dims, preferred_element_type=F32
        )

    def send_scales(lines):
        for g in range(nz):
            share = []
            for e in range(nx):
                chosen = [
                    jnp.where(ids_ref[k : k + 1, :] == g * nx + e, weight_ref[k : k + 1, :], 0.0) for k in range(2)
                ]
                share.append(chosen[0] + chosen[1])
            scales[g, :, 0:cap] = compact(lines + share, g)
        others(lambda d: t_copy(d).start())
        scaled[sp] = scales[z]

    def x_copy(kind, t, xs, g, where):
        block = xbuf.at[t, xs, g]
        return remote(block, block, x_send.at[kind, g], x_recv.at[t, xs, g], where)

    def x_wait(t, xs, g):
        block = xbuf.at[t, xs, g]
        remote(block, block, x_send.at[0, 0], x_recv.at[t, xs, g], to_mate).wait_recv()

    def when_x_first(g, fn):
        pl.when(lax.rem(g, 2) == 0)(fn)

    def when_y_first(g, fn):
        pl.when(lax.rem(g, 2) == 1)(fn)

    def own_out(i):
        g = near(i)
        if i:
            for k in range(2):
                block = xbuf.at[tp, x, g, :, k * half : (k + 1) * half]
                remote(block, block, a_send.at[0, 0], a_recv.at[k, g], to_mate).wait_recv()
        x_copy(1, tp, x, g, to_x).start()
        x_copy(2, tp, x, g, to_y).start()
        x_copy(0, tp, x, g, to_mate).start()

    def pass_on(i):
        g = near(i)
        x_wait(tp, 1 - x, g)
        when_x_first(g, lambda: x_copy(4, tp, 1 - x, g, to_y).start())
        x_copy(3, tp, 1 - x, g, to_mate).start()
        x_wait(far, x, g)
        when_y_first(g, lambda: x_copy(6, far, x, g, to_x).start())
        x_copy(5, far, x, g, to_mate).start()

    def pass_diag(i):
        g = near(i)
        x_wait(far, 1 - x, g)
        x_copy(7, far, 1 - x, g, to_mate).start()

    def t_wait(j):
        remote(scaled.at[j], scaled.at[j], t_send.at[0], t_recv.at[j], to_mate).wait_recv()

    def piece(t, xs, fresh):
        factor, shift = [], []
        for g in range(nz):
            j = g * nx + xs
            factor.append(scaled[j, 0:1, :])
            shift.append(scaled[j, pl.ds(1 + t, 1), :])
        turned = jnp.transpose(jnp.concatenate(factor + shift, axis=0))
        gain, bias = affine[t, 0:1, :], affine[t, 1:2, :]
        block = jnp.concatenate(
            [
                (
                    (xbuf[t, xs, g].astype(F32) * turned[0:cap, g : g + 1] + turned[0:cap, nz + g : nz + g + 1]) * gain
                    + bias
                ).astype(BF16)
                for g in range(nz)
            ],
            axis=0,
        )
        at = pl.ds(pl.multiple_of(t * cols, 128), cols)
        g = jnp.dot(block, wg[at, :], preferred_element_type=F32)
        u = jnp.dot(block, wu[at, :], preferred_element_type=F32)
        if fresh:
            gate[xs] = g
            up[xs] = u
        else:
            gate[xs] += g
            up[xs] += u

    def all_in(t, xs):
        def one(g, carry):
            x_wait(t, xs, g)
            return carry

        lax.fori_loop(0, nz, one, 0)

    def first_rows(part, k):
        send_rows(part, k)
        if k == 1:
            own_out(0)
            own_out(1)
            pass_on(0)

    attention(early, first_rows, send_scales)
    for i in range(2, nz):
        own_out(i)
        if i < nz - 1:
            pass_on(i - 1)
            pass_diag(i - 2)
    loads[0].wait()
    loads[1].wait()
    others(t_wait)
    for o in range(1, n_tp):
        peer = lax.rem(tp + o, n_tp)
        remote(affine.at[peer], affine.at[peer], g_send.at[0], g_recv.at[peer], to_mate).wait_recv()
    piece(tp, x, True)
    pass_on(nz - 2)
    pass_diag(nz - 3)
    all_in(mate, x)
    piece(mate, x, False)
    pass_on(nz - 1)
    pass_diag(nz - 2)
    piece(tp, 1 - x, True)
    piece(far, x, False)
    pass_diag(nz - 1)
    all_in(far_mate, x)
    piece(far_mate, x, False)
    all_in(mate, 1 - x)
    piece(mate, 1 - x, False)
    piece(far, 1 - x, False)
    all_in(far_mate, 1 - x)
    piece(far_mate, 1 - x, False)
    for xs in range(nx):
        value = gate[xs]
        line = [scaled[g * nx + xs, pl.ds(1 + n_tp + x, 1), :] for g in range(nz)]
        turned = jnp.transpose(jnp.concatenate(line + line, axis=0))
        weight = jnp.concatenate([turned[0:cap, g : g + 1] for g in range(nz)], axis=0)
        hid[xs * nz * cap : (xs + 1) * nz * cap] = (value / (1.0 + jnp.exp(-value)) * up[xs] * weight).astype(BF16)
    loads[2].wait()

    def down(t):
        at = pl.ds(pl.multiple_of(t * cols, 128), cols)
        result = jnp.dot(hid[...], wd[:, at], preferred_element_type=F32)
        return result.astype(BF16).reshape(nx, nz, cap, cols)

    def d_copy(k, xs):
        return remote(away.at[k, xs], arrived.at[k, xs], d_send.at[k, xs], d_recv.at[k, xs], to_mate)

    away[1] = down(far_mate)
    d_copy(1, 1 - x).start()
    d_copy(1, x).start()
    away[0] = down(mate)
    d_copy(0, 1 - x).start()
    d_copy(0, x).start()
    home[1] = down(far)

    def pair(k, xs, g):
        return home[k, xs, g].astype(F32) + arrived[k, xs, g].astype(F32)

    def m_copy(kind, src, dst, g, where):
        return remote(src.at[g], dst.at[g], m_send.at[kind, g], m_recv.at[kind, g], where)

    def diag_copy(g, where):
        return m_copy(0, mid, gotd, g, where)

    def x_send_copy(g):
        return m_copy(1, midx, gotx, g, to_x)

    def y_send_copy(g):
        return m_copy(2, midy, goty, g, to_y)

    order = range(nz - 1, -1, -1)
    late = order[nz // 2 :]

    def plain(i):
        g = near(i)

        def plain_x():
            midx[g] = pair(0, 1 - x, g).astype(BF16)
            x_send_copy(g).start()

        def plain_y():
            midy[g] = pair(1, x, g).astype(BF16)
            y_send_copy(g).start()

        when_x_first(g, plain_x)
        when_y_first(g, plain_y)

    def joined(i):
        g = near(i)
        diag_copy(g, to_mate).wait_recv()

        def joined_y():
            midy[g] = (pair(1, x, g) + gotd[g].astype(F32)).astype(BF16)
            y_send_copy(g).start()

        def joined_x():
            midx[g] = (pair(0, 1 - x, g) + gotd[g].astype(F32)).astype(BF16)
            x_send_copy(g).start()

        when_x_first(g, joined_y)
        when_y_first(g, joined_x)

    def diagonal(i):
        g = near(i)
        mid[g] = pair(1, 1 - x, g).astype(BF16)
        when_x_first(g, lambda: diag_copy(g, to_x).start())
        when_y_first(g, lambda: diag_copy(g, to_y).start())

    d_copy(1, 1 - x).wait_recv()
    for i in order:
        diagonal(i)
    home[0] = down(tp)
    d_copy(1, x).wait_recv()
    d_copy(0, 1 - x).wait_recv()
    for i in order[: nz // 2]:
        plain(i)
    for i in order[: nz // 2]:
        joined(i)
    for i in late:
        plain(i)
    for i in late:
        joined(i)

    def b_copy(i):
        g = near(i)
        return remote(outb.at[g], back.at[z], b_send.at[i], b_recv.at[z], {"sp": g * nx + x, "tp": tp})

    d_copy(0, x).wait_recv()
    for i in order:
        g = near(i)
        x_send_copy(g).wait_recv()
        y_send_copy(g).wait_recv()
        total = (pair(0, x, g) + gotx[g].astype(F32) + goty[g].astype(F32)).astype(BF16)
        if i:
            outb[g] = total
            b_copy(i).start()
        else:
            back[z] = total
    for i in range(1, nz):
        g = near(i)
        remote(outb.at[g], back.at[g], b_send.at[0], b_recv.at[g], to_mate).wait_recv()
    flat = back[...].reshape(nz * cap, cols)
    routed = lax.dot_general(hits[...], flat, (((0,), (0,)), ((), ())), preferred_element_type=F32)
    second = depth_scale * set_ref[...].astype(F32) + routed
    stats_start(n_tp, sp, tp, lane_sums(second), lane_sums(second * second), stat, s_send, s_recv)
    others(lambda d: t_copy(d).wait_send())
    for o in range(1, n_tp):
        g_copy(o).wait_send()
    for i in range(nz):
        g = near(i)
        if i:
            a_copy(i, 0).wait_send()
            a_copy(i, 1).wait_send()
            b_copy(i).wait_send()
        x_copy(1, tp, x, g, to_x).wait_send()
        x_copy(2, tp, x, g, to_y).wait_send()
        for kind in (0, 3, 5, 7):
            x_copy(kind, tp, x, g, to_mate).wait_send()
        when_x_first(g, lambda g=g: x_copy(4, tp, 1 - x, g, to_y).wait_send())
        when_y_first(g, lambda g=g: x_copy(6, far, x, g, to_x).wait_send())
        diag_copy(g, to_mate).wait_send()
        x_send_copy(g).wait_send()
        y_send_copy(g).wait_send()
    for k in range(2):
        d_copy(k, 0).wait_send()
        d_copy(k, 1).wait_send()
    one, two = stats_finish(n_tp, sp, tp, stat, s_send, s_recv, rows)
    out_ref[...] = norm(second, one, two, gf_ref[...], bf_ref[...], cols * n_tp)


def body(
    residual_in,
    query_alpha,
    pairs_alpha,
    offset_alpha,
    gain_alpha,
    query_beta,
    pairs_beta,
    offset_beta,
    gain_beta,
    project_alpha,
    project_beta,
    gain_settle,
    bias_settle,
    expert_ids,
    route_weight,
    expert_gate,
    expert_up,
    expert_down,
    gain_final,
    bias_final,
):
    n_sp = lax.axis_size("sp")
    n_tp = lax.axis_size("tp")
    nx = 2 ** ((n_sp.bit_length() - 1) // 2)
    nz = n_sp // nx
    rows, cols = residual_in.shape
    kva = pairs_alpha.shape[1]
    kvb = pairs_beta.shape[1]
    heads = 2 * kva + kvb
    heads_pad = -(-heads // 8) * 8
    kv_cols = kva * 128 + kvb * 256
    inner = kva * 128
    inner_b = kvb * 128
    vm = pl.BlockSpec(memory_space=VMEM)
    hbm = pl.BlockSpec(memory_space=pl.ANY)
    row = lambda v: v.reshape(1, -1)
    cap = -(-(3 * rows // n_sp) // 16) * 16
    places = n_sp * cap
    ny = n_tp // 2
    width, units = expert_gate.shape[1:]
    attend_scratch = [
        VMEM((n_sp, rows, kv_cols), BF16),
        VMEM((n_sp, heads_pad, rows), F32),
        VMEM((kva, 2 * rows, 128), BF16),
        VMEM((rows, inner + inner_b), F32),
        VMEM((heads * rows, 128), F32),
        VMEM(project_alpha.shape, BF16),
        VMEM(project_beta.shape, BF16),
        VMEM((n_tp, rows, cols), F32),
        VMEM((n_tp, rows, cols), F32),
        VMEM((n_tp, rows, cols), BF16),
        VMEM((n_tp, rows, cols), BF16),
        VMEM((n_tp, 2, 8, rows), F32),
        VMEM((n_tp, 2, 8, rows), F32),
        DMA((5,)),
        DMA((nz, nx)),
        DMA((n_sp,)),
        DMA((nz, nx)),
        DMA((n_sp,)),
        DMA((n_tp,)),
        DMA((n_tp,)),
        DMA((n_tp,)),
        DMA((n_tp,)),
        DMA((n_tp,)),
        DMA((n_tp,)),
    ]
    balanced = (nx, ny, kva, kvb) == (2, 2, nz, nz)
    tall = nx * rows
    plane_scratch = [
        VMEM((rows * kva, 128), BF16),
        VMEM((rows * kvb * 2, 128), BF16),
        VMEM((rows * kva, 128), F32),
        VMEM((rows * kvb * 2, 128), F32),
        VMEM((kva, rows, 128), BF16),
        VMEM((kvb, 2, rows, 128), BF16),
        VMEM((2, nz, 2, 128), F32),
        VMEM((n_sp, rows, 128), BF16),
        VMEM((2, n_sp, rows, 128), BF16),
        VMEM((n_sp, 2, 128), F32),
        VMEM((nz, 2 * tall, 128), BF16),
        VMEM((nz, 2 * tall, 128), BF16),
        VMEM((2, nz, tall, 128), F32),
        VMEM((nz, tall, 128), F32),
        VMEM((n_sp, rows, 128), BF16),
        VMEM((n_sp, rows, 128), BF16),
        VMEM(project_alpha.shape, BF16),
        VMEM(project_beta.shape, BF16),
        VMEM((ny, rows, cols), F32),
        VMEM((ny, rows, cols), F32),
        VMEM((ny, 2, rows, cols), BF16),
        VMEM((ny, 2, rows, cols), BF16),
        VMEM((2, rows, cols), BF16),
        VMEM((n_tp, 2, 8, rows), F32),
        VMEM((n_tp, 3, 8, rows), F32),
        DMA((4,)),
        DMA((3, n_sp)),
        DMA((3, n_sp)),
        DMA((n_sp,)),
        DMA((n_sp,)),
        DMA((n_tp,)),
        DMA((n_tp,)),
        DMA((n_tp,)),
        DMA((n_tp,)),
        DMA((n_tp,)),
        DMA((n_tp,)),
    ]
    expert_scratch = [
        VMEM((width, units), BF16),
        VMEM((width, units), BF16),
        VMEM((units, width), BF16),
        VMEM((n_sp, cap, cols), BF16),
        VMEM((n_tp, n_sp, cap, cols), BF16),
        VMEM((places, units), F32),
        VMEM((places, units), F32),
        VMEM((places, units), BF16),
        VMEM((ny, n_sp, cap, cols), BF16),
        VMEM((ny, n_sp, cap, cols), BF16),
        VMEM((ny, n_sp, cap, cols), BF16),
        VMEM((ny, n_sp, cap, cols), BF16),
        VMEM((ny, n_sp, cap, cols), BF16),
        VMEM((n_sp, cap, cols), BF16),
        VMEM((n_sp, cap, cols), BF16),
        VMEM((n_tp, 2, 8, rows), F32),
        DMA((3,)),
        DMA((n_sp,)),
        DMA((n_sp,)),
        DMA((ny, n_sp)),
        DMA((n_tp, n_sp)),
        DMA((ny, n_sp)),
        DMA((ny,)),
        DMA((ny,)),
        DMA((ny, n_sp)),
        DMA((ny, n_sp)),
        DMA((n_sp,)),
        DMA((n_sp,)),
        DMA((n_tp,)),
        DMA((n_tp,)),
    ]
    block = (nz, cap, cols)
    grouped_scratch = [
        VMEM((width, units), BF16),
        VMEM((width, units), BF16),
        VMEM((units, width), BF16),
        VMEM((nz * cap, rows), BF16),
        VMEM(block, BF16),
        VMEM((nz, 8, 128), F32),
        VMEM((n_sp, 8, 128), F32),
        VMEM((n_tp, 8, cols), F32),
        VMEM((n_tp, nx) + block, BF16),
        VMEM((nx, nz * cap, units), F32),
        VMEM((nx, nz * cap, units), F32),
        VMEM((places, units), BF16),
        VMEM((ny, nx) + block, BF16),
        VMEM((ny, nx) + block, BF16),
        VMEM((ny, nx) + block, BF16),
        VMEM(block, BF16),
        VMEM(block, BF16),
        VMEM(block, BF16),
        VMEM(block, BF16),
        VMEM(block, BF16),
        VMEM(block, BF16),
        VMEM(block, BF16),
        VMEM(block, BF16),
        VMEM((n_tp, 2, 8, rows), F32),
        DMA((3,)),
        DMA((2, nz)),
        DMA((2, nz)),
        DMA((n_sp,)),
        DMA((n_sp,)),
        DMA((n_tp,)),
        DMA((n_tp,)),
        DMA((8, nz)),
        DMA((n_tp, nx, nz)),
        DMA((ny, nx)),
        DMA((ny, nx)),
        DMA((3, nz)),
        DMA((3, nz)),
        DMA((nz,)),
        DMA((nz,)),
        DMA((n_tp,)),
        DMA((n_tp,)),
    ]
    if balanced:
        attend_scratch, expert_scratch = plane_scratch, grouped_scratch
    n_attend = len(attend_scratch)
    if balanced:
        halves = pairs_beta.reshape(rows, kvb, 2, 128).transpose(0, 2, 1, 3)
        keyed = [
            pairs_alpha.reshape(rows * kva, 128),
            halves.reshape(rows * kvb * 2, 128),
            offset_alpha.T,
            offset_beta.T,
        ]
        places_in = [vm, vm]
        routes = [expert_ids.T, route_weight.T]
    else:
        off = jnp.transpose(jnp.concatenate([offset_alpha, offset_beta], axis=1))
        off = jnp.pad(off, ((0, heads_pad - heads), (0, 0)))
        keyed = [pairs_alpha.reshape(rows, -1), pairs_beta.reshape(rows, -1), off]
        places_in = [hbm]
        routes = [jnp.concatenate([expert_ids.astype(F32), route_weight], axis=1)]
    n_in = len(keyed) + 9
    n_all = n_in + len(routes) + 5

    def kernel(*refs):
        refs = list(refs)
        loads = []
        for k, i in enumerate(small):
            loads.append(pltpu.make_async_copy(refs[i], refs[k - len(small) - 1], refs[-1].at[k]))
            refs[i] = refs[k - len(small) - 1]
        attend_in = refs[:n_in]
        out_ref, settled = refs[n_all : n_all + 2]
        expert_in = refs[n_in:n_all]
        own = refs[n_all + 2 : len(refs) - (len(small) + 1 if small else 0)]

        def attention(*hooks):
            attend = plane_attend if balanced else attend_kernel
            attend(*hooks, *(loads,) * balanced, n_sp, n_tp, nx, kva, kvb, *attend_in, settled, *own[:n_attend])

        if balanced:
            expert_in = attend_in[-2:] + expert_in
        expert = plane_expert if balanced else expert_kernel
        expert(attention, n_sp, n_tp, nx, cap, settled, *expert_in, out_ref, *own[n_attend:])

    operands = [
        query_alpha,
        query_beta,
        *keyed,
        residual_in,
        row(gain_alpha),
        row(gain_beta),
        project_alpha,
        project_beta,
        row(gain_settle),
        row(bias_settle),
        *routes,
        expert_gate,
        expert_up,
        expert_down,
        row(gain_final),
        row(bias_final),
    ]
    specs = [vm, vm, hbm, hbm] + places_in + [vm] * 3 + [hbm] * 2 + [vm] * (2 + len(routes)) + [hbm] * 3 + [vm] * 2
    small = [i for i, spec in enumerate(specs) if spec is vm] if balanced else []
    scratch = [VMEM((rows, cols), BF16)] + attend_scratch + expert_scratch
    if small:
        scratch = scratch + [VMEM(operands[i].shape, operands[i].dtype) for i in small] + [DMA((len(small),))]
        specs = [hbm] * len(specs)
    return pl.pallas_call(
        kernel,
        out_shape=jax.ShapeDtypeStruct((rows, cols), BF16),
        in_specs=specs,
        out_specs=vm,
        scratch_shapes=scratch,
        compiler_params=pltpu.CompilerParams(
            collective_id=0, has_side_effects=True, vmem_limit_bytes=60 * 1024 * 1024
        ),
    )(*operands)


def solution(mesh):
    in_specs = (
        P("sp", "tp"),
        P("sp", "tp"),
        P("sp", "tp", None),
        P("sp", "tp"),
        P("tp"),
        P("sp", "tp"),
        P("sp", "tp", None),
        P("sp", "tp"),
        P("tp"),
        P("tp", None),
        P("tp", None),
        P("tp"),
        P("tp"),
        P("sp", None),
        P("sp", None),
        P("sp", None, "tp"),
        P("sp", None, "tp"),
        P("sp", "tp", None),
        P("tp"),
        P("tp"),
    )
    out_specs = P("sp", "tp")
    return jax.shard_map(body, mesh=mesh, in_specs=in_specs, out_specs=out_specs, check_vma=False)
```

```python
import functools
import jax
import jax.numpy as jnp
from jax import lax
from jax.experimental import pallas as pl
from jax.experimental.pallas import tpu as pltpu
from jax.sharding import PartitionSpec as P

depth_scale = 2.0**0.5
norm_eps = 1e-05
F32 = jnp.float32
BF16 = jnp.bfloat16
VMEM = pltpu.VMEM
DMA = pltpu.SemaphoreType.DMA


def remote(src, dst, send, recv, where):
    return pltpu.make_async_remote_copy(
        src_ref=src,
        dst_ref=dst,
        send_sem=send,
        recv_sem=recv,
        device_id=where,
        device_id_type=pl.DeviceIdType.MESH,
    )


def greet(n_sp, n_tp, sp, tp):
    barrier = pltpu.get_barrier_semaphore()
    for o in range(1, n_sp):
        pl.semaphore_signal(
            barrier,
            inc=1,
            device_id={"sp": lax.rem(sp + o, n_sp), "tp": tp},
            device_id_type=pl.DeviceIdType.MESH,
        )
    for o in range(1, n_tp):
        pl.semaphore_signal(
            barrier,
            inc=1,
            device_id={"sp": sp, "tp": lax.rem(tp + o, n_tp)},
            device_id_type=pl.DeviceIdType.MESH,
        )
    pl.semaphore_wait(barrier, n_sp + n_tp - 2)


def split(x):
    high = x.astype(BF16)
    return high, (x - high.astype(F32)).astype(BF16)


def lane_sums(x):
    ones = jnp.ones((8, x.shape[1]), BF16)
    dims = (((1,), (1,)), ((), ()))
    high, low = split(x)
    return lax.dot_general(ones, high, dims, preferred_element_type=F32) + lax.dot_general(
        ones, low, dims, preferred_element_type=F32
    )


def column(row, rows):
    return jnp.transpose(jnp.broadcast_to(row[0:1, :], (rows, rows)))[:, 0:1]


def stats_start(n_tp, sp, tp, one, two, stat, send, recv, *more):
    for k, value in enumerate((one, two) + more):
        stat[tp, k] = value
    for o in range(1, n_tp):
        remote(
            stat.at[tp], stat.at[tp], send.at[o], recv.at[tp], {"sp": sp, "tp": lax.rem(tp + o, n_tp)}
        ).start()


def stats_rows(n_tp, sp, tp, stat, send, recv):
    for o in range(1, n_tp):
        peer = lax.rem(tp + o, n_tp)
        remote(stat.at[peer], stat.at[peer], send.at[o], recv.at[peer], {"sp": sp, "tp": peer}).wait_recv()
    for o in range(1, n_tp):
        peer = lax.rem(tp + o, n_tp)
        remote(stat.at[tp], stat.at[tp], send.at[o], recv.at[tp], {"sp": sp, "tp": peer}).wait_send()
    total = stat[0]
    for t in range(1, n_tp):
        total = total + stat[t]
    return total[0], total[1]


def stats_finish(n_tp, sp, tp, stat, send, recv, rows):
    one, two = stats_rows(n_tp, sp, tp, stat, send, recv)
    return column(one, rows), column(two, rows)


def norm(total, one, two, gain, bias, columns):
    mean = one / columns
    var = two / columns - mean * mean
    return ((total - mean) * lax.rsqrt(var + norm_eps) * gain + bias).astype(BF16)


def attend_kernel(
    early,
    n_sp,
    n_tp,
    nx,
    kva,
    kvb,
    qa_ref,
    qb_ref,
    kva_hbm,
    kvb_hbm,
    off_hbm,
    res_ref,
    ga_ref,
    gb_ref,
    pa_hbm,
    pb_hbm,
    gs_ref,
    bs_ref,
    out_ref,
    kvbuf,
    offbuf,
    qs,
    acc,
    rem,
    pa,
    pb,
    ya,
    yb,
    part,
    got,
    stat1,
    stat2,
    load_sem,
    kv_send,
    kv_recv,
    off_send,
    off_recv,
    part_send,
    part_recv,
    s1_send,
    s1_recv,
    s2_send,
    s2_recv,
):
    sp = lax.axis_index("sp")
    tp = lax.axis_index("tp")
    nz = n_sp // nx
    z = sp // nx
    x = lax.rem(sp, nx)
    rows = qa_ref.shape[0]
    cols = out_ref.shape[1]
    loads = (
        pltpu.make_async_copy(kva_hbm, kvbuf.at[sp, :, 0 : kva * 128], load_sem.at[0]),
        pltpu.make_async_copy(off_hbm, offbuf.at[sp], load_sem.at[1]),
        pltpu.make_async_copy(pa_hbm, pa, load_sem.at[2]),
        pltpu.make_async_copy(pb_hbm, pb, load_sem.at[3]),
        pltpu.make_async_copy(kvb_hbm, kvbuf.at[sp, :, kva * 128 :], load_sem.at[4]),
    )
    for load in loads:
        load.start()
    greet(n_sp, n_tp, sp, tp)
    lane = lax.broadcasted_iota(jnp.int32, (rows, 128), 1)
    row_i = lax.broadcasted_iota(jnp.int32, (rows, 128), 0)
    first_half = lane < 64
    for u in range(kva):
        q32 = qa_ref[:, u * 128 : (u + 1) * 128].astype(F32) * (64**-0.5)
        qs[u, 0:rows] = jnp.where(first_half, q32, 0.0).astype(BF16)
        qs[u, rows : 2 * rows] = jnp.where(first_half, pltpu.roll(q32, 64, 1), 0.0).astype(BF16)
    acc[...] = jnp.zeros_like(acc)
    rem[...] = jnp.zeros_like(rem)
    tri_r = lax.broadcasted_iota(jnp.int32, (256, 256), 0) % 128
    tri_c = lax.broadcasted_iota(jnp.int32, (256, 256), 1)
    tri = jnp.where((tri_r > tri_c) | (tri_c >= 128), 1.0, 0.0).astype(BF16)

    def block(j):
        gap = (sp - j) * rows
        valid1 = lane < row_i + gap
        valid2 = jnp.concatenate([valid1.astype(F32)] * 2, axis=0) > 0.5

        def unit(query, key, value, offset, scale, valid, left):
            s = lax.dot_general(query, key, (((1,), (1,)), ((), ())), preferred_element_type=F32)
            s = (s if scale is None else s * scale) + offset
            soft = jnp.maximum(s, 0.0) + jnp.log(1.0 + jnp.exp(-jnp.abs(s)))
            used = jnp.where(valid, soft, 0.0)
            high, low = split(used)
            sums = jnp.dot(jnp.concatenate([high, low], axis=1), tri, preferred_element_type=F32)
            w = jnp.where(valid, jnp.exp(s - soft - sums[:, :128] + left), 0.0).astype(BF16)
            return jnp.dot(w, value, preferred_element_type=F32), sums[:, 128:]

        for u in range(kva):
            pair = kvbuf[j, :, u * 128 : (u + 1) * 128]
            offset = jnp.concatenate(
                [
                    jnp.broadcast_to(offbuf[j, 2 * u : 2 * u + 1, :], (rows, 128)),
                    jnp.broadcast_to(offbuf[j, 2 * u + 1 : 2 * u + 2, :], (rows, 128)),
                ],
                axis=0,
            )
            left = rem[2 * u * rows : (2 * u + 2) * rows]
            o, total = unit(qs[u], pair, pair, offset, None, valid2, left)
            rem[2 * u * rows : (2 * u + 2) * rows] = left - total
            acc[:, u * 128 : (u + 1) * 128] += jnp.where(
                first_half, pltpu.roll(o[:rows], 64, 1), o[rows:]
            )
        for u in range(kvb):
            base = kva * 128 + u * 256
            head = 2 * kva + u
            key = kvbuf[j, :, base : base + 128]
            value = kvbuf[j, :, base + 128 : base + 256]
            offset = offbuf[j, head : head + 1, :]
            left = rem[head * rows : (head + 1) * rows]
            query = qb_ref[:, u * 128 : (u + 1) * 128]
            o, total = unit(query, key, value, offset, 128**-0.5, valid1, left)
            rem[head * rows : (head + 1) * rows] = left - total
            c = (kva + u) * 128
            acc[:, c : c + 128] += o

    def sends(s):
        j0 = (z - s) * nx + x
        plan = [(z + 1 < nz, jnp.minimum(z + 1, nz - 1) * nx + x)]
        for d in range(1, nx):
            xo = lax.rem(x + d, nx)
            plan.append(((s > 0) | (x < xo), z * nx + xo))
        made = []
        for k, (cond, dest) in enumerate(plan):
            where = {"sp": dest, "tp": tp}
            made.append(
                (
                    cond,
                    remote(kvbuf.at[j0], kvbuf.at[j0], kv_send.at[s, k], kv_recv.at[j0], where),
                    remote(offbuf.at[j0], offbuf.at[j0], off_send.at[s, k], off_recv.at[j0], where),
                )
            )
        return made

    def wait_block(j):
        where = {"sp": sp, "tp": tp}
        remote(kvbuf.at[j], kvbuf.at[j], kv_send.at[0, 0], kv_recv.at[j], where).wait_recv()
        remote(offbuf.at[j], offbuf.at[j], off_send.at[0, 0], off_recv.at[j], where).wait_recv()

    loads[0].wait()
    loads[1].wait()
    loads[4].wait()

    def forward(s):
        @pl.when(s > 0)
        def _():
            wait_block((z - s) * nx + x)

        for cond, kv_copy, off_copy in sends(s):

            @pl.when(cond)
            def _(kv_copy=kv_copy, off_copy=off_copy):
                off_copy.start()
                kv_copy.start()

    forward(0)

    def level(s, carry):
        src = z - s

        @pl.when(s < z)
        def _():
            forward(s + 1)

        def across(i, inner):
            xo = nx - 1 - i

            @pl.when((s > 0) | (xo <= x))
            def _():
                @pl.when(xo != x)
                def _():
                    wait_block(src * nx + xo)

                block(src * nx + xo)

            return inner

        return lax.fori_loop(0, nx, across, carry)

    lax.fori_loop(0, z + 1, level, 0)
    early()

    wide = kva * 128
    aa = acc[:, :wide]
    ab = acc[:, wide:]
    stats_start(n_tp, sp, tp, lane_sums(aa * aa), lane_sums(ab * ab), stat1, s1_send, s1_recv)
    loads[2].wait()
    loads[3].wait()
    na = (aa * ga_ref[...]).astype(BF16)
    nb = (ab * gb_ref[...]).astype(BF16)
    for t in range(n_tp):
        ya[t] = jnp.dot(na, pa[:, t * cols : (t + 1) * cols], preferred_element_type=F32)
        yb[t] = jnp.dot(nb, pb[:, t * cols : (t + 1) * cols], preferred_element_type=F32)
    sq_a, sq_b = stats_finish(n_tp, sp, tp, stat1, s1_send, s1_recv, rows)
    scale_a = lax.rsqrt(sq_a / (wide * n_tp) + norm_eps)
    scale_b = lax.rsqrt(sq_b / (kvb * 128 * n_tp) + norm_eps)

    def part_copy(o):
        peer = lax.rem(tp + o, n_tp)
        return remote(
            part.at[peer], got.at[tp], part_send.at[o], part_recv.at[tp], {"sp": sp, "tp": peer}
        )

    for o in range(1, n_tp):
        peer = lax.rem(tp + o, n_tp)
        part[peer] = (ya[peer] * scale_a + yb[peer] * scale_b).astype(BF16)
        part_copy(o).start()
    total = (ya[tp] * scale_a + yb[tp] * scale_b).astype(BF16).astype(F32)
    for o in range(1, n_tp):
        peer = lax.rem(tp + o, n_tp)
        remote(
            part.at[peer], got.at[peer], part_send.at[o], part_recv.at[peer], {"sp": sp, "tp": peer}
        ).wait_recv()
        total = total + got[peer].astype(F32)
    mixed = total.astype(BF16).astype(F32)
    first = depth_scale * res_ref[...].astype(F32) + mixed
    stats_start(n_tp, sp, tp, lane_sums(first), lane_sums(first * first), stat2, s2_send, s2_recv)
    for o in range(1, n_tp):
        part_copy(o).wait_send()

    def drain(s, carry):
        for cond, kv_copy, off_copy in sends(s):

            @pl.when(cond)
            def _(kv_copy=kv_copy, off_copy=off_copy):
                off_copy.wait_send()
                kv_copy.wait_send()

        return carry

    lax.fori_loop(0, z + 1, drain, 0)
    one, two = stats_finish(n_tp, sp, tp, stat2, s2_send, s2_recv, rows)
    out_ref[...] = norm(first, one, two, gs_ref[...], bs_ref[...], cols * n_tp)


def plane_attend(
    early,
    send_rows,
    send_scales,
    small_loads,
    n_sp,
    n_tp,
    nx,
    kva,
    kvb,
    qa_ref,
    qb_ref,
    pairs_a_hbm,
    pairs_b_hbm,
    offa_ref,
    offb_ref,
    res_ref,
    ga_ref,
    gb_ref,
    pa_hbm,
    pb_hbm,
    gs_ref,
    bs_ref,
    out_ref,
    raw_a,
    raw_b,
    wide_a,
    wide_b,
    own_a,
    own_b,
    own_off,
    qin,
    kin,
    oin,
    keys2,
    values2,
    left,
    acc,
    obuf,
    ain,
    pa,
    pb,
    ya,
    yb,
    part,
    got,
    across,
    stat1,
    stat2,
    load_sem,
    in_send,
    in_recv,
    o_send,
    o_recv,
    part_send,
    part_recv,
    s1_send,
    s1_recv,
    s2_send,
    s2_recv,
):
    sp = lax.axis_index("sp")
    tp = lax.axis_index("tp")
    nz = n_sp // nx
    z = sp // nx
    x = lax.rem(sp, nx)
    rows = qa_ref.shape[0]
    cols = out_ref.shape[1]
    tall = nx * rows

    def is_alpha(zz, xx):
        return lax.rem(zz + xx, 2) == 0

    loads = (
        pltpu.make_async_copy(pairs_a_hbm, raw_a, load_sem.at[0]),
        pltpu.make_async_copy(pairs_b_hbm, raw_b, load_sem.at[1]),
        pltpu.make_async_copy(pa_hbm, pa, load_sem.at[2]),
        pltpu.make_async_copy(pb_hbm, pb, load_sem.at[3]),
    )
    loads[0].start()
    loads[1].start()
    for load in small_loads:
        load.start()
    greet(n_sp, n_tp, sp, tp)
    for load in small_loads:
        load.wait()
    for u in range(nz):
        own_off[0, u] = offa_ref[2 * u : 2 * u + 2]
        own_off[1, u] = jnp.broadcast_to(offb_ref[u : u + 1], (2, 128))
    loads[0].wait()
    wide_a[...] = raw_a[...].astype(F32)
    for u in range(kva):
        own_a[u] = wide_a[pl.ds(u, rows, stride=kva), :].astype(BF16)
    loads[1].wait()
    wide_b[...] = raw_b[...].astype(F32)
    for u in range(kvb):
        for h in range(2):
            own_b[u, h] = wide_b[pl.ds(h * kvb + u, rows, stride=2 * kvb), :].astype(BF16)
    loads[2].start()
    loads[3].start()

    def in_copies(zz, xx, alpha):
        dest = zz * nx + xx
        where = {"sp": dest, "tp": tp}
        at = pl.ds(pl.multiple_of(zz * 128, 128), 128)
        q_ref = qa_ref if alpha else qb_ref
        kv = (own_a.at[zz], kin.at[0, sp]) if alpha else (own_b.at[zz], kin.at[:, sp])
        return (
            remote(own_off.at[0 if alpha else 1, zz], oin.at[sp], in_send.at[0, dest], in_recv.at[0, sp], where),
            remote(q_ref.at[:, at], qin.at[sp], in_send.at[1, dest], in_recv.at[1, sp], where),
            remote(*kv, in_send.at[2, dest], in_recv.at[2, sp], where),
        )

    def each_dest(act, low, high):
        def hop(t, carry):
            zz = z
            for a in range(nz):
                for i, g in enumerate(sorted(range(nz), key=lambda g: (min(g, nz - 1 - g), abs(g - a)))):
                    zz = jnp.where((z == a) & (t == i), g, zz)
            for step in range(nx):
                xx = lax.rem(x + step + lax.rem(tp, 2), nx)
                there = (zz != z) | (xx != x)
                for alpha in (True, False):

                    @pl.when(there & (is_alpha(zz, xx) == alpha))
                    def _(xx=xx, alpha=alpha):
                        for copy in in_copies(zz, xx, alpha):
                            act(copy)

            return carry

        lax.fori_loop(low, high, hop, 0)

    hops = nz
    each_dest(lambda copy: copy.start(), 0, hops)
    early()

    def o_copy(d):
        return remote(obuf.at[d], ain.at[sp], o_send.at[d], o_recv.at[sp], {"sp": d, "tp": tp})

    lane_t = lax.broadcasted_iota(jnp.int32, (tall, tall), 1)
    row_t = lax.broadcasted_iota(jnp.int32, (tall, tall), 0)
    lane = lax.broadcasted_iota(jnp.int32, (tall, 128), 1)
    tri = jnp.where(row_t > lane_t, 1.0, 0.0).astype(BF16)

    def attend(alpha):
        heads = 2 if alpha else 1
        scale = 64**-0.5 if alpha else 128**-0.5
        at = pl.ds(pl.multiple_of(z * 128, 128), 128)
        oin[sp] = own_off[0 if alpha else 1, z]
        if alpha:
            qin[sp] = qa_ref[:, at]
            kin[0, sp] = own_a[z]
        else:
            qin[sp] = qb_ref[:, at]
            kin[:, sp] = own_b[z]

        def arrive(p):
            for xx in range(nx):
                s = p * nx + xx

                @pl.when(s != sp)
                def _(s=s):
                    where = {"sp": sp, "tp": tp}
                    kv = kin.at[0, s] if alpha else kin.at[:, s]
                    remote(oin.at[s], oin.at[s], in_send.at[0, 0], in_recv.at[0, s], where).wait_recv()
                    remote(qin.at[s], qin.at[s], in_send.at[1, 0], in_recv.at[1, s], where).wait_recv()
                    remote(kv, kv, in_send.at[2, 0], in_recv.at[2, s], where).wait_recv()

            if alpha:
                pair = kin[0, pl.ds(p * nx, nx)].reshape(tall, 128).astype(F32)
                turned = pltpu.roll(pair, 64, 1)
                keys2[p, 0:tall] = jnp.where(lane < 64, pair, 0.0).astype(BF16)
                keys2[p, tall:] = jnp.where(lane < 64, 0.0, turned).astype(BF16)
                values2[p, 0:tall] = jnp.where(lane < 64, turned, 0.0).astype(BF16)
                values2[p, tall:] = jnp.where(lane < 64, 0.0, pair).astype(BF16)

        def step(r, c, diag):
            query = qin[pl.ds(r * nx, nx)].reshape(tall, 128)
            if alpha:
                key, value = keys2[c], values2[c]
            else:
                key = kin[0, pl.ds(c * nx, nx)].reshape(tall, 128)
                value = kin[1, pl.ds(c * nx, nx)].reshape(tall, 128)
            scores = lax.dot_general(query, key, (((1,), (1,)), ((), ())), preferred_element_type=F32)
            valid = lane_t < row_t
            ws = []
            for h in range(heads):
                row = h
                offset = jnp.concatenate([oin[c * nx + i, row : row + 1, :] for i in range(nx)], axis=1)
                s = scores[:, h * tall : (h + 1) * tall] * scale + offset
                soft = jnp.maximum(s, 0.0) + jnp.log(1.0 + jnp.exp(-jnp.abs(s)))
                used = jnp.where(valid, soft, 0.0) if diag else soft
                sums = jnp.dot(used.astype(BF16), tri, preferred_element_type=F32)
                total = jnp.broadcast_to(sums[:, 0:1] + used[:, 0:1], (tall, 128))
                e = s - soft - sums
                if diag:
                    w = jnp.where(valid, jnp.exp(e), 0.0)
                    left[h, r] = -total
                else:
                    before = left[h, r]
                    w = jnp.exp(e + jnp.concatenate([before] * nx, axis=1))
                    left[h, r] = before - total
                ws.append(w.astype(BF16))
            w = ws[0] if heads == 1 else jnp.concatenate(ws, axis=1)
            o = jnp.dot(w, value, preferred_element_type=F32)
            o = o if diag else acc[r] + o
            acc[r] = o

        def finish(r, c):
            @pl.when(c == 0)
            def _():
                obuf[pl.ds(r * nx, nx)] = acc[r].astype(BF16).reshape(nx, rows, 128)
                for xx in range(nx):
                    d = r * nx + xx

                    @pl.when(d != sp)
                    def _(d=d):
                        o_copy(d).start()

                    @pl.when(d == sp)
                    def _(d=d):
                        ain[sp] = obuf[d]

        def phase(k, span):
            low, high = span
            lower_half = z < nz // 2
            up = jnp.where(lower_half, low == 0, high < nz - 1).astype(jnp.int32)
            first = (k == 0).astype(jnp.int32)
            p = first * z + (1 - first) * (up * (high + 1) + (1 - up) * (low - 1))

            arrive(p)


            def at(t):
                return p + t * (1 - up), p - t * up

            @pl.when(k == 0)
            def _():
                step(p, p, True)
                finish(p, p)

            @pl.when(k > 0)
            def _():
                step(p, p, True)
                step(*at(1), False)
                finish(p, p)
                finish(*at(1))

            def two(i, carry):
                step(*at(2 * i), False)
                step(*at(2 * i + 1), False)
                finish(*at(2 * i))
                finish(*at(2 * i + 1))
                return carry

            lax.fori_loop(1, (k + 1) // 2, two, 0)

            @pl.when((k > 0) & (lax.rem(k, 2) == 0))
            def _():
                step(*at(k), False)
                finish(*at(k))

            return jnp.minimum(low, p), jnp.maximum(high, p)

        lax.fori_loop(0, nz, phase, (z, z))

    for alpha in (True, False):

        @pl.when(is_alpha(z, x) == alpha)
        def _(alpha=alpha):
            attend(alpha)

    def o_wait(j, carry):
        @pl.when(j != sp)
        def _():
            remote(obuf.at[j], ain.at[j], o_send.at[0], o_recv.at[j], {"sp": sp, "tp": tp}).wait_recv()

        return carry

    lax.fori_loop(0, n_sp, o_wait, 0)
    wide = kva * 128
    aa = jnp.concatenate([ain[k * nx + k % 2] for k in range(nz)], axis=1).astype(F32)
    ab = jnp.concatenate([ain[k * nx + 1 - k % 2] for k in range(nz)], axis=1).astype(F32)
    stats_start(n_tp, sp, tp, lane_sums(aa * aa), lane_sums(ab * ab), stat1, s1_send, s1_recv)
    loads[2].wait()
    loads[3].wait()
    core = lax.rem(tp, 2)
    y = tp // 2
    sides = ((1 - y) * 2, y * 2)
    to_mate = {"sp": sp, "tp": y * 2 + 1 - core}
    to_far = {"sp": sp, "tp": (1 - y) * 2 + core}
    na = (aa * ga_ref[...]).astype(BF16)
    nb = (ab * gb_ref[...]).astype(BF16)

    def project(t):
        at = pl.ds(pl.multiple_of(t * cols, 128), cols)
        return (
            jnp.dot(na, pa[:, at], preferred_element_type=F32),
            jnp.dot(nb, pb[:, at], preferred_element_type=F32),
        )

    def mate_copy(k):
        return remote(part.at[k], got.at[k], part_send.at[k], part_recv.at[k], to_mate)

    for k in range(2):
        a, b = project(sides[k] + 1 - core)
        part[k, 0] = a.astype(BF16)
        part[k, 1] = b.astype(BF16)
        mate_copy(k).start()
    for k in range(2):
        ya[k], yb[k] = project(sides[k] + core)
    sq_a, sq_b = stats_finish(n_tp, sp, tp, stat1, s1_send, s1_recv, rows)
    scale_a = lax.rsqrt(sq_a / (wide * n_tp) + norm_eps)
    scale_b = lax.rsqrt(sq_b / (kvb * 128 * n_tp) + norm_eps)

    def chip_sum(k):
        mate_copy(k).wait_recv()
        return (ya[k] + got[k, 0].astype(F32)) * scale_a + (yb[k] + got[k, 1].astype(F32)) * scale_b

    half = cols // 2
    across[0] = chip_sum(0).astype(BF16)

    def far_copy(k):
        at = slice(k * half, (k + 1) * half)
        return remote(
            across.at[0, :, at], across.at[1, :, at], part_send.at[2 + k], part_recv.at[2 + k], to_far
        )

    far_copy(0).start()
    far_copy(1).start()
    total = chip_sum(1)
    residual = depth_scale * res_ref[...].astype(F32)
    firsts, sums, squares = [], [], []
    for k in range(2):
        at = slice(k * half, (k + 1) * half)
        far_copy(k).wait_recv()
        mixed = (total[:, at] + across[1, :, at].astype(F32)).astype(BF16).astype(F32)
        firsts.append(residual[:, at] + mixed)
        sums.append(lane_sums(firsts[k]))
        squares.append(lane_sums(firsts[k] * firsts[k]))
        if k == 0:
            centre = sums[0] / half
            middle = column(centre, rows)
        else:
            stats_start(n_tp, sp, tp, sums[0] + sums[1], squares[0] + squares[1], stat2, s2_send, s2_recv, centre)
        send_rows((firsts[k] - middle).astype(BF16), k)
    first = jnp.concatenate(firsts, axis=1)
    for k in range(2):
        far_copy(k).wait_send()
        mate_copy(k).wait_send()
    each_dest(lambda copy: copy.wait_send(), 0, hops)

    def o_drain(j, carry):
        @pl.when(j != sp)
        def _():
            o_copy(j).wait_send()

        return carry

    lax.fori_loop(0, n_sp, o_drain, 0)
    one, two = stats_rows(n_tp, sp, tp, stat2, s2_send, s2_recv)
    mean = one / (cols * n_tp)
    factor = lax.rsqrt(two / (cols * n_tp) - mean * mean + norm_eps)
    centres = [stat2[t, 2] for t in range(n_tp)]
    shifts = [(centres[t] - mean) * factor for t in range(n_tp)]
    send_scales([factor] + shifts)
    flat = (first - column(mean, rows)) * column(factor, rows)
    out_ref[...] = (flat * gs_ref[...] + bs_ref[...]).astype(BF16)


def expert_kernel(
    attention,
    n_sp,
    n_tp,
    nx,
    cap,
    set_ref,
    ids_ref,
    wg_hbm,
    wu_hbm,
    wd_hbm,
    gf_ref,
    bf_ref,
    out_ref,
    wg,
    wu,
    wd,
    sendbuf,
    xbuf,
    gate,
    up,
    hid,
    away,
    arrived,
    home,
    pre,
    peers,
    outb,
    back,
    stat,
    load_sem,
    a_send,
    a_recv,
    x_send,
    x_recv,
    relay_send,
    d_send,
    d_recv,
    y_send,
    y_recv,
    b_send,
    b_recv,
    s_send,
    s_recv,
):
    sp = lax.axis_index("sp")
    tp = lax.axis_index("tp")
    rows, cols = set_ref.shape
    places = n_sp * cap
    ny = n_tp // 2
    y = tp // 2
    core = lax.rem(tp, 2)
    mate = y * 2 + 1 - core
    loads = (
        pltpu.make_async_copy(wg_hbm.at[0], wg, load_sem.at[0]),
        pltpu.make_async_copy(wu_hbm.at[0], wu, load_sem.at[1]),
        pltpu.make_async_copy(wd_hbm.at[0], wd, load_sem.at[2]),
    )

    def loop(low, high, fn):
        def step(i, carry):
            fn(i)
            return carry

        lax.fori_loop(low, high, step, 0)

    def x_copies(j):
        made = []
        for k in range(ny):
            dest = mate if k == 0 else lax.rem(y + k, ny) * 2 + core
            made.append(
                remote(
                    xbuf.at[tp, j], xbuf.at[tp, j], x_send.at[k, j], x_recv.at[tp, j], {"sp": sp, "tp": dest}
                )
            )
        return made

    def spread_out(j):
        @pl.when(j != sp)
        def _():
            remote(
                sendbuf.at[j], xbuf.at[tp, j], a_send.at[0], a_recv.at[j], {"sp": sp, "tp": tp}
            ).wait_recv()

        for copy in x_copies(j):
            copy.start()

    ahead = jnp.maximum(sp // nx - 1, 0) * nx

    for load in loads:
        load.start()
    attention(lambda: loop(0, ahead, spread_out))
    ids = ids_ref[...][:, 0:2]
    expert = lax.broadcasted_iota(jnp.int32, (rows, 128), 1).astype(F32)
    hot = [jnp.where(ids[:, k : k + 1] == expert, 1.0, 0.0) for k in range(2)]
    r = lax.broadcasted_iota(jnp.int32, (rows, rows), 0)
    c = lax.broadcasted_iota(jnp.int32, (rows, rows), 1)
    lower = jnp.where(c < r, 1.0, 0.0).astype(BF16)
    before = jnp.dot(lower, (hot[0] + hot[1]).astype(BF16), preferred_element_type=F32)
    seat = lax.broadcasted_iota(jnp.int32, (rows, places), 1).astype(F32)
    hits = []
    for k in range(2):
        slot = jnp.sum(before * hot[k], axis=1, keepdims=True)
        place = ids[:, k : k + 1] * cap + slot
        hits.append(jnp.where(place == seat, 1.0, 0.0))
    spread = jnp.transpose(hits[0] + hits[1]).astype(BF16)
    sent = jnp.dot(spread, set_ref[...], preferred_element_type=F32).astype(BF16)
    sendbuf[...] = sent.reshape(n_sp, cap, cols)

    def at_sp(o):
        return lax.rem(sp + o, n_sp)

    def a_copy(o):
        dest = at_sp(o)
        return remote(
            sendbuf.at[dest], xbuf.at[tp, sp], a_send.at[o], a_recv.at[sp], {"sp": dest, "tp": tp}
        )

    loop(1, n_sp, lambda o: a_copy(o).start())
    xbuf[tp, sp] = sendbuf[sp]

    def x_wait(t, j):
        remote(xbuf.at[t, j], xbuf.at[t, j], x_send.at[0, 0], x_recv.at[t, j], {"sp": sp, "tp": t}).wait_recv()

    loop(ahead, n_sp, spread_out)

    def relay_copy(k, o):
        t = lax.rem(y + k, ny) * 2 + core
        j = o
        return remote(
            xbuf.at[t, j], xbuf.at[t, j], relay_send.at[k, o], x_recv.at[t, j], {"sp": sp, "tp": mate}
        )

    def gather_dot(t, fresh):
        xs = xbuf[t].reshape(places, cols)
        at = pl.ds(pl.multiple_of(t * cols, 128), cols)
        g = jnp.dot(xs, wg[at, :], preferred_element_type=F32)
        u = jnp.dot(xs, wu[at, :], preferred_element_type=F32)
        if fresh:
            gate[...] = g
            up[...] = u
        else:
            gate[...] += g
            up[...] += u

    loads[0].wait()
    loads[1].wait()
    gather_dot(tp, True)

    def arrive_mate(o):
        x_wait(mate, o)

    loop(0, n_sp, arrive_mate)
    gather_dot(mate, False)

    def from_y(k):
        t = lax.rem(y + k, ny) * 2 + core
        other = lax.rem(y + k, ny) * 2 + 1 - core

        def pass_on(o):
            x_wait(t, o)
            relay_copy(k, o).start()

        loop(0, n_sp, pass_on)
        gather_dot(t, False)

        def arrive(o):
            x_wait(other, o)

        loop(0, n_sp, arrive)
        gather_dot(other, False)

    loop(1, ny, from_y)
    value = gate[...]
    hid[...] = (value / (1.0 + jnp.exp(-value)) * up[...]).astype(BF16)
    loads[2].wait()

    def down(t):
        at = pl.ds(pl.multiple_of(t * cols, 128), cols)
        result = jnp.dot(hid[...], wd[:, at], preferred_element_type=F32)
        return result.astype(BF16).reshape(n_sp, cap, cols)

    def d_copy(k):
        return remote(away.at[k], arrived.at[k], d_send.at[k], d_recv.at[k], {"sp": sp, "tp": mate})

    def down_away(i):
        k = lax.rem(i + 1, ny)
        away[k] = down(lax.rem(y + k, ny) * 2 + 1 - core)
        d_copy(k).start()

    loop(0, ny, down_away)

    def down_home(i):
        k = lax.rem(i + 1, ny)
        home[k] = down(lax.rem(y + k, ny) * 2 + core)

    loop(0, ny, down_home)

    def y_copy(k, o):
        j = at_sp(o)
        return remote(
            pre.at[k, j],
            peers.at[k, j],
            y_send.at[k, o],
            y_recv.at[k, j],
            {"sp": sp, "tp": lax.rem(y + k, ny) * 2 + core},
        )

    for i in range(ny):
        k = (i + 1) % ny
        d_copy(k).wait_recv()
        if k:

            def to_y(o, k=k):
                j = at_sp(o)
                pre[k, j] = (home[k, j].astype(F32) + arrived[k, j].astype(F32)).astype(BF16)
                y_copy(k, o).start()

            loop(1, n_sp, to_y)
            to_y(0)

    def b_copy(o):
        dest = at_sp(o)
        return remote(outb.at[dest], back.at[sp], b_send.at[o], b_recv.at[sp], {"sp": dest, "tp": tp})

    def settle(o):
        j = at_sp(o)
        total = home[0, j].astype(F32) + arrived[0, j].astype(F32)
        for k in range(1, ny):
            remote(
                pre.at[k, j], peers.at[k, j], y_send.at[k, 0], y_recv.at[k, j], {"sp": sp, "tp": mate}
            ).wait_recv()
            total = total + peers[k, j].astype(F32)
        return total.astype(BF16)

    def give_back(o):
        outb[at_sp(o)] = settle(o)
        b_copy(o).start()

    loop(1, n_sp, give_back)
    back[sp] = settle(0)

    def wait_back(o):
        j = lax.rem(sp - o + n_sp, n_sp)
        remote(outb.at[j], back.at[j], b_send.at[0], b_recv.at[j], {"sp": j, "tp": tp}).wait_recv()

    loop(1, n_sp, wait_back)
    flat = back[...].reshape(places, cols)
    weight = ids_ref[...][:, 2:4]
    routed = weight[:, 0:1] * jnp.dot(hits[0].astype(BF16), flat, preferred_element_type=F32)
    routed = routed + weight[:, 1:2] * jnp.dot(hits[1].astype(BF16), flat, preferred_element_type=F32)
    second = depth_scale * set_ref[...].astype(F32) + routed
    stats_start(n_tp, sp, tp, lane_sums(second), lane_sums(second * second), stat, s_send, s_recv)

    def drain(o):
        for copy in x_copies(o):
            copy.wait_send()
        for k in range(1, ny):
            relay_copy(k, o).wait_send()
            y_copy(k, o).wait_send()

    loop(0, n_sp, drain)

    def drain_sp(o):
        a_copy(o).wait_send()
        b_copy(o).wait_send()

    loop(1, n_sp, drain_sp)
    for k in range(ny):
        d_copy(k).wait_send()
    one, two = stats_finish(n_tp, sp, tp, stat, s_send, s_recv, rows)
    out_ref[...] = norm(second, one, two, gf_ref[...], bf_ref[...], cols * n_tp)


def plane_expert(
    attention,
    n_sp,
    n_tp,
    nx,
    cap,
    set_ref,
    gs_ref,
    bs_ref,
    ids_ref,
    weight_ref,
    wg_hbm,
    wu_hbm,
    wd_hbm,
    gf_ref,
    bf_ref,
    out_ref,
    wg,
    wu,
    wd,
    hits,
    packed,
    scales,
    scaled,
    affine,
    xbuf,
    gate,
    up,
    hid,
    away,
    arrived,
    home,
    mid,
    midx,
    midy,
    gotd,
    gotx,
    goty,
    outb,
    back,
    stat,
    load_sem,
    a_send,
    a_recv,
    t_send,
    t_recv,
    g_send,
    g_recv,
    x_send,
    x_recv,
    d_send,
    d_recv,
    m_send,
    m_recv,
    b_send,
    b_recv,
    s_send,
    s_recv,
):
    sp = lax.axis_index("sp")
    tp = lax.axis_index("tp")
    rows, cols = set_ref.shape
    nz = n_sp // nx
    z = sp // nx
    x = lax.rem(sp, nx)
    core = lax.rem(tp, 2)
    y = tp // 2
    mate = y * 2 + 1 - core
    far = (1 - y) * 2 + core
    far_mate = (1 - y) * 2 + 1 - core
    to_mate = {"sp": sp, "tp": mate}
    to_x = {"sp": z * nx + 1 - x, "tp": tp}
    to_y = {"sp": sp, "tp": far}
    table = [sorted(range(nz), key=lambda g: (abs(g - a), (g - a) * (1 if a < nz // 2 else -1))) for a in range(nz)]

    def near(i):
        pick = table[0][i]
        for a in range(1, nz):
            pick = jnp.where(z == a, table[a][i], pick)
        return pick

    loads = (
        pltpu.make_async_copy(wg_hbm.at[0], wg, load_sem.at[0]),
        pltpu.make_async_copy(wu_hbm.at[0], wu, load_sem.at[1]),
        pltpu.make_async_copy(wd_hbm.at[0], wd, load_sem.at[2]),
    )

    def g_copy(o):
        where = {"sp": sp, "tp": lax.rem(tp + o, n_tp)}
        return remote(affine.at[tp], affine.at[tp], g_send.at[o], g_recv.at[tp], where)

    def others(fn):
        def one(d, carry):
            @pl.when(d != sp)
            def _():
                fn(d)

            return carry

        lax.fori_loop(0, n_sp, one, 0)

    def early():
        for load in loads:
            load.start()
        affine[tp, 0:1] = gs_ref[...]
        affine[tp, 1:2] = bs_ref[...]
        for o in range(1, n_tp):
            g_copy(o).start()
        ids = [ids_ref[k : k + 1, :] for k in range(2)]
        r = lax.broadcasted_iota(jnp.int32, (rows, rows), 0)
        c = lax.broadcasted_iota(jnp.int32, (rows, rows), 1)
        upper = jnp.where(r < c, 1.0, 0.0).astype(BF16)
        group = lax.broadcasted_iota(jnp.int32, (8, rows), 0) * nx
        hot = jnp.where((ids[0] >= group) & (ids[0] < group + nx), 1.0, 0.0)
        before = jnp.dot(hot.astype(BF16), upper, preferred_element_type=F32)
        seat = lax.broadcasted_iota(jnp.int32, (cap, rows), 0).astype(F32)
        for g in range(nz):
            match = jnp.where(seat == before[g : g + 1], hot[g : g + 1], 0.0).astype(BF16)
            hits[g * cap : (g + 1) * cap] = match
            scales[g] = jnp.zeros((8, 128), F32)

    def a_copy(i, k):
        g = near(i)
        at = slice(k * half, (k + 1) * half)
        return remote(
            packed.at[g, :, at],
            xbuf.at[tp, x, z, :, at],
            a_send.at[k, i],
            a_recv.at[k, z],
            {"sp": g * nx + x, "tp": tp},
        )

    def t_copy(d):
        return remote(scales.at[d // nx], scaled.at[sp], t_send.at[d], t_recv.at[sp], {"sp": d, "tp": tp})

    half = cols // 2

    def send_rows(part, k):
        sent = jnp.dot(hits[...], part, preferred_element_type=F32).astype(BF16)
        at = slice(k * half, (k + 1) * half)
        packed[:, :, at] = sent.reshape(nz, cap, half)
        for i in range(1, nz):
            a_copy(i, k).start()
        xbuf[tp, x, z, :, at] = packed[z, :, at]

    def compact(lines, g):
        line = lax.broadcasted_iota(jnp.int32, (8, rows), 0)
        tile = jnp.zeros((8, rows), F32)
        for k, value in enumerate(lines):
            tile = jnp.where(line == k, value, tile)
        high, low = split(tile)
        dims = (((1,), (1,)), ((), ()))
        match = hits[g * cap : (g + 1) * cap]
        return lax.dot_general(high, match, dims, preferred_element_type=F32) + lax.dot_general(
            low, match, dims, preferred_element_type=F32
        )

    def send_scales(lines):
        for g in range(nz):
            share = []
            for e in range(nx):
                chosen = [
                    jnp.where(ids_ref[k : k + 1, :] == g * nx + e, weight_ref[k : k + 1, :], 0.0) for k in range(2)
                ]
                share.append(chosen[0] + chosen[1])
            scales[g, :, 0:cap] = compact(lines + share, g)
        others(lambda d: t_copy(d).start())
        scaled[sp] = scales[z]

    def x_copy(kind, t, xs, g, where):
        block = xbuf.at[t, xs, g]
        return remote(block, block, x_send.at[kind, g], x_recv.at[t, xs, g], where)

    def x_wait(t, xs, g):
        block = xbuf.at[t, xs, g]
        remote(block, block, x_send.at[0, 0], x_recv.at[t, xs, g], to_mate).wait_recv()

    def when_x_first(g, fn):
        pl.when(lax.rem(g, 2) == 0)(fn)

    def when_y_first(g, fn):
        pl.when(lax.rem(g, 2) == 1)(fn)

    def own_out(i):
        g = near(i)
        if i:
            for k in range(2):
                block = xbuf.at[tp, x, g, :, k * half : (k + 1) * half]
                remote(block, block, a_send.at[0, 0], a_recv.at[k, g], to_mate).wait_recv()
        x_copy(1, tp, x, g, to_x).start()
        x_copy(2, tp, x, g, to_y).start()
        x_copy(0, tp, x, g, to_mate).start()

    def pass_on(i):
        g = near(i)
        x_wait(tp, 1 - x, g)
        when_x_first(g, lambda: x_copy(4, tp, 1 - x, g, to_y).start())
        x_copy(3, tp, 1 - x, g, to_mate).start()
        x_wait(far, x, g)
        when_y_first(g, lambda: x_copy(6, far, x, g, to_x).start())
        x_copy(5, far, x, g, to_mate).start()

    def pass_diag(i):
        g = near(i)
        x_wait(far, 1 - x, g)
        x_copy(7, far, 1 - x, g, to_mate).start()

    def t_wait(j):
        remote(scaled.at[j], scaled.at[j], t_send.at[0], t_recv.at[j], to_mate).wait_recv()

    def piece(t, xs, fresh):
        factor, shift = [], []
        for g in range(nz):
            j = g * nx + xs
            factor.append(scaled[j, 0:1, :])
            shift.append(scaled[j, pl.ds(1 + t, 1), :])
        turned = jnp.transpose(jnp.concatenate(factor + shift, axis=0))
        gain, bias = affine[t, 0:1, :], affine[t, 1:2, :]
        block = jnp.concatenate(
            [
                (
                    (xbuf[t, xs, g].astype(F32) * turned[0:cap, g : g + 1] + turned[0:cap, nz + g : nz + g + 1]) * gain
                    + bias
                ).astype(BF16)
                for g in range(nz)
            ],
            axis=0,
        )
        at = pl.ds(pl.multiple_of(t * cols, 128), cols)
        g = jnp.dot(block, wg[at, :], preferred_element_type=F32)
        u = jnp.dot(block, wu[at, :], preferred_element_type=F32)
        if fresh:
            gate[xs] = g
            up[xs] = u
        else:
            gate[xs] += g
            up[xs] += u

    def all_in(t, xs):
        def one(g, carry):
            x_wait(t, xs, g)
            return carry

        lax.fori_loop(0, nz, one, 0)

    def first_rows(part, k):
        send_rows(part, k)
        if k == 1:
            own_out(0)
            own_out(1)
            pass_on(0)

    attention(early, first_rows, send_scales)
    for i in range(2, nz):
        own_out(i)
        if i < nz - 1:
            pass_on(i - 1)
            pass_diag(i - 2)
    loads[0].wait()
    loads[1].wait()
    others(t_wait)
    for o in range(1, n_tp):
        peer = lax.rem(tp + o, n_tp)
        remote(affine.at[peer], affine.at[peer], g_send.at[0], g_recv.at[peer], to_mate).wait_recv()
    piece(tp, x, True)
    pass_on(nz - 2)
    pass_diag(nz - 3)
    all_in(mate, x)
    piece(mate, x, False)
    pass_on(nz - 1)
    pass_diag(nz - 2)
    piece(tp, 1 - x, True)
    piece(far, x, False)
    all_in(far_mate, x)
    piece(far_mate, x, False)
    pass_diag(nz - 1)
    all_in(mate, 1 - x)
    piece(mate, 1 - x, False)
    piece(far, 1 - x, False)
    all_in(far_mate, 1 - x)
    piece(far_mate, 1 - x, False)
    for xs in range(nx):
        value = gate[xs]
        line = [scaled[g * nx + xs, pl.ds(1 + n_tp + x, 1), :] for g in range(nz)]
        turned = jnp.transpose(jnp.concatenate(line + line, axis=0))
        weight = jnp.concatenate([turned[0:cap, g : g + 1] for g in range(nz)], axis=0)
        hid[xs * nz * cap : (xs + 1) * nz * cap] = (value / (1.0 + jnp.exp(-value)) * up[xs] * weight).astype(BF16)
    loads[2].wait()

    def down(t, xs):
        at = pl.ds(pl.multiple_of(t * cols, 128), cols)
        part = hid[pl.ds(pl.multiple_of(xs * (nz * cap), 16), nz * cap), :]
        result = jnp.dot(part, wd[:, at], preferred_element_type=F32)
        return result.astype(BF16).reshape(nz, cap, cols)

    def d_copy(k, xs):
        return remote(away.at[k, xs], arrived.at[k, xs], d_send.at[k, xs], d_recv.at[k, xs], to_mate)

    away[1, 1 - x] = down(far_mate, 1 - x)
    d_copy(1, 1 - x).start()
    home[1, 1 - x] = down(far, 1 - x)
    away[0, 1 - x] = down(mate, 1 - x)
    d_copy(0, 1 - x).start()
    away[1, x] = down(far_mate, x)
    d_copy(1, x).start()

    def pair(k, xs, g):
        return home[k, xs, g].astype(F32) + arrived[k, xs, g].astype(F32)

    def m_copy(kind, src, dst, g, where):
        return remote(src.at[g], dst.at[g], m_send.at[kind, g], m_recv.at[kind, g], where)

    def diag_copy(g, where):
        return m_copy(0, mid, gotd, g, where)

    def x_send_copy(g):
        return m_copy(1, midx, gotx, g, to_x)

    def y_send_copy(g):
        return m_copy(2, midy, goty, g, to_y)

    order = range(nz - 1, -1, -1)
    late = order[nz // 2 :]

    def plain(i):
        g = near(i)

        def plain_x():
            midx[g] = pair(0, 1 - x, g).astype(BF16)
            x_send_copy(g).start()

        def plain_y():
            midy[g] = pair(1, x, g).astype(BF16)
            y_send_copy(g).start()

        when_x_first(g, plain_x)
        when_y_first(g, plain_y)

    def joined(i):
        g = near(i)
        diag_copy(g, to_mate).wait_recv()

        def joined_y():
            midy[g] = (pair(1, x, g) + gotd[g].astype(F32)).astype(BF16)
            y_send_copy(g).start()

        def joined_x():
            midx[g] = (pair(0, 1 - x, g) + gotd[g].astype(F32)).astype(BF16)
            x_send_copy(g).start()

        when_x_first(g, joined_y)
        when_y_first(g, joined_x)

    def diagonal(i):
        g = near(i)
        mid[g] = pair(1, 1 - x, g).astype(BF16)
        when_x_first(g, lambda: diag_copy(g, to_x).start())
        when_y_first(g, lambda: diag_copy(g, to_y).start())

    d_copy(1, 1 - x).wait_recv()
    for i in order:
        diagonal(i)
    home[0, 1 - x] = down(tp, 1 - x)
    home[1, x] = down(far, x)
    d_copy(1, x).wait_recv()
    d_copy(0, 1 - x).wait_recv()
    for i in order[: nz // 2]:
        plain(i)
    for i in order[: nz // 2]:
        joined(i)
    away[0, x] = down(mate, x)
    d_copy(0, x).start()
    for i in late:
        plain(i)
    for i in late:
        joined(i)

    def b_copy(i):
        g = near(i)
        return remote(outb.at[g], back.at[z], b_send.at[i], b_recv.at[z], {"sp": g * nx + x, "tp": tp})

    home[0, x] = down(tp, x)
    d_copy(0, x).wait_recv()
    for i in order:
        g = near(i)
        x_send_copy(g).wait_recv()
        y_send_copy(g).wait_recv()
        total = (pair(0, x, g) + gotx[g].astype(F32) + goty[g].astype(F32)).astype(BF16)
        if i:
            outb[g] = total
            b_copy(i).start()
        else:
            back[z] = total
    for i in range(1, nz):
        g = near(i)
        remote(outb.at[g], back.at[g], b_send.at[0], b_recv.at[g], to_mate).wait_recv()
    flat = back[...].reshape(nz * cap, cols)
    routed = lax.dot_general(hits[...], flat, (((0,), (0,)), ((), ())), preferred_element_type=F32)
    second = depth_scale * set_ref[...].astype(F32) + routed
    stats_start(n_tp, sp, tp, lane_sums(second), lane_sums(second * second), stat, s_send, s_recv)
    others(lambda d: t_copy(d).wait_send())
    for o in range(1, n_tp):
        g_copy(o).wait_send()
    for i in range(nz):
        g = near(i)
        if i:
            a_copy(i, 0).wait_send()
            a_copy(i, 1).wait_send()
            b_copy(i).wait_send()
        x_copy(1, tp, x, g, to_x).wait_send()
        x_copy(2, tp, x, g, to_y).wait_send()
        for kind in (0, 3, 5, 7):
            x_copy(kind, tp, x, g, to_mate).wait_send()
        when_x_first(g, lambda g=g: x_copy(4, tp, 1 - x, g, to_y).wait_send())
        when_y_first(g, lambda g=g: x_copy(6, far, x, g, to_x).wait_send())
        diag_copy(g, to_mate).wait_send()
        x_send_copy(g).wait_send()
        y_send_copy(g).wait_send()
    for k in range(2):
        d_copy(k, 0).wait_send()
        d_copy(k, 1).wait_send()
    one, two = stats_finish(n_tp, sp, tp, stat, s_send, s_recv, rows)
    out_ref[...] = norm(second, one, two, gf_ref[...], bf_ref[...], cols * n_tp)


def body(
    residual_in,
    query_alpha,
    pairs_alpha,
    offset_alpha,
    gain_alpha,
    query_beta,
    pairs_beta,
    offset_beta,
    gain_beta,
    project_alpha,
    project_beta,
    gain_settle,
    bias_settle,
    expert_ids,
    route_weight,
    expert_gate,
    expert_up,
    expert_down,
    gain_final,
    bias_final,
):
    n_sp = lax.axis_size("sp")
    n_tp = lax.axis_size("tp")
    nx = 2 ** ((n_sp.bit_length() - 1) // 2)
    nz = n_sp // nx
    rows, cols = residual_in.shape
    kva = pairs_alpha.shape[1]
    kvb = pairs_beta.shape[1]
    heads = 2 * kva + kvb
    heads_pad = -(-heads // 8) * 8
    kv_cols = kva * 128 + kvb * 256
    inner = kva * 128
    inner_b = kvb * 128
    vm = pl.BlockSpec(memory_space=VMEM)
    hbm = pl.BlockSpec(memory_space=pl.ANY)
    row = lambda v: v.reshape(1, -1)
    cap = -(-(3 * rows // n_sp) // 16) * 16
    places = n_sp * cap
    ny = n_tp // 2
    width, units = expert_gate.shape[1:]
    attend_scratch = [
        VMEM((n_sp, rows, kv_cols), BF16),
        VMEM((n_sp, heads_pad, rows), F32),
        VMEM((kva, 2 * rows, 128), BF16),
        VMEM((rows, inner + inner_b), F32),
        VMEM((heads * rows, 128), F32),
        VMEM(project_alpha.shape, BF16),
        VMEM(project_beta.shape, BF16),
        VMEM((n_tp, rows, cols), F32),
        VMEM((n_tp, rows, cols), F32),
        VMEM((n_tp, rows, cols), BF16),
        VMEM((n_tp, rows, cols), BF16),
        VMEM((n_tp, 2, 8, rows), F32),
        VMEM((n_tp, 2, 8, rows), F32),
        DMA((5,)),
        DMA((nz, nx)),
        DMA((n_sp,)),
        DMA((nz, nx)),
        DMA((n_sp,)),
        DMA((n_tp,)),
        DMA((n_tp,)),
        DMA((n_tp,)),
        DMA((n_tp,)),
        DMA((n_tp,)),
        DMA((n_tp,)),
    ]
    balanced = (nx, ny, kva, kvb) == (2, 2, nz, nz)
    tall = nx * rows
    plane_scratch = [
        VMEM((rows * kva, 128), BF16),
        VMEM((rows * kvb * 2, 128), BF16),
        VMEM((rows * kva, 128), F32),
        VMEM((rows * kvb * 2, 128), F32),
        VMEM((kva, rows, 128), BF16),
        VMEM((kvb, 2, rows, 128), BF16),
        VMEM((2, nz, 2, 128), F32),
        VMEM((n_sp, rows, 128), BF16),
        VMEM((2, n_sp, rows, 128), BF16),
        VMEM((n_sp, 2, 128), F32),
        VMEM((nz, 2 * tall, 128), BF16),
        VMEM((nz, 2 * tall, 128), BF16),
        VMEM((2, nz, tall, 128), F32),
        VMEM((nz, tall, 128), F32),
        VMEM((n_sp, rows, 128), BF16),
        VMEM((n_sp, rows, 128), BF16),
        VMEM(project_alpha.shape, BF16),
        VMEM(project_beta.shape, BF16),
        VMEM((ny, rows, cols), F32),
        VMEM((ny, rows, cols), F32),
        VMEM((ny, 2, rows, cols), BF16),
        VMEM((ny, 2, rows, cols), BF16),
        VMEM((2, rows, cols), BF16),
        VMEM((n_tp, 2, 8, rows), F32),
        VMEM((n_tp, 3, 8, rows), F32),
        DMA((4,)),
        DMA((3, n_sp)),
        DMA((3, n_sp)),
        DMA((n_sp,)),
        DMA((n_sp,)),
        DMA((n_tp,)),
        DMA((n_tp,)),
        DMA((n_tp,)),
        DMA((n_tp,)),
        DMA((n_tp,)),
        DMA((n_tp,)),
    ]
    expert_scratch = [
        VMEM((width, units), BF16),
        VMEM((width, units), BF16),
        VMEM((units, width), BF16),
        VMEM((n_sp, cap, cols), BF16),
        VMEM((n_tp, n_sp, cap, cols), BF16),
        VMEM((places, units), F32),
        VMEM((places, units), F32),
        VMEM((places, units), BF16),
        VMEM((ny, n_sp, cap, cols), BF16),
        VMEM((ny, n_sp, cap, cols), BF16),
        VMEM((ny, n_sp, cap, cols), BF16),
        VMEM((ny, n_sp, cap, cols), BF16),
        VMEM((ny, n_sp, cap, cols), BF16),
        VMEM((n_sp, cap, cols), BF16),
        VMEM((n_sp, cap, cols), BF16),
        VMEM((n_tp, 2, 8, rows), F32),
        DMA((3,)),
        DMA((n_sp,)),
        DMA((n_sp,)),
        DMA((ny, n_sp)),
        DMA((n_tp, n_sp)),
        DMA((ny, n_sp)),
        DMA((ny,)),
        DMA((ny,)),
        DMA((ny, n_sp)),
        DMA((ny, n_sp)),
        DMA((n_sp,)),
        DMA((n_sp,)),
        DMA((n_tp,)),
        DMA((n_tp,)),
    ]
    block = (nz, cap, cols)
    grouped_scratch = [
        VMEM((width, units), BF16),
        VMEM((width, units), BF16),
        VMEM((units, width), BF16),
        VMEM((nz * cap, rows), BF16),
        VMEM(block, BF16),
        VMEM((nz, 8, 128), F32),
        VMEM((n_sp, 8, 128), F32),
        VMEM((n_tp, 8, cols), F32),
        VMEM((n_tp, nx) + block, BF16),
        VMEM((nx, nz * cap, units), F32),
        VMEM((nx, nz * cap, units), F32),
        VMEM((places, units), BF16),
        VMEM((ny, nx) + block, BF16),
        VMEM((ny, nx) + block, BF16),
        VMEM((ny, nx) + block, BF16),
        VMEM(block, BF16),
        VMEM(block, BF16),
        VMEM(block, BF16),
        VMEM(block, BF16),
        VMEM(block, BF16),
        VMEM(block, BF16),
        VMEM(block, BF16),
        VMEM(block, BF16),
        VMEM((n_tp, 2, 8, rows), F32),
        DMA((3,)),
        DMA((2, nz)),
        DMA((2, nz)),
        DMA((n_sp,)),
        DMA((n_sp,)),
        DMA((n_tp,)),
        DMA((n_tp,)),
        DMA((8, nz)),
        DMA((n_tp, nx, nz)),
        DMA((ny, nx)),
        DMA((ny, nx)),
        DMA((3, nz)),
        DMA((3, nz)),
        DMA((nz,)),
        DMA((nz,)),
        DMA((n_tp,)),
        DMA((n_tp,)),
    ]
    if balanced:
        attend_scratch, expert_scratch = plane_scratch, grouped_scratch
    n_attend = len(attend_scratch)
    if balanced:
        halves = pairs_beta.reshape(rows, kvb, 2, 128).transpose(0, 2, 1, 3)
        keyed = [
            pairs_alpha.reshape(rows * kva, 128),
            halves.reshape(rows * kvb * 2, 128),
            offset_alpha.T,
            offset_beta.T,
        ]
        places_in = [vm, vm]
        routes = [expert_ids.T, route_weight.T]
    else:
        off = jnp.transpose(jnp.concatenate([offset_alpha, offset_beta], axis=1))
        off = jnp.pad(off, ((0, heads_pad - heads), (0, 0)))
        keyed = [pairs_alpha.reshape(rows, -1), pairs_beta.reshape(rows, -1), off]
        places_in = [hbm]
        routes = [jnp.concatenate([expert_ids.astype(F32), route_weight], axis=1)]
    n_in = len(keyed) + 9
    n_all = n_in + len(routes) + 5

    def kernel(*refs):
        refs = list(refs)
        loads = []
        for k, i in enumerate(small):
            loads.append(pltpu.make_async_copy(refs[i], refs[k - len(small) - 1], refs[-1].at[k]))
            refs[i] = refs[k - len(small) - 1]
        attend_in = refs[:n_in]
        out_ref, settled = refs[n_all : n_all + 2]
        expert_in = refs[n_in:n_all]
        own = refs[n_all + 2 : len(refs) - (len(small) + 1 if small else 0)]

        def attention(*hooks):
            attend = plane_attend if balanced else attend_kernel
            attend(*hooks, *(loads,) * balanced, n_sp, n_tp, nx, kva, kvb, *attend_in, settled, *own[:n_attend])

        if balanced:
            expert_in = attend_in[-2:] + expert_in
        expert = plane_expert if balanced else expert_kernel
        expert(attention, n_sp, n_tp, nx, cap, settled, *expert_in, out_ref, *own[n_attend:])

    operands = [
        query_alpha,
        query_beta,
        *keyed,
        residual_in,
        row(gain_alpha),
        row(gain_beta),
        project_alpha,
        project_beta,
        row(gain_settle),
        row(bias_settle),
        *routes,
        expert_gate,
        expert_up,
        expert_down,
        row(gain_final),
        row(bias_final),
    ]
    specs = [vm, vm, hbm, hbm] + places_in + [vm] * 3 + [hbm] * 2 + [vm] * (2 + len(routes)) + [hbm] * 3 + [vm] * 2
    small = [i for i, spec in enumerate(specs) if spec is vm] if balanced else []
    scratch = [VMEM((rows, cols), BF16)] + attend_scratch + expert_scratch
    if small:
        scratch = scratch + [VMEM(operands[i].shape, operands[i].dtype) for i in small] + [DMA((len(small),))]
        specs = [hbm] * len(specs)
    return pl.pallas_call(
        kernel,
        out_shape=jax.ShapeDtypeStruct((rows, cols), BF16),
        in_specs=specs,
        out_specs=vm,
        scratch_shapes=scratch,
        compiler_params=pltpu.CompilerParams(
            collective_id=0, has_side_effects=True, vmem_limit_bytes=60 * 1024 * 1024
        ),
    )(*operands)


def solution(mesh):
    in_specs = (
        P("sp", "tp"),
        P("sp", "tp"),
        P("sp", "tp", None),
        P("sp", "tp"),
        P("tp"),
        P("sp", "tp"),
        P("sp", "tp", None),
        P("sp", "tp"),
        P("tp"),
        P("tp", None),
        P("tp", None),
        P("tp"),
        P("tp"),
        P("sp", None),
        P("sp", None),
        P("sp", None, "tp"),
        P("sp", None, "tp"),
        P("sp", "tp", None),
        P("tp"),
        P("tp"),
    )
    out_specs = P("sp", "tp")
    return jax.shard_map(body, mesh=mesh, in_specs=in_specs, out_specs=out_specs, check_vma=False)
```
